32 devices in a mesh: ep: 8 (over z, x), tp: 4 (over y, core).
Axes of the slice: x: 2, y: 2, z: 4, core: 2. Of those that a mesh axis runs over, the one named last changes fastest.
Arguments:
- tokens: bfloat16 [1024, 4096], P('ep', 'tp'), may hold values from -6 to 6
- norm_gain: float32 [4096], replicated, may hold values from 0.1 to 1.9
- expert_ids: int32 [1024, 2], P('ep'), may hold values from 0 to 7, all different within a row; in each aligned block of 128 rows (0 to 127, 128 to 255, ...) at most 48 rows name the same one
- expert_gates: float32 [1024, 2], P('ep'), may hold values from 0.2 to 1
- gate_proj: bfloat16 [8, 4096, 512], P('ep', None, 'tp'), may hold values from -0.09375 to 0.09375
- up_proj: bfloat16 [8, 4096, 512], P('ep', None, 'tp'), may hold values from -0.09375 to 0.09375
- down_proj: bfloat16 [8, 512, 4096], P('ep', None, 'tp'), may hold values from -0.25 to 0.25
- shared_gate: bfloat16 [4096, 512], P('ep', 'tp'), may hold values from -0.09375 to 0.09375
- shared_up: bfloat16 [4096, 512], P('ep', 'tp'), may hold values from -0.09375 to 0.09375
- shared_down: bfloat16 [512, 4096], P(None, 'tp'), may hold values from -0.25 to 0.25
Outputs:
- mixed: bfloat16 [1024, 4096], P('ep', 'tp')
The draws below stay inside these ranges and needn't reach their ends.
Inputs may be any that keep to these rules, and one draw needn't show every extreme that they name: `expert_ids`: each row names 2 distinct experts. Among the 128 rows of one index of ep (aligned blocks) no expert is named by more than 48 rows, a bound that some block reaches.
All inputs are finite; a program needn't handle non-finite values.
Results may differ from the reference program's by a relative error of at most 0.0067.
Values may be sent and summed in bfloat16 or wider, within the bound.
A program may use at most 64 MiB of HBM per device.

```python
import math
import jax
import jax.numpy as jnp
import numpy as np
from jax import lax

D = 4096
EXPERT_DIM = 512
SHARED = 512
TOP = 2
TOK_DEV = 128
EXPERTS = 8
CAP = 48
TOKENS = 1024
N_EP = 8


def block_scale(stream_key, shape, shards, least, high):
    level = 1.0
    for axis_at, shards_of in shards:
        draws = jax.random.uniform(jax.random.fold_in(jax.random.fold_in(stream_key, 6), axis_at), (shards_of,), jnp.float32, least / len(shards), high / len(shards))
        level = level * jnp.repeat(jnp.exp(draws), shape[axis_at] // shards_of).reshape((-1,) + (1,) * (len(shape) - 1 - axis_at))
    return level


def routed_block(stream_key, own, number, rows, number_of, top, bound, lean):
    order = jax.random.permutation(stream_key, number_of)
    packed, usual = portions_of(number_of, rows * top, bound, lean, True), portions_of(number_of, rows * top, bound, lean, False)
    places = jnp.arange(number_of)

    def named(lengths, turn):
        used = int((lengths > 0).sum())
        fixed = max(1, used // 4)
        shifted = fixed + (places - fixed + turn * (used - fixed)) % max(1, number_of - fixed)
        return jnp.zeros((number_of,), jnp.int32).at[order[jnp.where(places < fixed, places, shifted)]].set(jnp.asarray(lengths, jnp.int32))

    lengths = jnp.where(number % 4 == 0, named(packed, number // 4), named(usual, number - number // 4 - 1))
    mixed = jax.random.permutation(jax.random.fold_in(own, 3), number_of)
    source_of, taker = mixed[0:number_of // 2 * 2:2], mixed[1:number_of // 2 * 2:2]
    room = jnp.minimum(lengths[source_of] - 1, bound - lengths[taker]) // 2
    room = jnp.where((source_of == order[0]) | (taker == order[0]) | (lengths[taker] == 0), 0, jnp.maximum(room, 0))
    shifted = jax.random.randint(jax.random.fold_in(own, 4), (number_of // 2,), 0, 1 << 20) % (room + 1)
    lengths = lengths.at[source_of].add(-shifted).at[taker].add(shifted)
    items = jnp.searchsorted(jnp.cumsum(lengths), jnp.arange(rows * top), side="right").astype(jnp.int32)
    listing = items.reshape(top, rows).T
    listing = listing[jax.random.permutation(jax.random.fold_in(own, 1), rows)]
    turn = jax.random.randint(jax.random.fold_in(own, 2), (rows, 1), 0, top)
    return jnp.take_along_axis(listing, (jnp.arange(top)[None, :] + turn) % top, axis=1)


def portions_of(amount, total, bound, slope, full):
    weights = [(1 << 20) // math.isqrt(rank ** slope) + 1 for rank in range(1, amount + 1)]
    largest = bound if full else min(bound, max(-(-total // amount), total * weights[0] // sum(weights)))
    least = 1 if total - largest >= amount - 1 else 0
    given, rest = [largest] + [least] * (amount - 1), total - largest - least * (amount - 1)
    while rest > 0:
        movable = [i for i in range(1, amount) if given[i] < largest] or [i for i in range(1, amount) if given[i] < bound]
        whole, budget = sum([weights[i] for i in movable]), rest
        for i in movable:
            extra = min(bound - given[i], max(1, budget * weights[i] // whole), rest)
            given[i] = given[i] + extra
            rest = rest - extra
    return np.array(given)


def scatter_about(own_key, shape, deviation, most, shards=(), held_as=jnp.bfloat16):
    loudness = block_scale(own_key, shape, shards, -0.22, 0.18) if shards else 1.0
    drawn = jax.random.normal(own_key, shape, jnp.float32) * deviation * loudness
    return jnp.minimum(jnp.maximum(drawn, -most), most).astype(held_as)


def setup_inputs(seed: int = 0) -> dict:
    seeds = jax.random.split(jax.random.key(seed), 11)
    tokens = scatter_about(seeds[0], (TOKENS, D), 1.0, 6.0, ((0, 8), (1, 4)))
    norm_gain = jnp.clip(1.0 + 0.18 * jax.random.normal(seeds[1], (D,), jnp.float32), 0.1, 1.9)
    expert_ids_keys = jax.random.split(jax.random.fold_in(seeds[2], 1), TOKENS // TOK_DEV)
    expert_ids_turns = jax.random.permutation(jax.random.fold_in(seeds[2], 3), TOKENS // TOK_DEV)
    expert_ids = jax.vmap(lambda own, number: routed_block(jax.random.fold_in(seeds[2], 2), own, number, TOK_DEV, EXPERTS, TOP, CAP, 2))(expert_ids_keys, expert_ids_turns).reshape((TOKENS, TOP))
    expert_gates = jnp.clip(jnp.exp(math.log(1.0) - 1.609438 * jax.random.uniform(seeds[3], (TOKENS, TOP), jnp.float32) ** block_scale(seeds[3], (TOKENS, TOP), ((0, 8),), -0.2, 0.2)), 0.2, 1.0)
    gate_proj = scatter_about(seeds[4], (EXPERTS, D, EXPERT_DIM), D ** -0.5, 0.09375, ((0, 8), (2, 4)))
    up_proj = scatter_about(seeds[5], (EXPERTS, D, EXPERT_DIM), D ** -0.5, 0.09375, ((0, 8), (2, 4)))
    down_proj = scatter_about(seeds[6], (EXPERTS, EXPERT_DIM, D), EXPERT_DIM ** -0.5, 0.25, ((0, 8), (2, 4)))
    shared_gate = scatter_about(seeds[7], (D, SHARED), D ** -0.5, 0.09375, ((0, 8), (1, 4)))
    shared_up = scatter_about(seeds[8], (D, SHARED), D ** -0.5, 0.09375, ((0, 8), (1, 4)))
    shared_down = scatter_about(seeds[9], (SHARED, D), SHARED ** -0.5, 0.25, ((1, 4),))
    return dict(tokens=tokens, norm_gain=norm_gain, expert_ids=expert_ids, expert_gates=expert_gates, gate_proj=gate_proj, up_proj=up_proj, down_proj=down_proj, shared_gate=shared_gate, shared_up=shared_up, shared_down=shared_down)


def reference(tokens, norm_gain, expert_ids, expert_gates, gate_proj, up_proj, down_proj, shared_gate, shared_up, shared_down):
    floats = tokens.astype(jnp.float32)
    scale = lax.rsqrt(lax.optimization_barrier(jnp.mean(floats * floats, axis=-1, keepdims=True)) + 1e-06)
    normed = (floats * scale * norm_gain[None, :]).astype(jnp.bfloat16)
    shared_g = jnp.dot(normed, shared_gate, preferred_element_type=jnp.float32)
    shared_u = jnp.dot(normed, shared_up, preferred_element_type=jnp.float32)
    shared_hidden = (jax.nn.silu(shared_g) * shared_u).astype(jnp.bfloat16)
    shared_out = jnp.dot(shared_hidden, shared_down, preferred_element_type=jnp.float32)
    ids = expert_ids.reshape(N_EP, TOK_DEV * TOP)
    onehot = (ids[:, :, None] == jnp.arange(EXPERTS, dtype=jnp.int32)[None, None, :]).astype(jnp.int32)
    slots = lax.optimization_barrier(jnp.sum((jnp.cumsum(onehot, axis=1) - onehot) * onehot, axis=-1)).astype(jnp.int32)
    dest = (ids * CAP + slots).astype(jnp.int32)
    local_tok = jnp.repeat(jnp.arange(TOK_DEV, dtype=jnp.int32), TOP)
    glob = local_tok[None, :] + jnp.arange(N_EP, dtype=jnp.int32)[:, None] * TOK_DEV
    blocks = jnp.broadcast_to(jnp.arange(N_EP, dtype=jnp.int32)[:, None], dest.shape)
    owner = jnp.full((N_EP, EXPERTS * CAP), TOKENS, jnp.int32).at[blocks, dest].set(glob)
    weight = jnp.zeros((N_EP, EXPERTS * CAP), jnp.float32).at[blocks, dest].set(expert_gates.reshape(N_EP, TOK_DEV * TOP))
    owner = owner.reshape(N_EP, EXPERTS, CAP).transpose(1, 0, 2).reshape(EXPERTS, N_EP * CAP)
    weight = weight.reshape(N_EP, EXPERTS, CAP).transpose(1, 0, 2).reshape(EXPERTS, N_EP * CAP)
    padded = jnp.concatenate([normed, jnp.zeros((1, D), jnp.bfloat16)], axis=0)

    def step(total, item):
        rows_idx, rows_weight, w_gate, w_up, w_down = item
        rows = padded[rows_idx]
        g = jnp.dot(rows, w_gate, preferred_element_type=jnp.float32)
        u = jnp.dot(rows, w_up, preferred_element_type=jnp.float32)
        hidden = (jax.nn.silu(g) * u).astype(jnp.bfloat16)
        result = jnp.dot(hidden, w_down, preferred_element_type=jnp.float32).astype(jnp.bfloat16)
        return (total.at[rows_idx].add(rows_weight[:, None] * result.astype(jnp.float32)), None)
    total = jnp.zeros((TOKENS + 1, D), jnp.float32)
    total, _ = lax.scan(step, total, (owner, weight, gate_proj, up_proj, down_proj))
    return (total[:TOKENS] + shared_out).astype(jnp.bfloat16)
```

```python
import functools

import jax
import jax.numpy as jnp
from jax import lax
from jax.experimental import pallas as pl
from jax.experimental.pallas import tpu as pltpu
from jax.sharding import PartitionSpec as P

MESH = pl.DeviceIdType.MESH


def shards_plain(
    tokens,
    norm_gain,
    expert_ids,
    expert_gates,
    gate_proj,
    up_proj,
    down_proj,
    shared_gate,
    shared_up,
    shared_down,
):
    n_ep = lax.axis_size("ep")
    n_tp = lax.axis_size("tp")
    whole = lax.all_gather(tokens, "tp", axis=1, tiled=True)
    tok_rows, width = whole.shape
    quarter = width // n_tp
    floats = whole.astype(jnp.float32)
    scale = lax.rsqrt(jnp.mean(floats * floats, axis=-1, keepdims=True) + 1e-06)
    normed = (floats * scale * norm_gain[None, :]).astype(jnp.bfloat16)
    gate_whole, up_whole = (
        lax.all_gather(shared_gate, "ep", axis=0, tiled=True),
        lax.all_gather(shared_up, "ep", axis=0, tiled=True),
    )
    shared_g = jnp.dot(normed, gate_whole, preferred_element_type=jnp.float32)
    shared_u = jnp.dot(normed, up_whole, preferred_element_type=jnp.float32)
    shared_hidden = (jax.nn.silu(shared_g) * shared_u).astype(jnp.bfloat16)
    rows = shared_down
    shared_out = jnp.dot(
        lax.all_gather(shared_hidden, "tp", axis=1, tiled=True),
        rows,
        preferred_element_type=jnp.float32,
    )
    exp_dev = gate_proj.shape[0]
    n_exp = exp_dev * n_ep
    top = expert_ids.shape[1]
    cap = 3 * tok_rows * top // (2 * n_exp)
    flat_ids = expert_ids.reshape(tok_rows * top)
    onehot = (flat_ids[:, None] == jnp.arange(n_exp, dtype=jnp.int32)[None, :]).astype(jnp.int32)
    slots = jnp.sum((jnp.cumsum(onehot, axis=0) - onehot) * onehot, axis=-1)
    dest = flat_ids * cap + slots
    local_tok = jnp.repeat(jnp.arange(tok_rows, dtype=jnp.int32), top)
    owner = jnp.full((n_exp * cap,), tok_rows, jnp.int32).at[dest].set(local_tok)
    padded = jnp.concatenate([normed, jnp.zeros((1, width), jnp.bfloat16)], axis=0)
    outgoing = padded[owner].reshape(n_ep, exp_dev, cap, width)
    received = lax.all_to_all(outgoing, "ep", split_axis=0, concat_axis=0, tiled=True)
    gate_vals = jnp.einsum(
        "secd,edh->sech", received, gate_proj, preferred_element_type=jnp.float32
    )
    up_vals = jnp.einsum("secd,edh->sech", received, up_proj, preferred_element_type=jnp.float32)
    expert_hidden = (jax.nn.silu(gate_vals) * up_vals).astype(jnp.bfloat16)
    rows = down_proj
    expert_out = jnp.einsum(
        "sech,ehd->secd",
        lax.all_gather(expert_hidden, "tp", axis=3, tiled=True),
        rows,
        preferred_element_type=jnp.float32,
    ).astype(jnp.bfloat16)
    returned = lax.all_to_all(expert_out, "ep", split_axis=0, concat_axis=0, tiled=True)
    picked = returned.reshape(n_exp * cap, quarter)[dest].reshape(tok_rows, top, quarter)
    routed = jnp.sum(expert_gates[:, :, None] * picked.astype(jnp.float32), axis=1)
    return (routed + shared_out).astype(jnp.bfloat16)


def fits(mesh):
    return mesh.shape["tp"] == 4 and mesh.shape["ep"] % 2 == 0 and mesh.shape["ep"] <= 16


def remote(src, dst, send, recv, ep, tp):
    return pltpu.make_async_remote_copy(
        src_ref=src, dst_ref=dst, send_sem=send, recv_sem=recv, device_id=(ep, tp), device_id_type=MESH
    )


def silu_mul(v, hid):
    g, u = v[:, :hid], v[:, hid:]
    return ((g / (1.0 + jnp.exp(-g))) * u).astype(jnp.bfloat16)


def kernel(
    n,
    tokens_hbm, gain_hbm, ids_hbm, gates_hbm, gate_w, up_w, down_w, sgate_w, sup_w, sdown_w,
    out,
    tokens, gain, ids, gates, wgu, wdn, sdn, pick, back, outbox, xs, own, hb, shb, ob, ret, sw, nown,
    load_sem, disp_s, disp_r, mate_s, mate_r, far_s, far_r, fwd_s, fwd_r,
    own_s, own_r, hid_s, hid_r, shid_s, shid_r, ret_s, ret_r, sw_s, sw_r, swx_s, swx_r,
):
    ep, tp = lax.axis_index("ep"), lax.axis_index("tp")
    nz = n // 2
    z, x = ep // 2, ep % 2
    ox = ep + 1 - 2 * x
    mate = tp + 1 - 2 * (tp % 2)
    far = (tp + 2) % 4
    diag = (mate + 2) % 4
    rows, quarter = tokens.shape
    cap = xs.shape[2]
    hid = gate_w.shape[2]
    slots = n * cap
    width = gain.shape[1]

    first = [
        pltpu.make_async_copy(ids_hbm, ids, load_sem.at[6]),
        pltpu.make_async_copy(tokens_hbm, tokens, load_sem.at[7]),
        pltpu.make_async_copy(gates_hbm, gates, load_sem.at[8]),
        pltpu.make_async_copy(gain_hbm, gain, load_sem.at[9]),
    ]
    for c in first:
        c.start()
    loads = [
        pltpu.make_async_copy(sgate_w, sw.at[ep, :, pl.ds(0, hid)], load_sem.at[0]),
        pltpu.make_async_copy(sup_w, sw.at[ep, :, pl.ds(hid, hid)], load_sem.at[1]),
        pltpu.make_async_copy(gate_w.at[0], wgu.at[:, pl.ds(0, hid)], load_sem.at[2]),
        pltpu.make_async_copy(up_w.at[0], wgu.at[:, pl.ds(hid, hid)], load_sem.at[3]),
        pltpu.make_async_copy(down_w.at[0], wdn, load_sem.at[4]),
        pltpu.make_async_copy(sdown_w, sdn, load_sem.at[5]),
    ]
    for c in loads:
        c.start()

    barrier = pltpu.get_barrier_semaphore()
    for d in range(1, n):
        pl.semaphore_signal(barrier, inc=1, device_id=((ep + d) % n, tp), device_id_type=MESH)
    for d in range(1, 4):
        pl.semaphore_signal(barrier, inc=1, device_id=(ep, (tp + d) % 4), device_id_type=MESH)

    def column(row):
        return jnp.broadcast_to(row.astype(jnp.float32), (rows, rows)).T

    lane = lax.broadcasted_iota(jnp.int32, (rows, 128), 1).astype(jnp.float32)
    first[0].wait()
    named0 = (lane == column(ids[0:1, :])).astype(jnp.float32)
    named1 = (lane == column(ids[1:2, :])).astype(jnp.float32)
    named = (named0 + named1).astype(jnp.bfloat16)
    before = (
        lax.broadcasted_iota(jnp.int32, (rows, rows), 1) < lax.broadcasted_iota(jnp.int32, (rows, rows), 0)
    ).astype(jnp.float32).astype(jnp.bfloat16)
    place = jnp.dot(before, named, preferred_element_type=jnp.float32).astype(jnp.bfloat16)
    low = lax.broadcasted_iota(jnp.int32, (128, slots), 0) * cap
    col = lax.broadcasted_iota(jnp.int32, (128, slots), 1)
    spread = ((col >= low) & (col < low + cap)).astype(jnp.float32).astype(jnp.bfloat16)
    place_x = jnp.dot(place, spread, preferred_element_type=jnp.float32)
    colf = lax.broadcasted_iota(jnp.int32, (rows, slots), 1).astype(jnp.float32)
    inner = colf - jnp.floor((colf + 0.5) / cap) * cap
    hit = jnp.abs(place_x - inner) < 0.5
    total = jnp.zeros((rows, slots), jnp.float32)
    for k, one in enumerate((named0, named1)):
        sel = jnp.where(
            hit, jnp.dot(one.astype(jnp.bfloat16), spread, preferred_element_type=jnp.float32), 0.0
        )
        back[k] = sel.astype(jnp.bfloat16)
        total = total + sel
    pick[...] = total.T.astype(jnp.bfloat16)
    first[1].wait()
    for e in range(n):
        outbox[e] = jnp.dot(
            pick[e * cap : (e + 1) * cap, :], tokens[...], preferred_element_type=jnp.float32
        ).astype(jnp.bfloat16)

    pl.semaphore_wait(barrier, n - 1 + 3)

    sends = []

    def go(c):
        c.start()
        sends.append(c)

    xs[tp, ep] = outbox[ep]

    def dispatch(e):
        go(remote(outbox.at[e], xs.at[tp, ep], disp_s.at[e], disp_r.at[ep], e, tp))

    for i in range(1, nz):
        for j in range(2):
            dispatch(((z + i) % nz) * 2 + (x + j) % 2)
        if i == 1:
            dispatch(ox)
            go(remote(tokens, own.at[tp], own_s.at[0], own_r.at[0], ep, mate))
            go(remote(tokens, own.at[tp], own_s.at[1], own_r.at[1], ep, far))
    if nz == 1:
        dispatch(ox)
        go(remote(tokens, own.at[tp], own_s.at[0], own_r.at[0], ep, mate))
        go(remote(tokens, own.at[tp], own_s.at[1], own_r.at[1], ep, far))
    own[tp] = tokens[...]

    loads[0].wait()
    loads[1].wait()

    def landed(dst, sem):
        return remote(dst, dst, sem, sem, ep, mate).wait_recv()

    def chain(k, way):
        s = ep - 2 * k * way
        f = (1 - way) // 2
        return remote(sw.at[s], sw.at[s], sw_s.at[f, k], sw_r.at[f, k + 1], ep + 2 * way, tp)

    def inside(zz):
        return (zz >= 0) & (zz < nz)

    def across(zz):
        s = zz * 2 + x
        return remote(sw.at[s], sw.at[s], swx_s.at[zz], swx_r.at[zz], ox, tp)

    def walk(k):
        if k == 0:
            across(z).start()
        for way in (1, -1):
            if k > 0:
                @pl.when(inside(z - k * way))
                def _():
                    s = ep - 2 * k * way
                    landed(sw.at[s], sw_r.at[(1 - way) // 2, k])
                    across(z - k * way).start()

            if k < nz - 1:
                @pl.when(inside(z - k * way) & inside(z + way))
                def _():
                    chain(k, way).start()

    def walked():
        for zz in range(nz):
            across(zz).wait_send()
        for k in range(nz - 1):
            for way in (1, -1):
                @pl.when(inside(z - k * way) & inside(z + way))
                def _():
                    chain(k, way).wait_send()

    walk(0)

    def pair(ref, k, i):
        zz = (z - i + nz) % nz
        return ref.at[k, pl.ds(zz * 2, 2)]

    def stage_a(i):
        zz = (z - i + nz) % nz
        for j in range(2):
            s = zz * 2 + j
            if i > 0:
                landed(xs.at[tp, s], disp_r.at[s])
        if i == 0:
            landed(xs.at[tp, ox], disp_r.at[ox])
        blk = pair(xs, tp, i)
        go(remote(blk, blk, far_s.at[i], far_r.at[i], ep, far))
        go(remote(blk, blk, mate_s.at[i], mate_r.at[i], ep, mate))

    def stage_b(i):
        blk = pair(xs, far, i)
        landed(blk, far_r.at[i])
        go(remote(blk, blk, fwd_s.at[i], fwd_r.at[i], ep, mate))

    def norm_scale(get, m):
        sq = jnp.zeros((m, 1), jnp.float32)
        for k in range(4):
            v = get(k).astype(jnp.float32)
            sq = sq + jnp.sum(v * v, axis=-1, keepdims=True)
        return lax.rsqrt(sq / width + 1e-06)

    def stage_c(i):
        landed(pair(xs, mate, i), mate_r.at[i])
        landed(pair(xs, diag, i), fwd_r.at[i])
        if i == 0:
            loads[2].wait()
            loads[3].wait()
            first[3].wait()
        zz = (z - i + nz) % nz

        def get(k):
            return xs[k, pl.ds(zz * 2, 2)].reshape(2 * cap, quarter)

        scale = norm_scale(get, 2 * cap)
        acc = jnp.zeros((2 * cap, 2 * hid), jnp.float32)
        for k in range(4):
            cols = slice(k * quarter, (k + 1) * quarter)
            nk = (get(k).astype(jnp.float32) * scale * gain[:, cols]).astype(jnp.bfloat16)
            acc = acc + jnp.dot(nk, wgu[cols, :], preferred_element_type=jnp.float32)
        at = pl.ds(pl.multiple_of(tp * hid, 128), hid)
        hb[pl.ds(zz * 2, 2), :, at] = silu_mul(acc, hid).reshape(2, cap, hid)
        for d in range(1, 4):
            blk = hb.at[pl.ds(zz * 2, 2), :, at]
            go(remote(blk, blk, hid_s.at[i, d], hid_r.at[i, d], ep, (tp + d) % 4))

    def stage_d(i):
        zz = (z - i + nz) % nz
        for d in range(1, 4):
            at = pl.ds(pl.multiple_of(((tp - d + 4) % 4) * hid, 128), hid)
            landed(hb.at[pl.ds(zz * 2, 2), :, at], hid_r.at[i, d])
        if i == 0:
            loads[4].wait()
        h = hb[pl.ds(zz * 2, 2)].reshape(2 * cap, 4 * hid)
        res = jnp.dot(h, wdn[...], preferred_element_type=jnp.float32).astype(jnp.bfloat16)
        ob[pl.ds(zz * 2, 2)] = res.reshape(2, cap, quarter)
        for j in range(2):
            s = zz * 2 + (x + j) % 2
            if i == 0 and j == 0:
                ret[ep] = ob[ep]
            else:
                go(remote(ob.at[s], ret.at[ep], ret_s.at[s], ret_r.at[ep], s, tp))

    def own_forward():
        landed(own.at[far], own_r.at[1])
        go(remote(own.at[far], own.at[far], own_s.at[2], own_r.at[2], ep, mate))

    depth = sw.shape[1]
    per = quarter // depth

    def own_normed():
        landed(own.at[mate], own_r.at[0])
        landed(own.at[diag], own_r.at[2])
        scale = norm_scale(lambda k: own[k], rows)
        for s in range(n):
            nown[s] = (
                own[s // per, :, (s % per) * depth : (s % per + 1) * depth].astype(jnp.float32)
                * scale
                * gain[:, s * depth : (s + 1) * depth]
            ).astype(jnp.bfloat16)

    for t in range(nz + 3):
        if t < nz:
            stage_a(t)
        if t == 1:
            own_forward()
        if 0 <= t - 1 < nz:
            stage_b(t - 1)
        if 0 <= t - 2 < nz:
            stage_c(t - 2)
        if t == nz - 1 and nz > 1:
            walk(1)
        if t == nz + 1 and nz > 2:
            walk(2)
        if 0 <= t - 3 < nz:
            stage_d(t - 3)

    own_normed()
    for k in range(3 if nz > 2 else nz, nz):
        walk(k)
    acc = jnp.zeros((rows, 2 * hid), jnp.float32)
    for i in range(nz):
        s = ((z - i + nz) % nz) * 2 + x
        acc = acc + jnp.dot(nown[s], sw[s], preferred_element_type=jnp.float32)
    for i in range(nz):
        zz = (z - i + nz) % nz
        s = zz * 2 + (1 - x)
        landed(sw.at[s], swx_r.at[zz])
        acc = acc + jnp.dot(nown[s], sw[s], preferred_element_type=jnp.float32)
    at = pl.ds(pl.multiple_of(tp * hid, 128), hid)
    shb[:, at] = silu_mul(acc, hid)
    for d in range(1, 4):
        go(remote(shb.at[:, at], shb.at[:, at], shid_s.at[d], shid_r.at[d], ep, (tp + d) % 4))
    for d in range(1, 4):
        frm = pl.ds(pl.multiple_of(((tp - d + 4) % 4) * hid, 128), hid)
        landed(shb.at[:, frm], shid_r.at[d])
    loads[5].wait()
    shared = jnp.dot(shb[...], sdn[...], preferred_element_type=jnp.float32)

    for d in range(1, n):
        s = (ep + d) % n
        landed(ret.at[s], ret_r.at[s])
    got = ret[...].reshape(slots, quarter)
    mixed = shared
    first[2].wait()
    for k in range(2):
        mixed = mixed + column(gates[k : k + 1, :])[:, 0:1] * jnp.dot(back[k], got, preferred_element_type=jnp.float32)
    out[...] = mixed.astype(jnp.bfloat16)
    for c in sends:
        c.wait_send()
    walked()


def shards(
    tokens, norm_gain, expert_ids, expert_gates, gate_proj, up_proj, down_proj,
    shared_gate, shared_up, shared_down, plain,
):
    n = lax.axis_size("ep")
    rows, quarter = tokens.shape
    top = expert_ids.shape[1]
    exp_dev = gate_proj.shape[0]
    cap = 3 * rows * top // (2 * exp_dev * n)
    hid = gate_proj.shape[2]
    ok = exp_dev == 1 and top == 2 and cap % 16 == 0 and hid % 128 == 0 and rows == 128
    ok = ok and shared_gate.shape[1] == hid and quarter % shared_gate.shape[0] == 0
    if plain or not ok:
        return shards_plain(
            tokens, norm_gain, expert_ids, expert_gates, gate_proj, up_proj, down_proj,
            shared_gate, shared_up, shared_down,
        )
    width = norm_gain.shape[0]
    bf = jnp.bfloat16
    nz = n // 2
    dma = pltpu.SemaphoreType.DMA
    vm = pl.BlockSpec(memory_space=pltpu.VMEM)
    hbm = pl.BlockSpec(memory_space=pltpu.HBM)
    return pl.pallas_call(
        functools.partial(kernel, n),
        out_shape=jax.ShapeDtypeStruct((rows, quarter), bf),
        in_specs=[hbm] * 10,
        out_specs=vm,
        scratch_shapes=[
            pltpu.VMEM(tokens.shape, bf),
            pltpu.VMEM((1, width), jnp.float32),
            pltpu.VMEM((top, rows), jnp.int32),
            pltpu.VMEM((top, rows), jnp.float32),
            pltpu.VMEM((width, 2 * hid), bf),
            pltpu.VMEM(down_proj.shape[1:], bf),
            pltpu.VMEM(shared_down.shape, bf),
            pltpu.VMEM((n * cap, rows), bf),
            pltpu.VMEM((2, rows, n * cap), bf),
            pltpu.VMEM((n, cap, quarter), bf),
            pltpu.VMEM((4, n, cap, quarter), bf),
            pltpu.VMEM((4, rows, quarter), bf),
            pltpu.VMEM((n, cap, 4 * hid), bf),
            pltpu.VMEM((rows, 4 * hid), bf),
            pltpu.VMEM((n, cap, quarter), bf),
            pltpu.VMEM((n, cap, quarter), bf),
            pltpu.VMEM((n, shared_gate.shape[0], 2 * hid), bf),
            pltpu.VMEM((n, rows, shared_gate.shape[0]), bf),
            dma((10,)),
            dma((n,)), dma((n,)),
            dma((nz,)), dma((nz,)),
            dma((nz,)), dma((nz,)),
            dma((nz,)), dma((nz,)),
            dma((3,)), dma((3,)),
            dma((nz, 4)), dma((nz, 4)),
            dma((4,)), dma((4,)),
            dma((n,)), dma((n,)),
            dma((2, nz)), dma((2, nz)),
            dma((nz,)), dma((nz,)),
        ],
        compiler_params=pltpu.CompilerParams(collective_id=0, has_side_effects=True, vmem_limit_bytes=67043328),
    )(tokens, norm_gain.reshape(1, width), expert_ids.T, expert_gates.T, gate_proj, up_proj, down_proj,
      shared_gate, shared_up, shared_down)


def solution(mesh):
    return jax.shard_map(
        functools.partial(shards, plain=not fits(mesh)),
        mesh=mesh,
        in_specs=(
            P("ep", "tp"),
            P(),
            P("ep", None),
            P("ep", None),
            P("ep", None, "tp"),
            P("ep", None, "tp"),
            P("ep", None, "tp"),
            P("ep", "tp"),
            P("ep", "tp"),
            P(None, "tp"),
        ),
        out_specs=P("ep", "tp"),
        check_vma=False,
    )
```

```python
import functools

import jax
import jax.numpy as jnp
from jax import lax
from jax.experimental import pallas as pl
from jax.experimental.pallas import tpu as pltpu
from jax.sharding import PartitionSpec as P

MESH = pl.DeviceIdType.MESH


def shards_plain(
    tokens,
    norm_gain,
    expert_ids,
    expert_gates,
    gate_proj,
    up_proj,
    down_proj,
    shared_gate,
    shared_up,
    shared_down,
):
    n_ep = lax.axis_size("ep")
    n_tp = lax.axis_size("tp")
    whole = lax.all_gather(tokens, "tp", axis=1, tiled=True)
    tok_rows, width = whole.shape
    quarter = width // n_tp
    floats = whole.astype(jnp.float32)
    scale = lax.rsqrt(jnp.mean(floats * floats, axis=-1, keepdims=True) + 1e-06)
    normed = (floats * scale * norm_gain[None, :]).astype(jnp.bfloat16)
    gate_whole, up_whole = (
        lax.all_gather(shared_gate, "ep", axis=0, tiled=True),
        lax.all_gather(shared_up, "ep", axis=0, tiled=True),
    )
    shared_g = jnp.dot(normed, gate_whole, preferred_element_type=jnp.float32)
    shared_u = jnp.dot(normed, up_whole, preferred_element_type=jnp.float32)
    shared_hidden = (jax.nn.silu(shared_g) * shared_u).astype(jnp.bfloat16)
    rows = shared_down
    shared_out = jnp.dot(
        lax.all_gather(shared_hidden, "tp", axis=1, tiled=True),
        rows,
        preferred_element_type=jnp.float32,
    )
    exp_dev = gate_proj.shape[0]
    n_exp = exp_dev * n_ep
    top = expert_ids.shape[1]
    cap = 3 * tok_rows * top // (2 * n_exp)
    flat_ids = expert_ids.reshape(tok_rows * top)
    onehot = (flat_ids[:, None] == jnp.arange(n_exp, dtype=jnp.int32)[None, :]).astype(jnp.int32)
    slots = jnp.sum((jnp.cumsum(onehot, axis=0) - onehot) * onehot, axis=-1)
    dest = flat_ids * cap + slots
    local_tok = jnp.repeat(jnp.arange(tok_rows, dtype=jnp.int32), top)
    owner = jnp.full((n_exp * cap,), tok_rows, jnp.int32).at[dest].set(local_tok)
    padded = jnp.concatenate([normed, jnp.zeros((1, width), jnp.bfloat16)], axis=0)
    outgoing = padded[owner].reshape(n_ep, exp_dev, cap, width)
    received = lax.all_to_all(outgoing, "ep", split_axis=0, concat_axis=0, tiled=True)
    gate_vals = jnp.einsum(
        "secd,edh->sech", received, gate_proj, preferred_element_type=jnp.float32
    )
    up_vals = jnp.einsum("secd,edh->sech", received, up_proj, preferred_element_type=jnp.float32)
    expert_hidden = (jax.nn.silu(gate_vals) * up_vals).astype(jnp.bfloat16)
    rows = down_proj
    expert_out = jnp.einsum(
        "sech,ehd->secd",
        lax.all_gather(expert_hidden, "tp", axis=3, tiled=True),
        rows,
        preferred_element_type=jnp.float32,
    ).astype(jnp.bfloat16)
    returned = lax.all_to_all(expert_out, "ep", split_axis=0, concat_axis=0, tiled=True)
    picked = returned.reshape(n_exp * cap, quarter)[dest].reshape(tok_rows, top, quarter)
    routed = jnp.sum(expert_gates[:, :, None] * picked.astype(jnp.float32), axis=1)
    return (routed + shared_out).astype(jnp.bfloat16)


def fits(mesh):
    return mesh.shape["tp"] == 4 and mesh.shape["ep"] == 8


def remote(src, dst, send, recv, ep, tp):
    return pltpu.make_async_remote_copy(
        src_ref=src, dst_ref=dst, send_sem=send, recv_sem=recv, device_id=(ep, tp), device_id_type=MESH
    )


def silu_mul(v, hid):
    g, u = v[:, :hid], v[:, hid:]
    return ((g / (1.0 + jnp.exp(-g))) * u).astype(jnp.bfloat16)


def kernel(
    n,
    tokens_hbm, gain_hbm, ids_hbm, gates_hbm, gate_w, up_w, down_w, sgate_w, sup_w, sdown_w,
    out,
    tokens, gain, ids, gates, wgu, wdn, sdn, pick, back, outbox, xs, tk, ssq, hb, shb, ob, ret, sw,
    acc, pin, mix,
    load_sem, disp_s, disp_r, mate_s, mate_r, far_s, far_r, fwd_s, fwd_r,
    tk_s, tk_r, ssq_s, ssq_r, hid_s, hid_r, shid_s, shid_r, ret_s, ret_r, sw_s, sw_r, part_s, part_r,
):
    ep, tp = lax.axis_index("ep"), lax.axis_index("tp")
    nz = n // 2
    z, x = ep // 2, ep % 2
    ox = ep + 1 - 2 * x
    mate = tp + 1 - 2 * (tp % 2)
    far = (tp + 2) % 4
    diag = (mate + 2) % 4
    rows, quarter = tokens.shape
    cap = xs.shape[2]
    hid = gate_w.shape[2]
    slots = n * cap
    width = gain.shape[1]
    depth = sgate_w.shape[0]

    side = 1 - 2 * (z // 2)
    inner = ((z + 1) // 2) % 2
    order = [z + side * (i - inner * (0, 0, 3, 1)[i]) for i in range(nz)]

    def load(src, dst, k):
        c = pltpu.make_async_copy(src, dst, load_sem.at[k])
        c.start()
        return c

    ids_in = load(ids_hbm, ids, 0)
    tokens_in = load(tokens_hbm, tokens, 1)
    gates_in = load(gates_hbm, gates, 2)
    gain_in = load(gain_hbm, gain, 3)
    shared_in = [
        load(sgate_w, sw.at[z, :, pl.ds(0, hid)], 4),
        load(sup_w, sw.at[z, :, pl.ds(hid, hid)], 5),
    ]
    expert_in = [
        load(gate_w.at[0], wgu.at[:, pl.ds(0, hid)], 6),
        load(up_w.at[0], wgu.at[:, pl.ds(hid, hid)], 7),
    ]
    down_in = load(down_w.at[0], wdn, 8)
    sdown_in = load(sdown_w, sdn, 9)

    barrier = pltpu.get_barrier_semaphore()
    for d in range(1, n):
        pl.semaphore_signal(barrier, inc=1, device_id=((ep + d) % n, tp), device_id_type=MESH)
    for d in range(1, 4):
        pl.semaphore_signal(barrier, inc=1, device_id=(ep, (tp + d) % 4), device_id_type=MESH)

    def column(row):
        return jnp.broadcast_to(row.astype(jnp.float32), (rows, rows)).T

    lane = lax.broadcasted_iota(jnp.int32, (rows, 128), 1).astype(jnp.float32)
    ids_in.wait()
    named0 = (lane == column(ids[0:1, :])).astype(jnp.float32)
    named1 = (lane == column(ids[1:2, :])).astype(jnp.float32)
    named = (named0 + named1).astype(jnp.bfloat16)
    before = (
        lax.broadcasted_iota(jnp.int32, (rows, rows), 1) < lax.broadcasted_iota(jnp.int32, (rows, rows), 0)
    ).astype(jnp.float32).astype(jnp.bfloat16)
    place = jnp.dot(before, named, preferred_element_type=jnp.float32).astype(jnp.bfloat16)
    low = lax.broadcasted_iota(jnp.int32, (128, slots), 0) * cap
    col = lax.broadcasted_iota(jnp.int32, (128, slots), 1)
    spread = ((col >= low) & (col < low + cap)).astype(jnp.float32).astype(jnp.bfloat16)
    place_x = jnp.dot(place, spread, preferred_element_type=jnp.float32)
    colf = lax.broadcasted_iota(jnp.int32, (rows, slots), 1).astype(jnp.float32)
    within = colf - jnp.floor((colf + 0.5) / cap) * cap
    hit = jnp.abs(place_x - within) < 0.5
    total = jnp.zeros((rows, slots), jnp.float32)
    for k, one in enumerate((named0, named1)):
        sel = jnp.where(
            hit, jnp.dot(one.astype(jnp.bfloat16), spread, preferred_element_type=jnp.float32), 0.0
        )
        for e in range(nz):
            back[k, e] = sel[:, 2 * e * cap : 2 * (e + 1) * cap].astype(jnp.bfloat16)
        total = total + sel
    pick[...] = total.T.astype(jnp.bfloat16)
    tokens_in.wait()
    for e in range(n):
        outbox[e] = jnp.dot(
            pick[e * cap : (e + 1) * cap, :], tokens[...], preferred_element_type=jnp.float32
        ).astype(jnp.bfloat16)
    own = tokens[...].astype(jnp.float32)
    sums = jnp.broadcast_to(jnp.sum(own * own, axis=-1, keepdims=True), (rows, 128)).T
    ssq[tp] = sums[0:8, :]

    pl.semaphore_wait(barrier, n - 1 + 3)

    sends = []

    def go(c):
        c.start()
        sends.append(c)

    def landed(dst, sem):
        remote(dst, dst, sem, sem, ep, mate).wait_recv()

    xs[tp, ep] = outbox[ep]

    def dispatch(e):
        go(remote(outbox.at[e], xs.at[tp, ep], disp_s.at[e], disp_r.at[ep], e, tp))

    dispatch(ox)
    for i in range(1, nz):
        for j in range(2):
            dispatch(order[i] * 2 + (x + j) % 2)

    mine = tokens.at[:, pl.ds(pl.multiple_of(x * depth, depth), depth)]
    theirs = tokens.at[:, pl.ds(pl.multiple_of((1 - x) * depth, depth), depth)]
    go(remote(mine, tk.at[tp, 0], tk_s.at[0], tk_r.at[0], ep, mate))
    go(remote(mine, tk.at[tp, 0], tk_s.at[1], tk_r.at[1], ep, far))
    go(remote(theirs, tk.at[tp, 1], tk_s.at[2], tk_r.at[2], ox, tp))
    for d in range(1, 4):
        go(remote(ssq.at[tp], ssq.at[tp], ssq_s.at[d], ssq_r.at[d], ep, (tp + d) % 4))
    tk[tp, 0] = mine[...]

    def other_tokens():
        landed(tk.at[tp, 1], tk_r.at[2])
        go(remote(tk.at[tp, 1], tk.at[tp, 1], tk_s.at[3], tk_r.at[3], ep, mate))
        go(remote(tk.at[tp, 1], tk.at[tp, 1], tk_s.at[4], tk_r.at[4], ep, far))

    def pass_tokens():
        landed(tk.at[far, 0], tk_r.at[1])
        landed(tk.at[far, 1], tk_r.at[4])
        go(remote(tk.at[far], tk.at[far], tk_s.at[5], tk_r.at[5], ep, mate))

    def have_tokens():
        landed(tk.at[mate, 0], tk_r.at[0])
        landed(tk.at[mate, 1], tk_r.at[3])
        landed(tk.at[diag], tk_r.at[5])

    def pair(ref, k, i):
        return ref.at[k, pl.ds(order[i] * 2, 2)]

    def stage_a(i):
        for j in range(2):
            s = order[i] * 2 + (x + j) % 2
            blk = xs.at[tp, s]
            if i > 0 or j > 0:
                landed(blk, disp_r.at[s])
            go(remote(blk, blk, far_s.at[i, j], far_r.at[i, j], ep, far))
            go(remote(blk, blk, mate_s.at[i, j], mate_r.at[i, j], ep, mate))

    def both(k, sem, i):
        for j in range(2):
            landed(xs.at[k, order[i] * 2 + (x + j) % 2], sem.at[i, j])

    def stage_b(i):
        both(far, far_r, i)
        blk = pair(xs, far, i)
        go(remote(blk, blk, fwd_s.at[i], fwd_r.at[i], ep, mate))

    def stage_c(i):
        both(mate, mate_r, i)
        landed(pair(xs, diag, i), fwd_r.at[i])
        if i == 0:
            expert_in[0].wait()
            expert_in[1].wait()
            gain_in.wait()
        zz = order[i]
        sq = jnp.zeros((2 * cap, 1), jnp.float32)
        for k in range(4):
            v = xs[k, pl.ds(zz * 2, 2)].reshape(2 * cap, quarter).astype(jnp.float32)
            sq = sq + jnp.sum(v * v, axis=-1, keepdims=True)
        scale = lax.rsqrt(sq / width + 1e-06)
        val = jnp.zeros((2 * cap, 2 * hid), jnp.float32)
        for k in range(4):
            cols = slice(k * quarter, (k + 1) * quarter)
            v = xs[k, pl.ds(zz * 2, 2)].reshape(2 * cap, quarter).astype(jnp.float32)
            nk = (v * scale * gain[:, cols]).astype(jnp.bfloat16)
            val = val + jnp.dot(nk, wgu[cols, :], preferred_element_type=jnp.float32)
        at = pl.ds(pl.multiple_of(tp * hid, 128), hid)
        hb[pl.ds(zz * 2, 2), :, at] = silu_mul(val, hid).reshape(2, cap, hid)
        for d in (2, 1, 3):
            blk = hb.at[pl.ds(zz * 2, 2), :, at]
            go(remote(blk, blk, hid_s.at[i, d], hid_r.at[i, d], ep, (tp + d) % 4))

    def stage_d(i):
        zz = order[i]
        for d in range(1, 4):
            at = pl.ds(pl.multiple_of(((tp - d + 4) % 4) * hid, 128), hid)
            landed(hb.at[pl.ds(zz * 2, 2), :, at], hid_r.at[i, d])
        if i == 0:
            down_in.wait()
        h = hb[pl.ds(zz * 2, 2)].reshape(2 * cap, 4 * hid)
        res = jnp.dot(h, wdn[...], preferred_element_type=jnp.float32).astype(jnp.bfloat16)
        ob[pl.ds(zz * 2, 2)] = res.reshape(2, cap, quarter)
        for j in range(2):
            s = zz * 2 + (x + j) % 2
            if i == 0 and j == 0:
                ret[ep] = ob[ep]
            else:
                go(remote(ob.at[s], ret.at[ep], ret_s.at[s], ret_r.at[ep], s, tp))

    def rows_of(i, way, k):
        blk = sw.at[order[i]]
        return remote(blk, blk, sw_s.at[k], sw_r.at[order[i]], ep + 2 * way * side, tp)

    chain = [(0, 1, 0), (0, -1, 1), (1, -1, 2), (2, 1, 3), (3, -1, 4)]

    def rows_start(i):
        if i == 0:
            for c in shared_in:
                c.wait()
            rows_of(*chain[0]).start()

            @pl.when(inner == 1)
            def _():
                rows_of(*chain[1]).start()
        else:
            landed(sw.at[order[i]], sw_r.at[order[i]])

            @pl.when(inner == 1)
            def _():
                rows_of(*chain[i + 1]).start()

    def rows_end():
        rows_of(*chain[0]).wait_send()

        @pl.when(inner == 1)
        def _():
            for c in chain[1:]:
                rows_of(*c).wait_send()

    def shared_add(i):
        zz = order[i]
        cols = pl.ds(pl.multiple_of((2 * zz + x) * depth, depth), depth)
        v = (tk[zz].reshape(2 * rows, depth).astype(jnp.float32) * gain[:, cols]).astype(jnp.bfloat16)
        part = jnp.dot(v, sw[zz], preferred_element_type=jnp.float32)
        acc[...] = part if i == 0 else acc[...] + part

    def combine(i):
        zz = order[i]
        for j in range(2):
            s = zz * 2 + (x + j) % 2
            if i > 0 or j > 0:
                landed(ret.at[s], ret_r.at[s])
        got = ret[pl.ds(zz * 2, 2)].reshape(2 * cap, quarter)
        for k in range(2):
            mix[...] += column(gates[k : k + 1, :])[:, 0:1] * jnp.dot(
                back[k, zz], got, preferred_element_type=jnp.float32
            )

    stage_a(0)
    stage_a(1)
    stage_b(0)
    other_tokens()
    stage_c(0)
    stage_b(1)
    stage_a(2)
    rows_start(0)
    stage_d(0)
    stage_c(1)
    stage_d(1)
    stage_b(2)
    stage_a(3)
    pass_tokens()
    stage_c(2)
    rows_start(1)
    stage_b(3)
    stage_d(2)
    stage_c(3)
    stage_d(3)
    have_tokens()
    shared_add(0)
    shared_add(1)
    rows_start(2)
    shared_add(2)
    rows_start(3)
    shared_add(3)
    go(remote(acc.at[pl.ds(rows, rows)], pin, part_s, part_r, ox, tp))
    square = ssq[tp]
    for d in range(1, 4):
        frm = (tp - d + 4) % 4
        landed(ssq.at[frm], ssq_r.at[d])
        square = square + ssq[frm]
    scale = column(lax.rsqrt(square[0:1, :] / width + 1e-06))[:, 0:1]
    mix[...] = jnp.zeros((rows, quarter), jnp.float32)
    gates_in.wait()
    combine(0)
    landed(pin, part_r)
    at = pl.ds(pl.multiple_of(tp * hid, 128), hid)
    shb[:, at] = silu_mul((acc[0:rows, :] + pin[...]) * scale, hid)
    for d in (2, 1, 3):
        go(remote(shb.at[:, at], shb.at[:, at], shid_s.at[d], shid_r.at[d], ep, (tp + d) % 4))
    combine(1)
    combine(2)
    for d in range(1, 4):
        frm = pl.ds(pl.multiple_of(((tp - d + 4) % 4) * hid, 128), hid)
        landed(shb.at[:, frm], shid_r.at[d])
    sdown_in.wait()
    mix[...] += jnp.dot(shb[...], sdn[...], preferred_element_type=jnp.float32)
    combine(3)
    out[...] = mix[...].astype(jnp.bfloat16)
    for c in sends:
        c.wait_send()
    rows_end()


def shards(
    tokens, norm_gain, expert_ids, expert_gates, gate_proj, up_proj, down_proj,
    shared_gate, shared_up, shared_down, plain,
):
    n = lax.axis_size("ep")
    rows, quarter = tokens.shape
    top = expert_ids.shape[1]
    exp_dev = gate_proj.shape[0]
    cap = 3 * rows * top // (2 * exp_dev * n)
    hid = gate_proj.shape[2]
    depth = shared_gate.shape[0]
    ok = exp_dev == 1 and top == 2 and cap % 16 == 0 and hid % 128 == 0 and rows == 128
    ok = ok and shared_gate.shape[1] == hid and quarter == 2 * depth and depth % 128 == 0
    if plain or not ok:
        return shards_plain(
            tokens, norm_gain, expert_ids, expert_gates, gate_proj, up_proj, down_proj,
            shared_gate, shared_up, shared_down,
        )
    width = norm_gain.shape[0]
    bf = jnp.bfloat16
    nz = n // 2
    dma = pltpu.SemaphoreType.DMA
    vm = pl.BlockSpec(memory_space=pltpu.VMEM)
    hbm = pl.BlockSpec(memory_space=pltpu.HBM)
    return pl.pallas_call(
        functools.partial(kernel, n),
        out_shape=jax.ShapeDtypeStruct((rows, quarter), bf),
        in_specs=[hbm] * 10,
        out_specs=vm,
        scratch_shapes=[
            pltpu.VMEM(tokens.shape, bf),
            pltpu.VMEM((1, width), jnp.float32),
            pltpu.VMEM((top, rows), jnp.int32),
            pltpu.VMEM((top, rows), jnp.float32),
            pltpu.VMEM((width, 2 * hid), bf),
            pltpu.VMEM(down_proj.shape[1:], bf),
            pltpu.VMEM(shared_down.shape, bf),
            pltpu.VMEM((n * cap, rows), bf),
            pltpu.VMEM((top, nz, rows, 2 * cap), bf),
            pltpu.VMEM((n, cap, quarter), bf),
            pltpu.VMEM((4, n, cap, quarter), bf),
            pltpu.VMEM((4, 2, rows, depth), bf),
            pltpu.VMEM((4, 8, rows), jnp.float32),
            pltpu.VMEM((n, cap, 4 * hid), bf),
            pltpu.VMEM((rows, 4 * hid), bf),
            pltpu.VMEM((n, cap, quarter), bf),
            pltpu.VMEM((n, cap, quarter), bf),
            pltpu.VMEM((nz, depth, 2 * hid), bf),
            pltpu.VMEM((2 * rows, 2 * hid), jnp.float32),
            pltpu.VMEM((rows, 2 * hid), jnp.float32),
            pltpu.VMEM((rows, quarter), jnp.float32),
            dma((10,)),
            dma((n,)), dma((n,)),
            dma((nz, 2)), dma((nz, 2)),
            dma((nz, 2)), dma((nz, 2)),
            dma((nz,)), dma((nz,)),
            dma((6,)), dma((6,)),
            dma((4,)), dma((4,)),
            dma((nz, 4)), dma((nz, 4)),
            dma((4,)), dma((4,)),
            dma((n,)), dma((n,)),
            dma((5,)), dma((nz,)),
            dma, dma,
        ],
        compiler_params=pltpu.CompilerParams(
            collective_id=0, has_side_effects=True, vmem_limit_bytes=67043328
        ),
    )(tokens, norm_gain.reshape(1, width), expert_ids.T, expert_gates.T, gate_proj, up_proj, down_proj,
      shared_gate, shared_up, shared_down)


def solution(mesh):
    return jax.shard_map(
        functools.partial(shards, plain=not fits(mesh)),
        mesh=mesh,
        in_specs=(
            P("ep", "tp"),
            P(),
            P("ep", None),
            P("ep", None),
            P("ep", None, "tp"),
            P("ep", None, "tp"),
            P("ep", None, "tp"),
            P("ep", "tp"),
            P("ep", "tp"),
            P(None, "tp"),
        ),
        out_specs=P("ep", "tp"),
        check_vma=False,
    )
```

```python
import functools

import jax
import jax.numpy as jnp
from jax import lax
from jax.experimental import pallas as pl
from jax.experimental.pallas import tpu as pltpu
from jax.sharding import PartitionSpec as P

MESH = pl.DeviceIdType.MESH


def shards_plain(
    tokens,
    norm_gain,
    expert_ids,
    expert_gates,
    gate_proj,
    up_proj,
    down_proj,
    shared_gate,
    shared_up,
    shared_down,
):
    n_ep = lax.axis_size("ep")
    n_tp = lax.axis_size("tp")
    whole = lax.all_gather(tokens, "tp", axis=1, tiled=True)
    tok_rows, width = whole.shape
    quarter = width // n_tp
    floats = whole.astype(jnp.float32)
    scale = lax.rsqrt(jnp.mean(floats * floats, axis=-1, keepdims=True) + 1e-06)
    normed = (floats * scale * norm_gain[None, :]).astype(jnp.bfloat16)
    gate_whole, up_whole = (
        lax.all_gather(shared_gate, "ep", axis=0, tiled=True),
        lax.all_gather(shared_up, "ep", axis=0, tiled=True),
    )
    shared_g = jnp.dot(normed, gate_whole, preferred_element_type=jnp.float32)
    shared_u = jnp.dot(normed, up_whole, preferred_element_type=jnp.float32)
    shared_hidden = (jax.nn.silu(shared_g) * shared_u).astype(jnp.bfloat16)
    rows = shared_down
    shared_out = jnp.dot(
        lax.all_gather(shared_hidden, "tp", axis=1, tiled=True),
        rows,
        preferred_element_type=jnp.float32,
    )
    exp_dev = gate_proj.shape[0]
    n_exp = exp_dev * n_ep
    top = expert_ids.shape[1]
    cap = 3 * tok_rows * top // (2 * n_exp)
    flat_ids = expert_ids.reshape(tok_rows * top)
    onehot = (flat_ids[:, None] == jnp.arange(n_exp, dtype=jnp.int32)[None, :]).astype(jnp.int32)
    slots = jnp.sum((jnp.cumsum(onehot, axis=0) - onehot) * onehot, axis=-1)
    dest = flat_ids * cap + slots
    local_tok = jnp.repeat(jnp.arange(tok_rows, dtype=jnp.int32), top)
    owner = jnp.full((n_exp * cap,), tok_rows, jnp.int32).at[dest].set(local_tok)
    padded = jnp.concatenate([normed, jnp.zeros((1, width), jnp.bfloat16)], axis=0)
    outgoing = padded[owner].reshape(n_ep, exp_dev, cap, width)
    received = lax.all_to_all(outgoing, "ep", split_axis=0, concat_axis=0, tiled=True)
    gate_vals = jnp.einsum(
        "secd,edh->sech", received, gate_proj, preferred_element_type=jnp.float32
    )
    up_vals = jnp.einsum("secd,edh->sech", received, up_proj, preferred_element_type=jnp.float32)
    expert_hidden = (jax.nn.silu(gate_vals) * up_vals).astype(jnp.bfloat16)
    rows = down_proj
    expert_out = jnp.einsum(
        "sech,ehd->secd",
        lax.all_gather(expert_hidden, "tp", axis=3, tiled=True),
        rows,
        preferred_element_type=jnp.float32,
    ).astype(jnp.bfloat16)
    returned = lax.all_to_all(expert_out, "ep", split_axis=0, concat_axis=0, tiled=True)
    picked = returned.reshape(n_exp * cap, quarter)[dest].reshape(tok_rows, top, quarter)
    routed = jnp.sum(expert_gates[:, :, None] * picked.astype(jnp.float32), axis=1)
    return (routed + shared_out).astype(jnp.bfloat16)


def fits(mesh):
    return mesh.shape["tp"] == 4 and mesh.shape["ep"] == 8


def remote(src, dst, send, recv, ep, tp):
    return pltpu.make_async_remote_copy(
        src_ref=src, dst_ref=dst, send_sem=send, recv_sem=recv, device_id=(ep, tp), device_id_type=MESH
    )


def silu_mul(v, hid):
    g, u = v[:, :hid], v[:, hid:]
    return ((g / (1.0 + jnp.exp(-g))) * u).astype(jnp.bfloat16)


def kernel(
    n,
    tokens_hbm, gain_hbm, ids_hbm, gates_hbm, gate_w, up_w, down_w, sgate_w, sup_w, sdown_w,
    out,
    tokens, gain, ids, gates, wgu, wdn, sdn, pick, back, outbox, xs, tk, ssq, hb, shb, ob, ret, sw,
    acc, pout, pin, she, mix,
    load_sem, disp_s, disp_r, mate_s, mate_r, far_s, far_r, fwd_s, fwd_r,
    tk_s, tk_r, ssq_s, ssq_r, hid_s, hid_r, shid_s, shid_r, ret_s, ret_r, sw_s, sw_r, part_s, part_r,
):
    ep, tp = lax.axis_index("ep"), lax.axis_index("tp")
    nz = n // 2
    z, x = ep // 2, ep % 2
    ox = ep + 1 - 2 * x
    mate = tp + 1 - 2 * (tp % 2)
    far = (tp + 2) % 4
    diag = (mate + 2) % 4
    rows, quarter = tokens.shape
    cap = xs.shape[2]
    hid = gate_w.shape[2]
    slots = n * cap
    width = gain.shape[1]
    depth = sgate_w.shape[0]

    side = 1 - 2 * (z // 2)
    inner = ((z + 1) // 2) % 2
    half = ep + 2 * side * (1 - 2 * inner)
    order = [z + side * (i - inner * (0, 2, 0, 2)[i]) for i in range(nz)]

    def load(src, dst, k):
        c = pltpu.make_async_copy(src, dst, load_sem.at[k])
        c.start()
        return c

    ids_in = load(ids_hbm, ids, 0)
    tokens_in = load(tokens_hbm, tokens, 1)
    gates_in = load(gates_hbm, gates, 2)
    gain_in = load(gain_hbm, gain, 3)
    shared_in = [
        load(sgate_w, sw.at[z, :, pl.ds(0, hid)], 4),
        load(sup_w, sw.at[z, :, pl.ds(hid, hid)], 5),
    ]
    expert_in = [
        load(gate_w.at[0], wgu.at[:, pl.ds(0, hid)], 6),
        load(up_w.at[0], wgu.at[:, pl.ds(hid, hid)], 7),
    ]
    down_in = load(down_w.at[0], wdn, 8)
    sdown_in = load(sdown_w, sdn, 9)

    barrier = pltpu.get_barrier_semaphore()
    for d in range(1, n):
        pl.semaphore_signal(barrier, inc=1, device_id=((ep + d) % n, tp), device_id_type=MESH)
    for d in range(1, 4):
        pl.semaphore_signal(barrier, inc=1, device_id=(ep, (tp + d) % 4), device_id_type=MESH)
        pl.semaphore_signal(barrier, inc=1, device_id=(half, (tp + d) % 4), device_id_type=MESH)

    def column(row):
        return jnp.broadcast_to(row.astype(jnp.float32), (rows, rows)).T

    lane = lax.broadcasted_iota(jnp.int32, (rows, 128), 1).astype(jnp.float32)
    ids_in.wait()
    named0 = (lane == column(ids[0:1, :])).astype(jnp.float32)
    named1 = (lane == column(ids[1:2, :])).astype(jnp.float32)
    named = (named0 + named1).astype(jnp.bfloat16)
    before = (
        lax.broadcasted_iota(jnp.int32, (rows, rows), 1) < lax.broadcasted_iota(jnp.int32, (rows, rows), 0)
    ).astype(jnp.float32).astype(jnp.bfloat16)
    place = jnp.dot(before, named, preferred_element_type=jnp.float32).astype(jnp.bfloat16)
    low = lax.broadcasted_iota(jnp.int32, (128, slots), 0) * cap
    col = lax.broadcasted_iota(jnp.int32, (128, slots), 1)
    spread = ((col >= low) & (col < low + cap)).astype(jnp.float32).astype(jnp.bfloat16)
    place_x = jnp.dot(place, spread, preferred_element_type=jnp.float32)
    colf = lax.broadcasted_iota(jnp.int32, (rows, slots), 1).astype(jnp.float32)
    within = colf - jnp.floor((colf + 0.5) / cap) * cap
    hit = jnp.abs(place_x - within) < 0.5
    total = jnp.zeros((rows, slots), jnp.float32)
    for k, one in enumerate((named0, named1)):
        sel = jnp.where(
            hit, jnp.dot(one.astype(jnp.bfloat16), spread, preferred_element_type=jnp.float32), 0.0
        )
        for e in range(nz):
            back[k, e] = sel[:, 2 * e * cap : 2 * (e + 1) * cap].astype(jnp.bfloat16)
        total = total + sel
    pick[...] = total.T.astype(jnp.bfloat16)
    tokens_in.wait()
    for e in range(n):
        outbox[e] = jnp.dot(
            pick[e * cap : (e + 1) * cap, :], tokens[...], preferred_element_type=jnp.float32
        ).astype(jnp.bfloat16)
    own = tokens[...].astype(jnp.float32)
    sums = jnp.broadcast_to(jnp.sum(own * own, axis=-1, keepdims=True), (rows, 128)).T
    ssq[1 - inner, tp] = sums[0:8, :]

    pl.semaphore_wait(barrier, n - 1 + 6)

    sends = []

    def go(c):
        c.start()
        sends.append(c)

    def landed(dst, sem):
        remote(dst, dst, sem, sem, ep, mate).wait_recv()

    xs[tp, ep] = outbox[ep]

    def dispatch(e):
        go(remote(outbox.at[e], xs.at[tp, ep], disp_s.at[e], disp_r.at[ep], e, tp))

    def spread_block(i, j):
        s = order[i] * 2 + (x + j) % 2
        blk = xs.at[tp, s]
        go(remote(blk, blk, far_s.at[i, j], far_r.at[i, j], ep, far))
        go(remote(blk, blk, mate_s.at[i, j], mate_r.at[i, j], ep, mate))

    def rows_of(i):
        blk = sw.at[order[i]]
        return remote(blk, blk, sw_s.at[i], sw_r.at[order[i]], ep + 2 * side, tp)

    def at_inner(f):
        pl.when(inner == 1)(f)

    def at_edge(f):
        pl.when(inner == 0)(f)

    spread_block(0, 0)
    dispatch(ox)
    for i in range(1, nz):
        for j in range(2):
            dispatch(order[i] * 2 + (x + j) % 2)
    for c in shared_in:
        c.wait()
    at_edge(lambda: rows_of(0).start())

    mine = tokens.at[:, pl.ds(pl.multiple_of(x * depth, depth), depth)]
    theirs = tokens.at[:, pl.ds(pl.multiple_of((1 - x) * depth, depth), depth)]
    home = ep + 2 * side * (1 - inner)
    home_ox = ox + 2 * side * (1 - inner)
    edge = ep - 2 * side
    plane = 1 - inner

    def own_tokens():
        return remote(mine, tk.at[1, tp, 0], tk_s.at[0, 0], tk_r.at[1, 0], home, tp)

    go(remote(theirs, tk.at[plane, tp, 1], tk_s.at[0, 1], tk_r.at[plane, 1], home_ox, tp))
    at_edge(lambda: own_tokens().start())
    for d in range(1, 4):
        go(remote(ssq.at[plane, tp], ssq.at[plane, tp], ssq_s.at[d], ssq_r.at[plane, tp], home, (tp + d) % 4))

    def own_square():
        return remote(ssq.at[1, tp], ssq.at[1, tp], ssq_s.at[0], ssq_r.at[1, tp], home, tp)

    at_edge(lambda: own_square().start())

    def first_tokens(who, k):
        return remote(mine, tk.at[0, tp, 0], tk_s.at[0, k], tk_r.at[0, k], ep, who)

    @pl.when(inner == 1)
    def _():
        first_tokens(far, 2).start()
        first_tokens(mate, 3).start()
        tk[0, tp, 0] = mine[...]

    def pair(ref, k, i):
        return ref.at[k, pl.ds(order[i] * 2, 2)]

    def stage_a(i):
        for j in range(2):
            s = order[i] * 2 + (x + j) % 2
            if i > 0 or j > 0:
                landed(xs.at[tp, s], disp_r.at[s])
                spread_block(i, j)

    def both(k, sem, i):
        for j in range(2):
            landed(xs.at[k, order[i] * 2 + (x + j) % 2], sem.at[i, j])

    def stage_b(i):
        both(far, far_r, i)
        blk = pair(xs, far, i)
        go(remote(blk, blk, fwd_s.at[i], fwd_r.at[i], ep, mate))

    def stage_c(i):
        both(mate, mate_r, i)
        landed(pair(xs, diag, i), fwd_r.at[i])
        if i == 0:
            expert_in[0].wait()
            expert_in[1].wait()
            gain_in.wait()
        zz = order[i]
        sq = jnp.zeros((2 * cap, 1), jnp.float32)
        for k in range(4):
            v = xs[k, pl.ds(zz * 2, 2)].reshape(2 * cap, quarter).astype(jnp.float32)
            sq = sq + jnp.sum(v * v, axis=-1, keepdims=True)
        scale = lax.rsqrt(sq / width + 1e-06)
        val = jnp.zeros((2 * cap, 2 * hid), jnp.float32)
        for k in range(4):
            cols = slice(k * quarter, (k + 1) * quarter)
            v = xs[k, pl.ds(zz * 2, 2)].reshape(2 * cap, quarter).astype(jnp.float32)
            nk = (v * scale * gain[:, cols]).astype(jnp.bfloat16)
            val = val + jnp.dot(nk, wgu[cols, :], preferred_element_type=jnp.float32)
        at = pl.ds(pl.multiple_of(tp * hid, 128), hid)
        hb[pl.ds(zz * 2, 2), :, at] = silu_mul(val, hid).reshape(2, cap, hid)
        for d in (2, 1, 3):
            blk = hb.at[pl.ds(zz * 2, 2), :, at]
            go(remote(blk, blk, hid_s.at[i, d], hid_r.at[i, d], ep, (tp + d) % 4))

    def stage_d(i):
        zz = order[i]
        for d in range(1, 4):
            at = pl.ds(pl.multiple_of(((tp - d + 4) % 4) * hid, 128), hid)
            landed(hb.at[pl.ds(zz * 2, 2), :, at], hid_r.at[i, d])
        if i == 0:
            down_in.wait()
        h = hb[pl.ds(zz * 2, 2)].reshape(2 * cap, 4 * hid)
        res = jnp.dot(h, wdn[...], preferred_element_type=jnp.float32).astype(jnp.bfloat16)
        ob[pl.ds(zz * 2, 2)] = res.reshape(2, cap, quarter)

    def back_to(i, j):
        s = order[i] * 2 + (x + j) % 2
        return remote(ob.at[s], ret.at[ep], ret_s.at[s], ret_r.at[ep], s, tp)

    backs = [[back_to(i, j) for j in range(i == 0, 2)] for i in range(nz)]

    def send_back(i):
        if i == 0:
            ret[ep] = ob[ep]
        for c in backs[i]:
            c.start()

    def rows_pass():
        @pl.when(inner == 1)
        def _():
            landed(sw.at[order[1]], sw_r.at[order[1]])
            rows_of(1).start()

    def tokens_to(p, who, k):
        blk = tk.at[1, tp] if p == 1 else tk.at[0, tp, 1]
        return remote(blk, blk, tk_s.at[p, k], tk_r.at[p, k], ep, who)

    def tokens_on(p):
        return remote(tk.at[p, far], tk.at[p, far], tk_s.at[p, 4], tk_r.at[p, 4], ep, mate)

    def spread_tokens(p):
        if p == 1:
            landed(tk.at[1, tp, 0], tk_r.at[1, 0])
        landed(tk.at[p, tp, 1], tk_r.at[p, 1])
        tokens_to(p, far, 5).start()
        tokens_to(p, mate, 6).start()

    def pass_tokens(p):
        if p == 0:
            landed(tk.at[0, far, 0], tk_r.at[0, 2])
            landed(tk.at[0, far, 1], tk_r.at[0, 5])
        else:
            landed(tk.at[1, far], tk_r.at[1, 5])
        tokens_on(p).start()

    def partial(p):
        return remote(pout.at[p], pin.at[p], part_s.at[p], part_r.at[p], ox, tp)

    def shared_sum(p):
        if p == 0:
            landed(tk.at[0, mate, 0], tk_r.at[0, 3])
            landed(tk.at[0, mate, 1], tk_r.at[0, 6])
        else:
            landed(tk.at[1, mate], tk_r.at[1, 6])
        landed(tk.at[p, diag], tk_r.at[p, 4])
        val = jnp.zeros((2 * rows, 2 * hid), jnp.float32)
        for i in (0, 1, 3, 2):
            zz = order[i]
            if p == 1 and i in (2, 3):
                landed(sw.at[zz], sw_r.at[zz])
            cols = pl.ds(pl.multiple_of((2 * zz + x) * depth, depth), depth)
            v = (tk[p, zz].reshape(2 * rows, depth).astype(jnp.float32) * gain[:, cols]).astype(jnp.bfloat16)
            val = val + jnp.dot(v, sw[zz], preferred_element_type=jnp.float32)
        acc[p] = val[0:rows, :]
        pout[p] = val[rows:, :].astype(jnp.bfloat16)
        partial(p).start()

    at = pl.ds(pl.multiple_of(tp * hid, 128), hid)

    def hidden_to(p, d):
        frm = shb.at[:, at] if p == 0 else she
        return remote(frm, shb.at[:, at], shid_s.at[p, d], shid_r.at[tp], ep if p == 0 else edge, (tp + d) % 4)

    def shared_hidden(p):
        square = jnp.zeros((8, rows), jnp.float32)
        for k in range(4):
            square = square + ssq[p, k]
        scale = column(lax.rsqrt(square[0:1, :] / width + 1e-06))[:, 0:1]
        landed(pin.at[p], part_r.at[p])
        val = silu_mul((acc[p] + pin[p].astype(jnp.float32)) * scale, hid)
        if p == 0:
            shb[:, at] = val
        else:
            she[...] = val
        for d in (2, 3, 1, 0):
            if p == 1 or d > 0:
                hidden_to(p, d).start()

    def shared_inner():
        @pl.when(inner == 1)
        def _():
            pass_tokens(1)
            for d in range(1, 4):
                landed(ssq.at[0, (tp + d) % 4], ssq_r.at[0, (tp + d) % 4])
            for k in range(4):
                landed(ssq.at[1, k], ssq_r.at[1, k])
            shared_sum(1)
            shared_sum(0)
            shared_hidden(1)
            shared_hidden(0)

    def shared_end():
        for d in range(1, 4):
            frm = (tp + d) % 4
            landed(shb.at[:, pl.ds(pl.multiple_of(frm * hid, 128), hid)], shid_r.at[frm])

        @pl.when(inner == 0)
        def _():
            landed(shb.at[:, at], shid_r.at[tp])

    def shared_drain():
        rows_of(0).wait_send()

        @pl.when(inner == 0)
        def _():
            own_tokens().wait_send()
            own_square().wait_send()

        @pl.when(inner == 1)
        def _():
            rows_of(1).wait_send()
            first_tokens(far, 2).wait_send()
            first_tokens(mate, 3).wait_send()
            for p in range(2):
                tokens_to(p, far, 5).wait_send()
                tokens_to(p, mate, 6).wait_send()
                tokens_on(p).wait_send()
                partial(p).wait_send()
                for d in range(4):
                    if p == 1 or d > 0:
                        hidden_to(p, d).wait_send()

    def combine(i):
        zz = order[i]
        for j in range(2):
            s = zz * 2 + (x + j) % 2
            if i > 0 or j > 0:
                landed(ret.at[s], ret_r.at[s])
        got = ret[pl.ds(zz * 2, 2)].reshape(2 * cap, quarter)
        for k in range(2):
            mix[...] += column(gates[k : k + 1, :])[:, 0:1] * jnp.dot(
                back[k, zz], got, preferred_element_type=jnp.float32
            )

    stage_a(0)
    stage_a(1)
    stage_b(0)
    stage_c(0)
    stage_b(1)
    stage_a(2)
    stage_c(1)
    at_inner(lambda: rows_of(0).start())
    stage_d(0)
    send_back(0)
    stage_b(2)
    stage_a(3)
    stage_d(1)
    send_back(1)
    rows_pass()
    stage_c(2)
    at_inner(lambda: spread_tokens(0))
    stage_b(3)
    stage_d(2)
    send_back(2)
    stage_c(3)
    at_inner(lambda: spread_tokens(1))
    at_inner(lambda: pass_tokens(0))
    stage_d(3)
    send_back(3)
    mix[...] = jnp.zeros((rows, quarter), jnp.float32)
    gates_in.wait()
    shared_inner()
    combine(0)
    combine(1)
    combine(2)
    shared_end()
    sdown_in.wait()
    mix[...] += jnp.dot(shb[...], sdn[...], preferred_element_type=jnp.float32)
    combine(3)
    out[...] = mix[...].astype(jnp.bfloat16)
    for c in sends + sum(backs, []):
        c.wait_send()
    shared_drain()


def shards(
    tokens, norm_gain, expert_ids, expert_gates, gate_proj, up_proj, down_proj,
    shared_gate, shared_up, shared_down, plain,
):
    n = lax.axis_size("ep")
    rows, quarter = tokens.shape
    top = expert_ids.shape[1]
    exp_dev = gate_proj.shape[0]
    cap = 3 * rows * top // (2 * exp_dev * n)
    hid = gate_proj.shape[2]
    depth = shared_gate.shape[0]
    ok = exp_dev == 1 and top == 2 and cap % 16 == 0 and hid % 128 == 0 and rows == 128
    ok = ok and shared_gate.shape[1] == hid and quarter == 2 * depth and depth % 128 == 0
    if plain or not ok:
        return shards_plain(
            tokens, norm_gain, expert_ids, expert_gates, gate_proj, up_proj, down_proj,
            shared_gate, shared_up, shared_down,
        )
    width = norm_gain.shape[0]
    bf = jnp.bfloat16
    nz = n // 2
    dma = pltpu.SemaphoreType.DMA
    vm = pl.BlockSpec(memory_space=pltpu.VMEM)
    hbm = pl.BlockSpec(memory_space=pltpu.HBM)
    return pl.pallas_call(
        functools.partial(kernel, n),
        out_shape=jax.ShapeDtypeStruct((rows, quarter), bf),
        in_specs=[hbm] * 10,
        out_specs=vm,
        scratch_shapes=[
            pltpu.VMEM(tokens.shape, bf),
            pltpu.VMEM((1, width), jnp.float32),
            pltpu.VMEM((top, rows), jnp.int32),
            pltpu.VMEM((top, rows), jnp.float32),
            pltpu.VMEM((width, 2 * hid), bf),
            pltpu.VMEM(down_proj.shape[1:], bf),
            pltpu.VMEM(shared_down.shape, bf),
            pltpu.VMEM((n * cap, rows), bf),
            pltpu.VMEM((top, nz, rows, 2 * cap), bf),
            pltpu.VMEM((n, cap, quarter), bf),
            pltpu.VMEM((4, n, cap, quarter), bf),
            pltpu.VMEM((2, 4, 2, rows, depth), bf),
            pltpu.VMEM((2, 4, 8, rows), jnp.float32),
            pltpu.VMEM((n, cap, 4 * hid), bf),
            pltpu.VMEM((rows, 4 * hid), bf),
            pltpu.VMEM((n, cap, quarter), bf),
            pltpu.VMEM((n, cap, quarter), bf),
            pltpu.VMEM((nz, depth, 2 * hid), bf),
            pltpu.VMEM((2, rows, 2 * hid), jnp.float32),
            pltpu.VMEM((2, rows, 2 * hid), bf),
            pltpu.VMEM((2, rows, 2 * hid), bf),
            pltpu.VMEM((rows, hid), bf),
            pltpu.VMEM((rows, quarter), jnp.float32),
            dma((10,)),
            dma((n,)), dma((n,)),
            dma((nz, 2)), dma((nz, 2)),
            dma((nz, 2)), dma((nz, 2)),
            dma((nz,)), dma((nz,)),
            dma((2, 7)), dma((2, 7)),
            dma((4,)), dma((2, 4)),
            dma((nz, 4)), dma((nz, 4)),
            dma((2, 4)), dma((4,)),
            dma((n,)), dma((n,)),
            dma((nz,)), dma((nz,)),
            dma((2,)), dma((2,)),
        ],
        compiler_params=pltpu.CompilerParams(
            collective_id=0, has_side_effects=True, vmem_limit_bytes=67043328
        ),
    )(tokens, norm_gain.reshape(1, width), expert_ids.T, expert_gates.T, gate_proj, up_proj, down_proj,
      shared_gate, shared_up, shared_down)


def solution(mesh):
    return jax.shard_map(
        functools.partial(shards, plain=not fits(mesh)),
        mesh=mesh,
        in_specs=(
            P("ep", "tp"),
            P(),
            P("ep", None),
            P("ep", None),
            P("ep", None, "tp"),
            P("ep", None, "tp"),
            P("ep", None, "tp"),
            P("ep", "tp"),
            P("ep", "tp"),
            P(None, "tp"),
        ),
        out_specs=P("ep", "tp"),
        check_vma=False,
    )
```

```python
import functools

import jax
import jax.numpy as jnp
from jax import lax
from jax.experimental import pallas as pl
from jax.experimental.pallas import tpu as pltpu
from jax.sharding import PartitionSpec as P

MESH = pl.DeviceIdType.MESH


def shards_plain(
    tokens,
    norm_gain,
    expert_ids,
    expert_gates,
    gate_proj,
    up_proj,
    down_proj,
    shared_gate,
    shared_up,
    shared_down,
):
    n_ep = lax.axis_size("ep")
    n_tp = lax.axis_size("tp")
    whole = lax.all_gather(tokens, "tp", axis=1, tiled=True)
    tok_rows, width = whole.shape
    quarter = width // n_tp
    floats = whole.astype(jnp.float32)
    scale = lax.rsqrt(jnp.mean(floats * floats, axis=-1, keepdims=True) + 1e-06)
    normed = (floats * scale * norm_gain[None, :]).astype(jnp.bfloat16)
    gate_whole, up_whole = (
        lax.all_gather(shared_gate, "ep", axis=0, tiled=True),
        lax.all_gather(shared_up, "ep", axis=0, tiled=True),
    )
    shared_g = jnp.dot(normed, gate_whole, preferred_element_type=jnp.float32)
    shared_u = jnp.dot(normed, up_whole, preferred_element_type=jnp.float32)
    shared_hidden = (jax.nn.silu(shared_g) * shared_u).astype(jnp.bfloat16)
    rows = shared_down
    shared_out = jnp.dot(
        lax.all_gather(shared_hidden, "tp", axis=1, tiled=True),
        rows,
        preferred_element_type=jnp.float32,
    )
    exp_dev = gate_proj.shape[0]
    n_exp = exp_dev * n_ep
    top = expert_ids.shape[1]
    cap = 3 * tok_rows * top // (2 * n_exp)
    flat_ids = expert_ids.reshape(tok_rows * top)
    onehot = (flat_ids[:, None] == jnp.arange(n_exp, dtype=jnp.int32)[None, :]).astype(jnp.int32)
    slots = jnp.sum((jnp.cumsum(onehot, axis=0) - onehot) * onehot, axis=-1)
    dest = flat_ids * cap + slots
    local_tok = jnp.repeat(jnp.arange(tok_rows, dtype=jnp.int32), top)
    owner = jnp.full((n_exp * cap,), tok_rows, jnp.int32).at[dest].set(local_tok)
    padded = jnp.concatenate([normed, jnp.zeros((1, width), jnp.bfloat16)], axis=0)
    outgoing = padded[owner].reshape(n_ep, exp_dev, cap, width)
    received = lax.all_to_all(outgoing, "ep", split_axis=0, concat_axis=0, tiled=True)
    gate_vals = jnp.einsum(
        "secd,edh->sech", received, gate_proj, preferred_element_type=jnp.float32
    )
    up_vals = jnp.einsum("secd,edh->sech", received, up_proj, preferred_element_type=jnp.float32)
    expert_hidden = (jax.nn.silu(gate_vals) * up_vals).astype(jnp.bfloat16)
    rows = down_proj
    expert_out = jnp.einsum(
        "sech,ehd->secd",
        lax.all_gather(expert_hidden, "tp", axis=3, tiled=True),
        rows,
        preferred_element_type=jnp.float32,
    ).astype(jnp.bfloat16)
    returned = lax.all_to_all(expert_out, "ep", split_axis=0, concat_axis=0, tiled=True)
    picked = returned.reshape(n_exp * cap, quarter)[dest].reshape(tok_rows, top, quarter)
    routed = jnp.sum(expert_gates[:, :, None] * picked.astype(jnp.float32), axis=1)
    return (routed + shared_out).astype(jnp.bfloat16)


def fits(mesh):
    return mesh.shape["tp"] == 4 and mesh.shape["ep"] == 8


def remote(src, dst, send, recv, ep, tp):
    return pltpu.make_async_remote_copy(
        src_ref=src, dst_ref=dst, send_sem=send, recv_sem=recv, device_id=(ep, tp), device_id_type=MESH
    )


def silu_mul(v, hid):
    g, u = v[:, :hid], v[:, hid:]
    return ((g / (1.0 + jnp.exp(-g))) * u).astype(jnp.bfloat16)


def kernel(
    n,
    tokens_hbm, gain_hbm, ids_hbm, gates_hbm, gate_w, up_w, down_w, sgate_w, sup_w, sdown_w,
    out,
    tokens, gain, ids, gates, wgu, wdn, sdn, back, outbox, xs, tk, ssq, hb, shb, ob, ret, sw,
    acc, pout, pin, she, mix,
    load_sem, sent, disp_r, far_r, near_r, tk_r, ssq_r, hid_r, shid_r, ret_r, sw_r, part_r,
):
    ep, tp = lax.axis_index("ep"), lax.axis_index("tp")
    nz = n // 2
    z, x = ep // 2, ep % 2
    ox = ep + 1 - 2 * x
    mate = tp + 1 - 2 * (tp % 2)
    far = (tp + 2) % 4
    diag = (mate + 2) % 4
    rows, quarter = tokens.shape
    cap = xs.shape[2]
    hid = gate_w.shape[2]
    slots = n * cap
    width = gain.shape[1]
    depth = sgate_w.shape[0]

    side = 1 - 2 * (z // 2)
    inner = ((z + 1) // 2) % 2
    half = ep + 2 * side * (1 - 2 * inner)
    order = [z + side * (i - inner * (0, 2, 0, 2)[i]) for i in range(nz)]

    def load(src, dst, k):
        c = pltpu.make_async_copy(src, dst, load_sem.at[k])
        c.start()
        return c

    ids_in = load(ids_hbm, ids, 0)
    tokens_in = load(tokens_hbm, tokens, 1)
    gates_in = load(gates_hbm, gates, 2)
    gain_in = load(gain_hbm, gain, 3)
    load(sgate_w, sw.at[z, :, pl.ds(0, hid)], 4)
    load(sup_w, sw.at[z, :, pl.ds(hid, hid)], 4)
    load(gate_w.at[0], wgu.at[:, pl.ds(0, hid)], 5)
    load(up_w.at[0], wgu.at[:, pl.ds(hid, hid)], 5)
    down_in = load(down_w.at[0], wdn, 6)
    sdown_in = load(sdown_w, sdn, 7)

    barrier = pltpu.get_barrier_semaphore()
    for d in range(1, n):
        pl.semaphore_signal(barrier, inc=1, device_id=((ep + d) % n, tp), device_id_type=MESH)
    for d in range(1, 4):
        pl.semaphore_signal(barrier, inc=1, device_id=(ep, (tp + d) % 4), device_id_type=MESH)
        pl.semaphore_signal(barrier, inc=1, device_id=(half, (tp + d) % 4), device_id_type=MESH)

    def column(row):
        return jnp.broadcast_to(row.astype(jnp.float32), (rows, rows)).T

    ids_in.wait()
    sub = lax.broadcasted_iota(jnp.int32, (rows, rows), 0)
    tok = lax.broadcasted_iota(jnp.int32, (rows, rows), 1)
    one = ((sub == ids[0:1, :]) | (sub == ids[1:2, :])).astype(jnp.float32).astype(jnp.bfloat16)
    earlier = (sub < tok).astype(jnp.float32).astype(jnp.bfloat16)
    place = jnp.dot(one, earlier, preferred_element_type=jnp.float32).astype(jnp.bfloat16)
    slot = lax.broadcasted_iota(jnp.int32, (slots, rows), 0)
    low = lax.broadcasted_iota(jnp.int32, (slots, rows), 1) * cap
    spread = ((slot >= low) & (slot < low + cap)).astype(jnp.float32).astype(jnp.bfloat16)
    place = jnp.dot(spread, place, preferred_element_type=jnp.float32)
    one = jnp.dot(spread, one, preferred_element_type=jnp.float32)
    slotf = slot.astype(jnp.float32)
    within = slotf - jnp.floor((slotf + 0.5) / cap) * cap
    pick = jnp.where(jnp.abs(place - within) < 0.5, one, 0.0).astype(jnp.bfloat16)
    tokens_in.wait()
    outbox[...] = (
        jnp.dot(pick, tokens[...], preferred_element_type=jnp.float32)
        .astype(jnp.bfloat16)
        .reshape(n, cap, quarter)
    )

    pl.semaphore_wait(barrier, n - 1 + 6)

    def landed(dst, sem):
        remote(dst, dst, sem, sem, ep, mate).wait_recv()

    def gone(src, k):
        remote(src, src, sent.at[k], sent.at[k], ep, mate).wait_send()

    xs[tp, ep] = outbox[ep]

    def dispatch(e):
        remote(outbox.at[e], xs.at[tp, ep], sent.at[0], disp_r.at[ep], e, tp).start()

    def spread_block(i, j):
        s = order[i] * 2 + (x + j) % 2
        blk = xs.at[tp, s]
        remote(blk, blk, sent.at[1], far_r.at[i], ep, far).start()
        remote(blk, blk, sent.at[1], near_r.at[i], ep, mate).start()

    def rows_of(i):
        blk = sw.at[order[i]]
        return remote(blk, blk, sent.at[9], sw_r.at[order[i]], ep + 2 * side, tp)

    def at_inner(f):
        pl.when(inner == 1)(f)

    def at_edge(f):
        pl.when(inner == 0)(f)

    spread_block(0, 0)
    dispatch(ox)
    for i in range(1, nz):
        for j in range(2):
            dispatch(order[i] * 2 + (x + j) % 2)
    pltpu.make_async_copy(sw.at[z], sw.at[z], load_sem.at[4]).wait()
    at_edge(lambda: rows_of(0).start())

    mine = tokens.at[:, pl.ds(pl.multiple_of(x * depth, depth), depth)]
    theirs = tokens.at[:, pl.ds(pl.multiple_of((1 - x) * depth, depth), depth)]
    home = ep + 2 * side * (1 - inner)
    home_ox = ox + 2 * side * (1 - inner)
    edge = ep - 2 * side
    plane = 1 - inner

    def own_tokens():
        return remote(mine, tk.at[1, tp, 0], sent.at[4], tk_r.at[1], home, tp)

    remote(theirs, tk.at[plane, tp, 1], sent.at[4], tk_r.at[plane], home_ox, tp).start()
    at_edge(lambda: own_tokens().start())
    own = tokens[...].astype(jnp.float32)
    sums = jnp.broadcast_to(jnp.sum(own * own, axis=-1, keepdims=True), (rows, 128)).T
    ssq[plane, tp] = sums[0:8, :]
    for d in range(1, 4):
        remote(ssq.at[plane, tp], ssq.at[plane, tp], sent.at[5], ssq_r.at[plane], home, (tp + d) % 4).start()

    def own_square():
        return remote(ssq.at[1, tp], ssq.at[1, tp], sent.at[5], ssq_r.at[1], home, tp)

    at_edge(lambda: own_square().start())

    def first_tokens(who, k):
        return remote(mine, tk.at[0, tp, 0], sent.at[3], tk_r.at[k], ep, who)

    @pl.when(inner == 1)
    def _():
        first_tokens(far, 2).start()
        first_tokens(mate, 4).start()
        tk[0, tp, 0] = mine[...]

    def places():
        lane = lax.broadcasted_iota(jnp.int32, (rows, 128), 1).astype(jnp.float32)
        ones = [(lane == column(ids[k : k + 1, :])).astype(jnp.float32) for k in range(2)]
        named = (ones[0] + ones[1]).astype(jnp.bfloat16)
        before = (tok < sub).astype(jnp.float32).astype(jnp.bfloat16)
        place = jnp.dot(before, named, preferred_element_type=jnp.float32).astype(jnp.bfloat16)
        low = lax.broadcasted_iota(jnp.int32, (128, slots), 0) * cap
        col = lax.broadcasted_iota(jnp.int32, (128, slots), 1)
        spread = ((col >= low) & (col < low + cap)).astype(jnp.float32).astype(jnp.bfloat16)
        place = jnp.dot(place, spread, preferred_element_type=jnp.float32)
        colf = lax.broadcasted_iota(jnp.int32, (rows, slots), 1).astype(jnp.float32)
        within = colf - jnp.floor((colf + 0.5) / cap) * cap
        hit = jnp.abs(place - within) < 0.5
        for k in range(2):
            sel = jnp.where(
                hit, jnp.dot(ones[k].astype(jnp.bfloat16), spread, preferred_element_type=jnp.float32), 0.0
            )
            for e in range(nz):
                back[k, e] = sel[:, 2 * e * cap : 2 * (e + 1) * cap].astype(jnp.bfloat16)

    places()

    def pair(ref, k, i):
        return ref.at[k, pl.ds(order[i] * 2, 2)]

    def stage_a(i):
        for j in range(2):
            s = order[i] * 2 + (x + j) % 2
            if i > 0 or j > 0:
                landed(xs.at[tp, s], disp_r.at[s])
                spread_block(i, j)

    def stage_b(i):
        blk = pair(xs, far, i)
        landed(blk, far_r.at[i])
        remote(blk, blk, sent.at[1], near_r.at[i], ep, mate).start()

    def stage_c(i):
        landed(xs.at[pl.ds(0, 2), pl.ds(0, 2)], near_r.at[i])
        if i == 0:
            pltpu.make_async_copy(wgu, wgu, load_sem.at[5]).wait()
            gain_in.wait()
        zz = order[i]
        sq = jnp.zeros((2 * cap, 1), jnp.float32)
        for k in range(4):
            v = xs[k, pl.ds(zz * 2, 2)].reshape(2 * cap, quarter).astype(jnp.float32)
            sq = sq + jnp.sum(v * v, axis=-1, keepdims=True)
        scale = lax.rsqrt(sq / width + 1e-06)
        val = jnp.zeros((2 * cap, 2 * hid), jnp.float32)
        for k in range(4):
            cols = slice(k * quarter, (k + 1) * quarter)
            v = xs[k, pl.ds(zz * 2, 2)].reshape(2 * cap, quarter).astype(jnp.float32)
            nk = (v * scale * gain[:, cols]).astype(jnp.bfloat16)
            val = val + jnp.dot(nk, wgu[cols, :], preferred_element_type=jnp.float32)
        hb[tp, pl.ds(zz * 2, 2)] = silu_mul(val, hid).reshape(2, cap, hid)
        blk = pair(hb, tp, i)
        for d in (2, 1, 3):
            remote(blk, blk, sent.at[2], hid_r.at[i], ep, (tp + d) % 4).start()

    def stage_d(i):
        zz = order[i]
        landed(hb.at[pl.ds(0, 3), pl.ds(0, 2)], hid_r.at[i])
        if i == 0:
            down_in.wait()
        h = jnp.concatenate([hb[k, pl.ds(zz * 2, 2)].reshape(2 * cap, hid) for k in range(4)], axis=-1)
        res = jnp.dot(h, wdn[...], preferred_element_type=jnp.float32).astype(jnp.bfloat16)
        ob[pl.ds(zz * 2, 2)] = res.reshape(2, cap, quarter)

    def back_to(i, j):
        s = order[i] * 2 + (x + j) % 2
        return remote(ob.at[s], ret.at[ep], sent.at[0], ret_r.at[z], s, tp)

    backs = [[back_to(i, j) for j in range(i == 0, 2)] for i in range(nz)]

    def send_back(i):
        if i == 0:
            ret[ep] = ob[ep]
        for c in backs[i]:
            c.start()

    def rows_pass():
        @pl.when(inner == 1)
        def _():
            landed(sw.at[order[1]], sw_r.at[order[1]])
            rows_of(1).start()

    def tokens_to(p, who, k):
        blk = tk.at[1, tp] if p == 1 else tk.at[0, tp, 1]
        return remote(blk, blk, sent.at[3], tk_r.at[k + p], ep, who)

    def tokens_on(p):
        return remote(tk.at[p, far], tk.at[p, far], sent.at[3], tk_r.at[4 + p], ep, mate)

    def spread_tokens(p):
        landed(tk.at[1, tp] if p == 1 else tk.at[0, tp, 1], tk_r.at[p])
        tokens_to(p, far, 2).start()
        tokens_to(p, mate, 4).start()

    def pass_tokens(p):
        landed(tk.at[p, far], tk_r.at[2 + p])
        tokens_on(p).start()

    def partial(p):
        return remote(pout.at[p], pin.at[p], sent.at[6], part_r.at[p], ox, tp)

    def shared_sum(p):
        landed(tk.at[p, pl.ds(0, 2)], tk_r.at[4 + p])
        val = jnp.zeros((2 * rows, 2 * hid), jnp.float32)
        for i in (0, 1, 3, 2):
            zz = order[i]
            if p == 1 and i in (2, 3):
                landed(sw.at[zz], sw_r.at[zz])
            cols = pl.ds(pl.multiple_of((2 * zz + x) * depth, depth), depth)
            v = (tk[p, zz].reshape(2 * rows, depth).astype(jnp.float32) * gain[:, cols]).astype(jnp.bfloat16)
            val = val + jnp.dot(v, sw[zz], preferred_element_type=jnp.float32)
        acc[p] = val[0:rows, :]
        pout[p] = val[rows:, :].astype(jnp.bfloat16)
        partial(p).start()

    def hidden_to(p, d):
        frm = shb.at[tp] if p == 0 else she
        return remote(frm, shb.at[tp], sent.at[7 + p], shid_r, ep if p == 0 else edge, (tp + d) % 4)

    def shared_hidden(p):
        square = jnp.zeros((8, rows), jnp.float32)
        for k in range(4):
            square = square + ssq[p, k]
        scale = column(lax.rsqrt(square[0:1, :] / width + 1e-06))[:, 0:1]
        landed(pin.at[p], part_r.at[p])
        val = silu_mul((acc[p] + pin[p].astype(jnp.float32)) * scale, hid)
        if p == 0:
            shb[tp] = val
        else:
            she[...] = val
        for d in (2, 3, 1, 0):
            if p == 1 or d > 0:
                hidden_to(p, d).start()

    def shared_inner():
        @pl.when(inner == 1)
        def _():
            pass_tokens(1)
            landed(ssq.at[0, pl.ds(0, 3)], ssq_r.at[0])
            landed(ssq.at[1], ssq_r.at[1])
            shared_sum(1)
            shared_sum(0)
            shared_hidden(1)
            shared_hidden(0)

    def shared_end():
        at_inner(lambda: landed(shb.at[pl.ds(0, 3)], shid_r))
        at_edge(lambda: landed(shb, shid_r))

    def drain():
        gone(xs.at[pl.ds(0, 2), pl.ds(0, n - 1)], 0)
        gone(xs.at[pl.ds(0, 3)], 1)
        gone(hb.at[pl.ds(0, 3)], 2)

        @pl.when(inner == 0)
        def _():
            gone(tk.at[0, 0], 4)
            gone(ssq.at[0], 5)
            gone(sw.at[0], 9)

        @pl.when(inner == 1)
        def _():
            gone(tk.at[pl.ds(0, 2), pl.ds(0, 3)], 3)
            gone(tk.at[0, 0, 0], 4)
            gone(ssq.at[0, pl.ds(0, 3)], 5)
            gone(pin, 6)
            gone(shb.at[pl.ds(0, 3)], 7)
            gone(shb, 8)
            gone(sw.at[pl.ds(0, 2)], 9)

    def combine(i):
        zz = order[i]
        landed(ret.at[pl.ds(0, 2)] if i > 0 else ret.at[0], ret_r.at[zz])
        got = ret[pl.ds(zz * 2, 2)].reshape(2 * cap, quarter)
        for k in range(2):
            mix[...] += column(gates[k : k + 1, :])[:, 0:1] * jnp.dot(
                back[k, zz], got, preferred_element_type=jnp.float32
            )

    stage_a(0)
    stage_a(1)
    stage_b(0)
    stage_c(0)
    stage_b(1)
    stage_a(2)
    stage_c(1)
    at_inner(lambda: rows_of(0).start())
    stage_d(0)
    send_back(0)
    stage_b(2)
    stage_a(3)
    stage_d(1)
    send_back(1)
    rows_pass()
    stage_c(2)
    at_inner(lambda: spread_tokens(0))
    stage_b(3)
    stage_d(2)
    send_back(2)
    stage_c(3)
    at_inner(lambda: spread_tokens(1))
    at_inner(lambda: pass_tokens(0))
    stage_d(3)
    send_back(3)
    mix[...] = jnp.zeros((rows, quarter), jnp.float32)
    gates_in.wait()
    shared_inner()
    combine(0)
    combine(1)
    combine(2)
    shared_end()
    sdown_in.wait()
    hidden = jnp.concatenate([shb[k] for k in range(4)], axis=-1)
    mix[...] += jnp.dot(hidden, sdn[...], preferred_element_type=jnp.float32)
    combine(3)
    out[...] = mix[...].astype(jnp.bfloat16)
    drain()


def shards(
    tokens, norm_gain, expert_ids, expert_gates, gate_proj, up_proj, down_proj,
    shared_gate, shared_up, shared_down, plain,
):
    n = lax.axis_size("ep")
    rows, quarter = tokens.shape
    top = expert_ids.shape[1]
    exp_dev = gate_proj.shape[0]
    cap = 3 * rows * top // (2 * exp_dev * n)
    hid = gate_proj.shape[2]
    depth = shared_gate.shape[0]
    ok = exp_dev == 1 and top == 2 and cap % 16 == 0 and hid % 128 == 0 and rows == 128
    ok = ok and shared_gate.shape[1] == hid and quarter == 2 * depth and depth % 128 == 0
    if plain or not ok:
        return shards_plain(
            tokens, norm_gain, expert_ids, expert_gates, gate_proj, up_proj, down_proj,
            shared_gate, shared_up, shared_down,
        )
    width = norm_gain.shape[0]
    bf = jnp.bfloat16
    nz = n // 2
    dma = pltpu.SemaphoreType.DMA
    vm = pl.BlockSpec(memory_space=pltpu.VMEM)
    hbm = pl.BlockSpec(memory_space=pltpu.HBM)
    operands = (
        tokens, norm_gain.reshape(1, width), expert_ids.T, expert_gates.T, gate_proj, up_proj, down_proj,
        shared_gate, shared_up, shared_down,
    )
    return pl.pallas_call(
        functools.partial(kernel, n),
        out_shape=jax.ShapeDtypeStruct((rows, quarter), bf),
        in_specs=[hbm] * 10,
        out_specs=vm,
        scratch_shapes=[
            pltpu.VMEM(tokens.shape, bf),
            pltpu.VMEM((1, width), jnp.float32),
            pltpu.VMEM((top, rows), jnp.int32),
            pltpu.VMEM((top, rows), jnp.float32),
            pltpu.VMEM((width, 2 * hid), bf),
            pltpu.VMEM(down_proj.shape[1:], bf),
            pltpu.VMEM(shared_down.shape, bf),
            pltpu.VMEM((top, nz, rows, 2 * cap), bf),
            pltpu.VMEM((n, cap, quarter), bf),
            pltpu.VMEM((4, n, cap, quarter), bf),
            pltpu.VMEM((2, 4, 2, rows, depth), bf),
            pltpu.VMEM((2, 4, 8, rows), jnp.float32),
            pltpu.VMEM((4, n, cap, hid), bf),
            pltpu.VMEM((4, rows, hid), bf),
            pltpu.VMEM((n, cap, quarter), bf),
            pltpu.VMEM((n, cap, quarter), bf),
            pltpu.VMEM((nz, depth, 2 * hid), bf),
            pltpu.VMEM((2, rows, 2 * hid), jnp.float32),
            pltpu.VMEM((2, rows, 2 * hid), bf),
            pltpu.VMEM((2, rows, 2 * hid), bf),
            pltpu.VMEM((rows, hid), bf),
            pltpu.VMEM((rows, quarter), jnp.float32),
            dma((8,)), dma((10,)), dma((n,)),
            dma((nz,)), dma((nz,)), dma((6,)), dma((2,)), dma((nz,)), dma, dma((nz,)), dma((nz,)), dma((2,)),
        ],
        compiler_params=pltpu.CompilerParams(
            collective_id=0, has_side_effects=True, vmem_limit_bytes=48 * 1024 * 1024
        ),
    )(*(pltpu.with_memory_space_constraint(a, pltpu.HBM) for a in operands))


def solution(mesh):
    return jax.shard_map(
        functools.partial(shards, plain=not fits(mesh)),
        mesh=mesh,
        in_specs=(
            P("ep", "tp"),
            P(),
            P("ep", None),
            P("ep", None),
            P("ep", None, "tp"),
            P("ep", None, "tp"),
            P("ep", None, "tp"),
            P("ep", "tp"),
            P("ep", "tp"),
            P(None, "tp"),
        ),
        out_specs=P("ep", "tp"),
        check_vma=False,
    )
```

```python
import functools

import jax
import jax.numpy as jnp
from jax import lax
from jax.experimental import pallas as pl
from jax.experimental.pallas import tpu as pltpu
from jax.sharding import PartitionSpec as P

MESH = pl.DeviceIdType.MESH


def shards_plain(
    tokens,
    norm_gain,
    expert_ids,
    expert_gates,
    gate_proj,
    up_proj,
    down_proj,
    shared_gate,
    shared_up,
    shared_down,
):
    n_ep = lax.axis_size("ep")
    n_tp = lax.axis_size("tp")
    whole = lax.all_gather(tokens, "tp", axis=1, tiled=True)
    tok_rows, width = whole.shape
    quarter = width // n_tp
    floats = whole.astype(jnp.float32)
    scale = lax.rsqrt(jnp.mean(floats * floats, axis=-1, keepdims=True) + 1e-06)
    normed = (floats * scale * norm_gain[None, :]).astype(jnp.bfloat16)
    gate_whole, up_whole = (
        lax.all_gather(shared_gate, "ep", axis=0, tiled=True),
        lax.all_gather(shared_up, "ep", axis=0, tiled=True),
    )
    shared_g = jnp.dot(normed, gate_whole, preferred_element_type=jnp.float32)
    shared_u = jnp.dot(normed, up_whole, preferred_element_type=jnp.float32)
    shared_hidden = (jax.nn.silu(shared_g) * shared_u).astype(jnp.bfloat16)
    rows = shared_down
    shared_out = jnp.dot(
        lax.all_gather(shared_hidden, "tp", axis=1, tiled=True),
        rows,
        preferred_element_type=jnp.float32,
    )
    exp_dev = gate_proj.shape[0]
    n_exp = exp_dev * n_ep
    top = expert_ids.shape[1]
    cap = 3 * tok_rows * top // (2 * n_exp)
    flat_ids = expert_ids.reshape(tok_rows * top)
    onehot = (flat_ids[:, None] == jnp.arange(n_exp, dtype=jnp.int32)[None, :]).astype(jnp.int32)
    slots = jnp.sum((jnp.cumsum(onehot, axis=0) - onehot) * onehot, axis=-1)
    dest = flat_ids * cap + slots
    local_tok = jnp.repeat(jnp.arange(tok_rows, dtype=jnp.int32), top)
    owner = jnp.full((n_exp * cap,), tok_rows, jnp.int32).at[dest].set(local_tok)
    padded = jnp.concatenate([normed, jnp.zeros((1, width), jnp.bfloat16)], axis=0)
    outgoing = padded[owner].reshape(n_ep, exp_dev, cap, width)
    received = lax.all_to_all(outgoing, "ep", split_axis=0, concat_axis=0, tiled=True)
    gate_vals = jnp.einsum(
        "secd,edh->sech", received, gate_proj, preferred_element_type=jnp.float32
    )
    up_vals = jnp.einsum("secd,edh->sech", received, up_proj, preferred_element_type=jnp.float32)
    expert_hidden = (jax.nn.silu(gate_vals) * up_vals).astype(jnp.bfloat16)
    rows = down_proj
    expert_out = jnp.einsum(
        "sech,ehd->secd",
        lax.all_gather(expert_hidden, "tp", axis=3, tiled=True),
        rows,
        preferred_element_type=jnp.float32,
    ).astype(jnp.bfloat16)
    returned = lax.all_to_all(expert_out, "ep", split_axis=0, concat_axis=0, tiled=True)
    picked = returned.reshape(n_exp * cap, quarter)[dest].reshape(tok_rows, top, quarter)
    routed = jnp.sum(expert_gates[:, :, None] * picked.astype(jnp.float32), axis=1)
    return (routed + shared_out).astype(jnp.bfloat16)


def fits(mesh):
    return mesh.shape["tp"] == 4 and mesh.shape["ep"] == 8


def remote(src, dst, send, recv, ep, tp):
    return pltpu.make_async_remote_copy(
        src_ref=src, dst_ref=dst, send_sem=send, recv_sem=recv, device_id=(ep, tp), device_id_type=MESH
    )


def silu_mul(v, hid):
    g, u = v[:, :hid], v[:, hid:]
    return ((g / (1.0 + jnp.exp(-g))) * u).astype(jnp.bfloat16)


def kernel(
    n,
    tokens_hbm, gain_hbm, ids_hbm, gates_hbm, gate_w, up_w, down_w, sgate_w, sup_w, sdown_w,
    out,
    tokens, gain, ids, gates, wgu, wdn, sdn, back, outbox, xs, tk, ssq, hb, shb, ob, ret, sw,
    acc, pout, pin, she, mix,
    load_sem, sent, disp_r, far_r, near_r, tk_r, ssq_r, hid_r, shid_r, ret_r, sw_r, part_r,
):
    ep, tp = lax.axis_index("ep"), lax.axis_index("tp")
    nz = n // 2
    z, x = ep // 2, ep % 2
    ox = ep + 1 - 2 * x
    mate = tp + 1 - 2 * (tp % 2)
    far = (tp + 2) % 4
    diag = (mate + 2) % 4
    rows, quarter = tokens.shape
    cap = xs.shape[2]
    hid = gate_w.shape[2]
    slots = n * cap
    width = gain.shape[1]
    depth = sgate_w.shape[0]

    side = 1 - 2 * (z // 2)
    inner = ((z + 1) // 2) % 2
    half = ep + 2 * side * (1 - 2 * inner)
    order = [z + side * (i - inner * (0, 2, 0, 2)[i]) for i in range(nz)]

    def load(src, dst, k):
        c = pltpu.make_async_copy(src, dst, load_sem.at[k])
        c.start()
        return c

    ids_in = load(ids_hbm, ids, 0)
    tokens_in = load(tokens_hbm, tokens, 1)
    gates_in = load(gates_hbm, gates, 2)
    gain_in = load(gain_hbm, gain, 3)
    load(sgate_w, sw.at[z, :, pl.ds(0, hid)], 4)
    load(sup_w, sw.at[z, :, pl.ds(hid, hid)], 4)
    load(gate_w.at[0], wgu.at[:, pl.ds(0, hid)], 5)
    load(up_w.at[0], wgu.at[:, pl.ds(hid, hid)], 5)
    down_in = load(down_w.at[0], wdn, 6)
    sdown_in = load(sdown_w, sdn, 7)

    barrier = pltpu.get_barrier_semaphore()
    for d in range(1, n):
        pl.semaphore_signal(barrier, inc=1, device_id=((ep + d) % n, tp), device_id_type=MESH)
    for d in range(1, 4):
        pl.semaphore_signal(barrier, inc=1, device_id=(ep, (tp + d) % 4), device_id_type=MESH)
        pl.semaphore_signal(barrier, inc=1, device_id=(half, (tp + d) % 4), device_id_type=MESH)

    def column(row):
        return jnp.broadcast_to(row.astype(jnp.float32), (rows, rows)).T

    ids_in.wait()
    sub = lax.broadcasted_iota(jnp.int32, (rows, rows), 0)
    tok = lax.broadcasted_iota(jnp.int32, (rows, rows), 1)
    one = ((sub == ids[0:1, :]) | (sub == ids[1:2, :])).astype(jnp.float32).astype(jnp.bfloat16)
    earlier = (sub < tok).astype(jnp.float32).astype(jnp.bfloat16)
    place = jnp.dot(one, earlier, preferred_element_type=jnp.float32).astype(jnp.bfloat16)
    slot = lax.broadcasted_iota(jnp.int32, (slots, rows), 0)
    low = lax.broadcasted_iota(jnp.int32, (slots, rows), 1) * cap
    spread = ((slot >= low) & (slot < low + cap)).astype(jnp.float32).astype(jnp.bfloat16)
    place = jnp.dot(spread, place, preferred_element_type=jnp.float32)
    one = jnp.dot(spread, one, preferred_element_type=jnp.float32)
    slotf = slot.astype(jnp.float32)
    within = slotf - jnp.floor((slotf + 0.5) / cap) * cap
    pick = jnp.where(jnp.abs(place - within) < 0.5, one, 0.0).astype(jnp.bfloat16)
    tokens_in.wait()
    outbox[...] = (
        jnp.dot(pick, tokens[...], preferred_element_type=jnp.float32)
        .astype(jnp.bfloat16)
        .reshape(n, cap, quarter)
    )

    pl.semaphore_wait(barrier, n - 1 + 6)

    def landed(dst, sem):
        remote(dst, dst, sem, sem, ep, mate).wait_recv()

    def gone(src, k):
        remote(src, src, sent.at[k], sent.at[k], ep, mate).wait_send()

    xs[tp, ep] = outbox[ep]

    def dispatch(e):
        remote(outbox.at[e], xs.at[tp, ep], sent.at[0], disp_r.at[ep], e, tp).start()

    def spread_block(i, j):
        s = order[i] * 2 + (x + j) % 2
        blk = xs.at[tp, s]
        remote(blk, blk, sent.at[1], far_r.at[i], ep, far).start()
        remote(blk, blk, sent.at[1], near_r.at[i], ep, mate).start()

    def rows_of(i):
        blk = sw.at[order[i]]
        return remote(blk, blk, sent.at[9], sw_r.at[order[i]], ep + 2 * side, tp)

    def at_inner(f):
        pl.when(inner == 1)(f)

    def at_edge(f):
        pl.when(inner == 0)(f)

    spread_block(0, 0)
    dispatch(ox)
    for i in range(1, nz):
        for j in range(2):
            dispatch(order[i] * 2 + (x + j) % 2)
    pltpu.make_async_copy(sw.at[z], sw.at[z], load_sem.at[4]).wait()
    at_edge(lambda: rows_of(0).start())

    mine = tokens.at[:, pl.ds(pl.multiple_of(x * depth, depth), depth)]
    theirs = tokens.at[:, pl.ds(pl.multiple_of((1 - x) * depth, depth), depth)]
    home = ep + 2 * side * (1 - inner)
    home_ox = ox + 2 * side * (1 - inner)
    edge = ep - 2 * side
    plane = 1 - inner

    def own_tokens():
        return remote(mine, tk.at[1, tp, 0], sent.at[4], tk_r.at[6], home, tp)

    remote(theirs, tk.at[plane, tp, 1], sent.at[4], tk_r.at[plane], home_ox, tp).start()
    at_edge(lambda: own_tokens().start())
    own = tokens[...].astype(jnp.float32)
    sums = jnp.broadcast_to(jnp.sum(own * own, axis=-1, keepdims=True), (rows, 128)).T
    ssq[plane, tp] = sums[0:8, :]
    for d in range(1, 4):
        remote(ssq.at[plane, tp], ssq.at[plane, tp], sent.at[5], ssq_r.at[plane], home, (tp + d) % 4).start()

    def own_square():
        return remote(ssq.at[1, tp], ssq.at[1, tp], sent.at[5], ssq_r.at[1], home, tp)

    at_edge(lambda: own_square().start())

    def first_tokens(who, k):
        return remote(mine, tk.at[0, tp, 0], sent.at[3], tk_r.at[k], ep, who)

    @pl.when(inner == 1)
    def _():
        first_tokens(far, 2).start()
        first_tokens(mate, 4).start()
        tk[0, tp, 0] = mine[...]

    def places():
        lane = lax.broadcasted_iota(jnp.int32, (rows, 128), 1).astype(jnp.float32)
        ones = [(lane == column(ids[k : k + 1, :])).astype(jnp.float32) for k in range(2)]
        named = (ones[0] + ones[1]).astype(jnp.bfloat16)
        before = (tok < sub).astype(jnp.float32).astype(jnp.bfloat16)
        place = jnp.dot(before, named, preferred_element_type=jnp.float32).astype(jnp.bfloat16)
        low = lax.broadcasted_iota(jnp.int32, (128, slots), 0) * cap
        col = lax.broadcasted_iota(jnp.int32, (128, slots), 1)
        spread = ((col >= low) & (col < low + cap)).astype(jnp.float32).astype(jnp.bfloat16)
        place = jnp.dot(place, spread, preferred_element_type=jnp.float32)
        colf = lax.broadcasted_iota(jnp.int32, (rows, slots), 1).astype(jnp.float32)
        within = colf - jnp.floor((colf + 0.5) / cap) * cap
        hit = jnp.abs(place - within) < 0.5
        for k in range(2):
            sel = jnp.where(
                hit, jnp.dot(ones[k].astype(jnp.bfloat16), spread, preferred_element_type=jnp.float32), 0.0
            )
            for e in range(nz):
                back[k, e] = sel[:, 2 * e * cap : 2 * (e + 1) * cap].astype(jnp.bfloat16)

    places()

    def pair(ref, k, i):
        return ref.at[k, pl.ds(order[i] * 2, 2)]

    def stage_a(i):
        for j in range(2):
            s = order[i] * 2 + (x + j) % 2
            if i > 0 or j > 0:
                landed(xs.at[tp, s], disp_r.at[s])
                spread_block(i, j)

    def stage_b(i):
        blk = pair(xs, far, i)
        landed(blk, far_r.at[i])
        remote(blk, blk, sent.at[1], near_r.at[i], ep, mate).start()

    def stage_c(i):
        landed(xs.at[pl.ds(0, 2), pl.ds(0, 2)], near_r.at[i])
        if i == 0:
            pltpu.make_async_copy(wgu, wgu, load_sem.at[5]).wait()
            gain_in.wait()
        zz = order[i]
        sq = jnp.zeros((2 * cap, 1), jnp.float32)
        for k in range(4):
            v = xs[k, pl.ds(zz * 2, 2)].reshape(2 * cap, quarter).astype(jnp.float32)
            sq = sq + jnp.sum(v * v, axis=-1, keepdims=True)
        scale = lax.rsqrt(sq / width + 1e-06)
        val = jnp.zeros((2 * cap, 2 * hid), jnp.float32)
        for k in range(4):
            cols = slice(k * quarter, (k + 1) * quarter)
            v = xs[k, pl.ds(zz * 2, 2)].reshape(2 * cap, quarter).astype(jnp.float32)
            nk = (v * scale * gain[:, cols]).astype(jnp.bfloat16)
            val = val + jnp.dot(nk, wgu[cols, :], preferred_element_type=jnp.float32)
        hb[tp, pl.ds(zz * 2, 2)] = silu_mul(val, hid).reshape(2, cap, hid)
        blk = pair(hb, tp, i)
        for d in (2, 1, 3):
            remote(blk, blk, sent.at[2], hid_r.at[i], ep, (tp + d) % 4).start()

    def stage_d(i):
        zz = order[i]
        landed(hb.at[pl.ds(0, 3), pl.ds(0, 2)], hid_r.at[i])
        if i == 0:
            down_in.wait()
        h = jnp.concatenate([hb[k, pl.ds(zz * 2, 2)].reshape(2 * cap, hid) for k in range(4)], axis=-1)
        res = jnp.dot(h, wdn[...], preferred_element_type=jnp.float32).astype(jnp.bfloat16)
        ob[pl.ds(zz * 2, 2)] = res.reshape(2, cap, quarter)

    def back_to(i, j):
        s = order[i] * 2 + (x + j) % 2
        return remote(ob.at[s], ret.at[ep], sent.at[0], ret_r.at[z], s, tp)

    backs = [[back_to(i, j) for j in range(i == 0, 2)] for i in range(nz)]

    def send_back(i):
        if i == 0:
            ret[ep] = ob[ep]
        for c in backs[i]:
            c.start()

    def rows_pass():
        @pl.when(inner == 1)
        def _():
            landed(sw.at[order[1]], sw_r.at[order[1]])
            rows_of(1).start()

    def tokens_to(p, b, who, k):
        blk = tk.at[p, tp, b]
        return remote(blk, blk, sent.at[3], tk_r.at[k + p], ep, who)

    def tokens_on(p):
        return remote(tk.at[p, far], tk.at[p, far], sent.at[3], tk_r.at[4 + p], ep, mate)

    def spread_tokens(p, b):
        landed(tk.at[p, tp, b], tk_r.at[p if b == 1 else 6])
        tokens_to(p, b, far, 2).start()
        tokens_to(p, b, mate, 4).start()

    def pass_tokens(p):
        landed(tk.at[p, far], tk_r.at[2 + p])
        tokens_on(p).start()

    def partial(p):
        return remote(pout.at[p], pin.at[p], sent.at[6], part_r.at[p], ox, tp)

    def shared_sum(p):
        landed(tk.at[p, pl.ds(0, 2)], tk_r.at[4 + p])
        val = jnp.zeros((2 * rows, 2 * hid), jnp.float32)
        for i in (0, 1, 3, 2):
            zz = order[i]
            if p == 1 and i in (2, 3):
                landed(sw.at[zz], sw_r.at[zz])
            cols = pl.ds(pl.multiple_of((2 * zz + x) * depth, depth), depth)
            v = (tk[p, zz].reshape(2 * rows, depth).astype(jnp.float32) * gain[:, cols]).astype(jnp.bfloat16)
            val = val + jnp.dot(v, sw[zz], preferred_element_type=jnp.float32)
        acc[p] = val[0:rows, :]
        pout[p] = val[rows:, :].astype(jnp.bfloat16)
        partial(p).start()

    def hidden_to(p, d):
        frm = shb.at[tp] if p == 0 else she
        return remote(frm, shb.at[tp], sent.at[7 + p], shid_r.at[0], ep if p == 0 else edge, (tp + d) % 4)

    def shared_hidden(p):
        square = jnp.zeros((8, rows), jnp.float32)
        for k in range(4):
            square = square + ssq[p, k]
        scale = column(lax.rsqrt(square[0:1, :] / width + 1e-06))[:, 0:1]
        landed(pin.at[p], part_r.at[p])
        val = silu_mul((acc[p] + pin[p].astype(jnp.float32)) * scale, hid)
        if p == 0:
            shb[tp] = val
        else:
            she[...] = val
        for d in (2, 3, 1) if p == 0 else (2, 0):
            hidden_to(p, d).start()

    def shared_inner():
        @pl.when(inner == 1)
        def _():
            pass_tokens(1)
            landed(ssq.at[0, pl.ds(0, 3)], ssq_r.at[0])
            landed(ssq.at[1], ssq_r.at[1])
            shared_sum(1)
            shared_sum(0)
            shared_hidden(1)
            shared_hidden(0)

    def shared_end():
        at_inner(lambda: landed(shb.at[pl.ds(0, 3)], shid_r.at[0]))

        @pl.when(inner == 0)
        def _():
            landed(shb.at[pl.ds(0, 2)], shid_r.at[0])
            for k in (tp, far):
                remote(shb.at[k], shb.at[k], sent.at[7], shid_r.at[1], ep, mate).start()
            landed(shb.at[pl.ds(0, 2)], shid_r.at[1])

    def drain():
        gone(xs.at[pl.ds(0, 2), pl.ds(0, n - 1)], 0)
        gone(xs.at[pl.ds(0, 3)], 1)
        gone(hb.at[pl.ds(0, 3)], 2)

        @pl.when(inner == 0)
        def _():
            gone(tk.at[0, 0], 4)
            gone(ssq.at[0], 5)
            gone(shb.at[pl.ds(0, 2)], 7)
            gone(sw.at[0], 9)

        @pl.when(inner == 1)
        def _():
            gone(tk.at[pl.ds(0, 2), pl.ds(0, 3)], 3)
            gone(tk.at[0, 0, 0], 4)
            gone(ssq.at[0, pl.ds(0, 3)], 5)
            gone(pin, 6)
            gone(shb.at[pl.ds(0, 3)], 7)
            gone(shb.at[pl.ds(0, 2)], 8)
            gone(sw.at[pl.ds(0, 2)], 9)

    def combine(i):
        zz = order[i]
        landed(ret.at[pl.ds(0, 2)] if i > 0 else ret.at[0], ret_r.at[zz])
        got = ret[pl.ds(zz * 2, 2)].reshape(2 * cap, quarter)
        for k in range(2):
            mix[...] += column(gates[k : k + 1, :])[:, 0:1] * jnp.dot(
                back[k, zz], got, preferred_element_type=jnp.float32
            )

    stage_a(0)
    stage_a(1)
    stage_b(0)
    stage_c(0)
    stage_b(1)
    stage_a(2)
    stage_c(1)
    at_inner(lambda: rows_of(0).start())
    stage_d(0)
    send_back(0)
    stage_b(2)
    stage_a(3)
    stage_d(1)
    send_back(1)
    rows_pass()
    stage_c(2)
    at_inner(lambda: spread_tokens(0, 1))
    stage_b(3)
    at_inner(lambda: spread_tokens(1, 1))
    stage_d(2)
    send_back(2)
    stage_c(3)
    at_inner(lambda: spread_tokens(1, 0))
    at_inner(lambda: pass_tokens(0))
    stage_d(3)
    send_back(3)
    mix[...] = jnp.zeros((rows, quarter), jnp.float32)
    gates_in.wait()
    shared_inner()
    combine(0)
    combine(1)
    combine(2)
    shared_end()
    sdown_in.wait()
    hidden = jnp.concatenate([shb[k] for k in range(4)], axis=-1)
    mix[...] += jnp.dot(hidden, sdn[...], preferred_element_type=jnp.float32)
    combine(3)
    out[...] = mix[...].astype(jnp.bfloat16)
    drain()


def shards(
    tokens, norm_gain, expert_ids, expert_gates, gate_proj, up_proj, down_proj,
    shared_gate, shared_up, shared_down, plain,
):
    n = lax.axis_size("ep")
    rows, quarter = tokens.shape
    top = expert_ids.shape[1]
    exp_dev = gate_proj.shape[0]
    cap = 3 * rows * top // (2 * exp_dev * n)
    hid = gate_proj.shape[2]
    depth = shared_gate.shape[0]
    ok = exp_dev == 1 and top == 2 and cap % 16 == 0 and hid % 128 == 0 and rows == 128
    ok = ok and shared_gate.shape[1] == hid and quarter == 2 * depth and depth % 128 == 0
    if plain or not ok:
        return shards_plain(
            tokens, norm_gain, expert_ids, expert_gates, gate_proj, up_proj, down_proj,
            shared_gate, shared_up, shared_down,
        )
    width = norm_gain.shape[0]
    bf = jnp.bfloat16
    nz = n // 2
    dma = pltpu.SemaphoreType.DMA
    vm = pl.BlockSpec(memory_space=pltpu.VMEM)
    hbm = pl.BlockSpec(memory_space=pltpu.HBM)
    operands = (
        tokens, norm_gain.reshape(1, width), expert_ids.T, expert_gates.T, gate_proj, up_proj, down_proj,
        shared_gate, shared_up, shared_down,
    )
    return pl.pallas_call(
        functools.partial(kernel, n),
        out_shape=jax.ShapeDtypeStruct((rows, quarter), bf),
        in_specs=[hbm] * 10,
        out_specs=vm,
        scratch_shapes=[
            pltpu.VMEM(tokens.shape, bf),
            pltpu.VMEM((1, width), jnp.float32),
            pltpu.VMEM((top, rows), jnp.int32),
            pltpu.VMEM((top, rows), jnp.float32),
            pltpu.VMEM((width, 2 * hid), bf),
            pltpu.VMEM(down_proj.shape[1:], bf),
            pltpu.VMEM(shared_down.shape, bf),
            pltpu.VMEM((top, nz, rows, 2 * cap), bf),
            pltpu.VMEM((n, cap, quarter), bf),
            pltpu.VMEM((4, n, cap, quarter), bf),
            pltpu.VMEM((2, 4, 2, rows, depth), bf),
            pltpu.VMEM((2, 4, 8, rows), jnp.float32),
            pltpu.VMEM((4, n, cap, hid), bf),
            pltpu.VMEM((4, rows, hid), bf),
            pltpu.VMEM((n, cap, quarter), bf),
            pltpu.VMEM((n, cap, quarter), bf),
            pltpu.VMEM((nz, depth, 2 * hid), bf),
            pltpu.VMEM((2, rows, 2 * hid), jnp.float32),
            pltpu.VMEM((2, rows, 2 * hid), bf),
            pltpu.VMEM((2, rows, 2 * hid), bf),
            pltpu.VMEM((rows, hid), bf),
            pltpu.VMEM((rows, quarter), jnp.float32),
            dma((8,)), dma((10,)), dma((n,)),
            dma((nz,)), dma((nz,)), dma((7,)), dma((2,)), dma((nz,)), dma((2,)), dma((nz,)), dma((nz,)), dma((2,)),
        ],
        compiler_params=pltpu.CompilerParams(
            collective_id=0, has_side_effects=True, vmem_limit_bytes=48 * 1024 * 1024
        ),
    )(*(pltpu.with_memory_space_constraint(a, pltpu.HBM) for a in operands))


def solution(mesh):
    return jax.shard_map(
        functools.partial(shards, plain=not fits(mesh)),
        mesh=mesh,
        in_specs=(
            P("ep", "tp"),
            P(),
            P("ep", None),
            P("ep", None),
            P("ep", None, "tp"),
            P("ep", None, "tp"),
            P("ep", None, "tp"),
            P("ep", "tp"),
            P("ep", "tp"),
            P(None, "tp"),
        ),
        out_specs=P("ep", "tp"),
        check_vma=False,
    )
```

```python
import functools

import jax
import jax.numpy as jnp
from jax import lax
from jax.experimental import pallas as pl
from jax.experimental.pallas import tpu as pltpu
from jax.sharding import PartitionSpec as P

MESH = pl.DeviceIdType.MESH


def shards_plain(
    tokens,
    norm_gain,
    expert_ids,
    expert_gates,
    gate_proj,
    up_proj,
    down_proj,
    shared_gate,
    shared_up,
    shared_down,
):
    n_ep = lax.axis_size("ep")
    n_tp = lax.axis_size("tp")
    whole = lax.all_gather(tokens, "tp", axis=1, tiled=True)
    tok_rows, width = whole.shape
    quarter = width // n_tp
    floats = whole.astype(jnp.float32)
    scale = lax.rsqrt(jnp.mean(floats * floats, axis=-1, keepdims=True) + 1e-06)
    normed = (floats * scale * norm_gain[None, :]).astype(jnp.bfloat16)
    gate_whole, up_whole = (
        lax.all_gather(shared_gate, "ep", axis=0, tiled=True),
        lax.all_gather(shared_up, "ep", axis=0, tiled=True),
    )
    shared_g = jnp.dot(normed, gate_whole, preferred_element_type=jnp.float32)
    shared_u = jnp.dot(normed, up_whole, preferred_element_type=jnp.float32)
    shared_hidden = (jax.nn.silu(shared_g) * shared_u).astype(jnp.bfloat16)
    rows = shared_down
    shared_out = jnp.dot(
        lax.all_gather(shared_hidden, "tp", axis=1, tiled=True),
        rows,
        preferred_element_type=jnp.float32,
    )
    exp_dev = gate_proj.shape[0]
    n_exp = exp_dev * n_ep
    top = expert_ids.shape[1]
    cap = 3 * tok_rows * top // (2 * n_exp)
    flat_ids = expert_ids.reshape(tok_rows * top)
    onehot = (flat_ids[:, None] == jnp.arange(n_exp, dtype=jnp.int32)[None, :]).astype(jnp.int32)
    slots = jnp.sum((jnp.cumsum(onehot, axis=0) - onehot) * onehot, axis=-1)
    dest = flat_ids * cap + slots
    local_tok = jnp.repeat(jnp.arange(tok_rows, dtype=jnp.int32), top)
    owner = jnp.full((n_exp * cap,), tok_rows, jnp.int32).at[dest].set(local_tok)
    padded = jnp.concatenate([normed, jnp.zeros((1, width), jnp.bfloat16)], axis=0)
    outgoing = padded[owner].reshape(n_ep, exp_dev, cap, width)
    received = lax.all_to_all(outgoing, "ep", split_axis=0, concat_axis=0, tiled=True)
    gate_vals = jnp.einsum(
        "secd,edh->sech", received, gate_proj, preferred_element_type=jnp.float32
    )
    up_vals = jnp.einsum("secd,edh->sech", received, up_proj, preferred_element_type=jnp.float32)
    expert_hidden = (jax.nn.silu(gate_vals) * up_vals).astype(jnp.bfloat16)
    rows = down_proj
    expert_out = jnp.einsum(
        "sech,ehd->secd",
        lax.all_gather(expert_hidden, "tp", axis=3, tiled=True),
        rows,
        preferred_element_type=jnp.float32,
    ).astype(jnp.bfloat16)
    returned = lax.all_to_all(expert_out, "ep", split_axis=0, concat_axis=0, tiled=True)
    picked = returned.reshape(n_exp * cap, quarter)[dest].reshape(tok_rows, top, quarter)
    routed = jnp.sum(expert_gates[:, :, None] * picked.astype(jnp.float32), axis=1)
    return (routed + shared_out).astype(jnp.bfloat16)


def fits(mesh):
    return mesh.shape["tp"] == 4 and mesh.shape["ep"] == 8


def remote(src, dst, send, recv, ep, tp):
    return pltpu.make_async_remote_copy(
        src_ref=src, dst_ref=dst, send_sem=send, recv_sem=recv, device_id=(ep, tp), device_id_type=MESH
    )


def silu_mul(v, hid):
    g, u = v[:, :hid], v[:, hid:]
    return ((g / (1.0 + jnp.exp(-g))) * u).astype(jnp.bfloat16)


def kernel(
    n,
    tokens_hbm, gain_hbm, ids_hbm, gates_hbm, gate_w, up_w, down_w, sgate_w, sup_w, sdown_w,
    out,
    tokens, gain, ids, gates, wgu, wdn, sdn, back, outbox, xs, tk, ssq, hb, shb, ob, ret, sw,
    acc, pout, pin, she, mix,
    load_sem, sent, disp_r, far_r, near_r, tk_r, ssq_r, hid_r, hid_far, shid_r, ret_r, sw_r, part_r,
):
    ep, tp = lax.axis_index("ep"), lax.axis_index("tp")
    nz = n // 2
    z, x = ep // 2, ep % 2
    ox = ep + 1 - 2 * x
    mate = tp + 1 - 2 * (tp % 2)
    far = (tp + 2) % 4
    diag = (mate + 2) % 4
    rows, quarter = tokens.shape
    cap = xs.shape[2]
    hid = gate_w.shape[2]
    slots = n * cap
    width = gain.shape[1]
    depth = sgate_w.shape[0]

    side = 1 - 2 * (z // 2)
    inner = ((z + 1) // 2) % 2
    half = ep + 2 * side * (1 - 2 * inner)
    order = [z + side * (i - inner * (0, 2, 0, 2)[i]) for i in range(nz)]

    def load(src, dst, k):
        c = pltpu.make_async_copy(src, dst, load_sem.at[k])
        c.start()
        return c

    ids_in = load(ids_hbm, ids, 0)
    tokens_in = load(tokens_hbm, tokens, 1)
    gates_in = load(gates_hbm, gates, 2)
    gain_in = load(gain_hbm, gain, 3)
    load(sgate_w, sw.at[z, :, pl.ds(0, hid)], 4)
    load(sup_w, sw.at[z, :, pl.ds(hid, hid)], 4)
    load(gate_w.at[0], wgu.at[:, pl.ds(0, hid)], 5)
    load(up_w.at[0], wgu.at[:, pl.ds(hid, hid)], 5)
    down_in = load(down_w.at[0], wdn, 6)
    sdown_in = load(sdown_w, sdn, 7)

    barrier = pltpu.get_barrier_semaphore()
    for d in range(1, n):
        pl.semaphore_signal(barrier, inc=1, device_id=((ep + d) % n, tp), device_id_type=MESH)
    for d in range(1, 4):
        pl.semaphore_signal(barrier, inc=1, device_id=(ep, (tp + d) % 4), device_id_type=MESH)
        pl.semaphore_signal(barrier, inc=1, device_id=(half, (tp + d) % 4), device_id_type=MESH)

    def column(row):
        return jnp.broadcast_to(row.astype(jnp.float32), (rows, rows)).T

    ids_in.wait()
    sub = lax.broadcasted_iota(jnp.int32, (rows, rows), 0)
    tok = lax.broadcasted_iota(jnp.int32, (rows, rows), 1)
    one = ((sub == ids[0:1, :]) | (sub == ids[1:2, :])).astype(jnp.float32).astype(jnp.bfloat16)
    earlier = (sub < tok).astype(jnp.float32).astype(jnp.bfloat16)
    place = jnp.dot(one, earlier, preferred_element_type=jnp.float32).astype(jnp.bfloat16)
    slot = lax.broadcasted_iota(jnp.int32, (slots, rows), 0)
    low = lax.broadcasted_iota(jnp.int32, (slots, rows), 1) * cap
    spread = ((slot >= low) & (slot < low + cap)).astype(jnp.float32).astype(jnp.bfloat16)
    place = jnp.dot(spread, place, preferred_element_type=jnp.float32)
    one = jnp.dot(spread, one, preferred_element_type=jnp.float32)
    slotf = slot.astype(jnp.float32)
    within = slotf - jnp.floor((slotf + 0.5) / cap) * cap
    pick = jnp.where(jnp.abs(place - within) < 0.5, one, 0.0).astype(jnp.bfloat16)
    tokens_in.wait()
    outbox[...] = (
        jnp.dot(pick, tokens[...], preferred_element_type=jnp.float32)
        .astype(jnp.bfloat16)
        .reshape(n, cap, quarter)
    )

    pl.semaphore_wait(barrier, n - 1 + 6)

    def landed(dst, sem):
        remote(dst, dst, sem, sem, ep, mate).wait_recv()

    def gone(src, k):
        remote(src, src, sent.at[k], sent.at[k], ep, mate).wait_send()

    xs[tp, ep] = outbox[ep]

    def dispatch(e):
        remote(outbox.at[e], xs.at[tp, ep], sent.at[0], disp_r.at[ep], e, tp).start()

    def spread_block(i, j):
        s = order[i] * 2 + (x + j) % 2
        blk = xs.at[tp, s]
        remote(blk, blk, sent.at[1], far_r.at[i], ep, far).start()
        remote(blk, blk, sent.at[1], near_r.at[i], ep, mate).start()

    def rows_of(i):
        blk = sw.at[order[i]]
        return remote(blk, blk, sent.at[9], sw_r.at[order[i]], ep + 2 * side, tp)

    def at_inner(f):
        pl.when(inner == 1)(f)

    def at_edge(f):
        pl.when(inner == 0)(f)

    spread_block(0, 0)
    dispatch(ox)
    for i in range(1, nz):
        for j in range(2):
            dispatch(order[i] * 2 + (x + j) % 2)
    pltpu.make_async_copy(sw.at[z], sw.at[z], load_sem.at[4]).wait()
    at_edge(lambda: rows_of(0).start())

    mine = tokens.at[:, pl.ds(pl.multiple_of(x * depth, depth), depth)]
    theirs = tokens.at[:, pl.ds(pl.multiple_of((1 - x) * depth, depth), depth)]
    home = ep + 2 * side * (1 - inner)
    home_ox = ox + 2 * side * (1 - inner)
    edge = ep - 2 * side
    plane = 1 - inner

    def own_tokens():
        return remote(mine, tk.at[1, tp, 0], sent.at[4], tk_r.at[6], home, tp)

    remote(theirs, tk.at[plane, tp, 1], sent.at[4], tk_r.at[plane], home_ox, tp).start()
    at_edge(lambda: own_tokens().start())
    own = tokens[...].astype(jnp.float32)
    sums = jnp.broadcast_to(jnp.sum(own * own, axis=-1, keepdims=True), (rows, 128)).T
    ssq[plane, tp] = sums[0:8, :]
    for d in range(1, 4):
        remote(ssq.at[plane, tp], ssq.at[plane, tp], sent.at[5], ssq_r.at[plane], home, (tp + d) % 4).start()

    def own_square():
        return remote(ssq.at[1, tp], ssq.at[1, tp], sent.at[5], ssq_r.at[1], home, tp)

    at_edge(lambda: own_square().start())

    def first_tokens(who, k):
        return remote(mine, tk.at[0, tp, 0], sent.at[3], tk_r.at[k], ep, who)

    @pl.when(inner == 1)
    def _():
        first_tokens(far, 2).start()
        first_tokens(mate, 4).start()
        tk[0, tp, 0] = mine[...]

    def places():
        lane = lax.broadcasted_iota(jnp.int32, (rows, 128), 1).astype(jnp.float32)
        ones = [(lane == column(ids[k : k + 1, :])).astype(jnp.float32) for k in range(2)]
        named = (ones[0] + ones[1]).astype(jnp.bfloat16)
        before = (tok < sub).astype(jnp.float32).astype(jnp.bfloat16)
        place = jnp.dot(before, named, preferred_element_type=jnp.float32).astype(jnp.bfloat16)
        low = lax.broadcasted_iota(jnp.int32, (128, slots), 0) * cap
        col = lax.broadcasted_iota(jnp.int32, (128, slots), 1)
        spread = ((col >= low) & (col < low + cap)).astype(jnp.float32).astype(jnp.bfloat16)
        place = jnp.dot(place, spread, preferred_element_type=jnp.float32)
        colf = lax.broadcasted_iota(jnp.int32, (rows, slots), 1).astype(jnp.float32)
        within = colf - jnp.floor((colf + 0.5) / cap) * cap
        hit = jnp.abs(place - within) < 0.5
        for k in range(2):
            sel = jnp.where(
                hit, jnp.dot(ones[k].astype(jnp.bfloat16), spread, preferred_element_type=jnp.float32), 0.0
            )
            for e in range(nz):
                back[k, e] = sel[:, 2 * e * cap : 2 * (e + 1) * cap].astype(jnp.bfloat16)

    places()

    def pair(ref, k, i):
        return ref.at[k, pl.ds(order[i] * 2, 2)]

    def stage_a(i):
        for j in range(2):
            s = order[i] * 2 + (x + j) % 2
            if i > 0 or j > 0:
                landed(xs.at[tp, s], disp_r.at[s])
                spread_block(i, j)

    def stage_b(i):
        blk = pair(xs, far, i)
        landed(blk, far_r.at[i])
        remote(blk, blk, sent.at[1], near_r.at[i], ep, mate).start()

    via = (0, 1)

    def stage_c(i):
        landed(xs.at[pl.ds(0, 2), pl.ds(0, 2)], near_r.at[i])
        if i == 0:
            pltpu.make_async_copy(wgu, wgu, load_sem.at[5]).wait()
            gain_in.wait()
        zz = order[i]
        sq = jnp.zeros((2 * cap, 1), jnp.float32)
        for k in range(4):
            v = xs[k, pl.ds(zz * 2, 2)].reshape(2 * cap, quarter).astype(jnp.float32)
            sq = sq + jnp.sum(v * v, axis=-1, keepdims=True)
        scale = lax.rsqrt(sq / width + 1e-06)
        val = jnp.zeros((2 * cap, 2 * hid), jnp.float32)
        for k in range(4):
            cols = slice(k * quarter, (k + 1) * quarter)
            v = xs[k, pl.ds(zz * 2, 2)].reshape(2 * cap, quarter).astype(jnp.float32)
            nk = (v * scale * gain[:, cols]).astype(jnp.bfloat16)
            val = val + jnp.dot(nk, wgu[cols, :], preferred_element_type=jnp.float32)
        hb[tp, pl.ds(zz * 2, 2)] = silu_mul(val, hid).reshape(2, cap, hid)
        blk = pair(hb, tp, i)
        if i in via:
            remote(blk, blk, sent.at[2], hid_far.at[i], ep, far).start()
            remote(blk, blk, sent.at[2], hid_r.at[i], ep, mate).start()
        else:
            for d in (2, 1, 3):
                remote(blk, blk, sent.at[2], hid_r.at[i], ep, (tp + d) % 4).start()

    def hidden_on(i):
        if i in via:
            blk = pair(hb, far, i)
            landed(blk, hid_far.at[i])
            remote(blk, blk, sent.at[2], hid_r.at[i], ep, mate).start()

    def stage_d(i):
        zz = order[i]
        landed(hb.at[pl.ds(0, 2 if i in via else 3), pl.ds(0, 2)], hid_r.at[i])
        if i == 0:
            down_in.wait()
        h = jnp.concatenate([hb[k, pl.ds(zz * 2, 2)].reshape(2 * cap, hid) for k in range(4)], axis=-1)
        res = jnp.dot(h, wdn[...], preferred_element_type=jnp.float32).astype(jnp.bfloat16)
        ob[pl.ds(zz * 2, 2)] = res.reshape(2, cap, quarter)

    def back_to(i, j):
        s = order[i] * 2 + (x + j) % 2
        return remote(ob.at[s], ret.at[ep], sent.at[0], ret_r.at[z], s, tp)

    backs = [[back_to(i, j) for j in range(i == 0, 2)] for i in range(nz)]

    def send_back(i):
        if i == 0:
            ret[ep] = ob[ep]
        for c in backs[i]:
            c.start()

    def rows_pass():
        @pl.when(inner == 1)
        def _():
            landed(sw.at[order[1]], sw_r.at[order[1]])
            rows_of(1).start()

    def tokens_to(p, b, who, k):
        blk = tk.at[p, tp, b]
        return remote(blk, blk, sent.at[3], tk_r.at[k + p], ep, who)

    def tokens_on(p):
        return remote(tk.at[p, far], tk.at[p, far], sent.at[3], tk_r.at[4 + p], ep, mate)

    def spread_tokens(p, b):
        landed(tk.at[p, tp, b], tk_r.at[p if b == 1 else 6])
        tokens_to(p, b, far, 2).start()
        tokens_to(p, b, mate, 4).start()

    def pass_tokens(p):
        landed(tk.at[p, far], tk_r.at[2 + p])
        tokens_on(p).start()

    def partial(p):
        return remote(pout.at[p], pin.at[p], sent.at[6], part_r.at[p], ox, tp)

    def shared_sum(p):
        landed(tk.at[p, pl.ds(0, 2)], tk_r.at[4 + p])
        val = jnp.zeros((2 * rows, 2 * hid), jnp.float32)
        for i in (0, 1, 3, 2):
            zz = order[i]
            if p == 1 and i in (2, 3):
                landed(sw.at[zz], sw_r.at[zz])
            cols = pl.ds(pl.multiple_of((2 * zz + x) * depth, depth), depth)
            v = (tk[p, zz].reshape(2 * rows, depth).astype(jnp.float32) * gain[:, cols]).astype(jnp.bfloat16)
            val = val + jnp.dot(v, sw[zz], preferred_element_type=jnp.float32)
        acc[p] = val[0:rows, :]
        pout[p] = val[rows:, :].astype(jnp.bfloat16)
        partial(p).start()

    def hidden_to(p, d):
        frm = shb.at[tp] if p == 0 else she
        return remote(frm, shb.at[tp], sent.at[7 + p], shid_r.at[0], ep if p == 0 else edge, (tp + d) % 4)

    def shared_hidden(p):
        square = jnp.zeros((8, rows), jnp.float32)
        for k in range(4):
            square = square + ssq[p, k]
        scale = column(lax.rsqrt(square[0:1, :] / width + 1e-06))[:, 0:1]
        landed(pin.at[p], part_r.at[p])
        val = silu_mul((acc[p] + pin[p].astype(jnp.float32)) * scale, hid)
        if p == 0:
            shb[tp] = val
        else:
            she[...] = val
        for d in (2, 3, 1) if p == 0 else (2, 0):
            hidden_to(p, d).start()

    def shared_inner():
        @pl.when(inner == 1)
        def _():
            pass_tokens(1)
            landed(ssq.at[0, pl.ds(0, 3)], ssq_r.at[0])
            landed(ssq.at[1], ssq_r.at[1])
            shared_sum(1)
            send_back(3)
            pass_tokens(0)
            shared_sum(0)
            shared_hidden(1)
            shared_hidden(0)

    def shared_end():
        at_inner(lambda: landed(shb.at[pl.ds(0, 3)], shid_r.at[0]))

        @pl.when(inner == 0)
        def _():
            landed(shb.at[pl.ds(0, 2)], shid_r.at[0])
            for k in (tp, far):
                remote(shb.at[k], shb.at[k], sent.at[7], shid_r.at[1], ep, mate).start()
            landed(shb.at[pl.ds(0, 2)], shid_r.at[1])

    def drain():
        gone(xs.at[pl.ds(0, 2), pl.ds(0, n - 1)], 0)
        gone(xs.at[pl.ds(0, 3)], 1)
        gone(hb.at[pl.ds(0, 3)], 2)

        @pl.when(inner == 0)
        def _():
            gone(tk.at[0, 0], 4)
            gone(ssq.at[0], 5)
            gone(shb.at[pl.ds(0, 2)], 7)
            gone(sw.at[0], 9)

        @pl.when(inner == 1)
        def _():
            gone(tk.at[pl.ds(0, 2), pl.ds(0, 3)], 3)
            gone(tk.at[0, 0, 0], 4)
            gone(ssq.at[0, pl.ds(0, 3)], 5)
            gone(pin, 6)
            gone(shb.at[pl.ds(0, 3)], 7)
            gone(shb.at[pl.ds(0, 2)], 8)
            gone(sw.at[pl.ds(0, 2)], 9)

    def combine(i):
        zz = order[i]
        landed(ret.at[pl.ds(0, 2)] if i > 0 else ret.at[0], ret_r.at[zz])
        got = ret[pl.ds(zz * 2, 2)].reshape(2 * cap, quarter)
        for k in range(2):
            mix[...] += column(gates[k : k + 1, :])[:, 0:1] * jnp.dot(
                back[k, zz], got, preferred_element_type=jnp.float32
            )

    stage_a(0)
    stage_a(1)
    stage_b(0)
    stage_c(0)
    stage_b(1)
    stage_a(2)
    hidden_on(0)
    stage_c(1)
    at_inner(lambda: rows_of(0).start())
    stage_d(0)
    send_back(0)
    stage_b(2)
    hidden_on(1)
    stage_a(3)
    stage_d(1)
    send_back(1)
    rows_pass()
    stage_c(2)
    stage_b(3)
    at_inner(lambda: spread_tokens(1, 1))
    at_inner(lambda: spread_tokens(0, 1))
    stage_d(2)
    send_back(2)
    stage_c(3)
    at_inner(lambda: spread_tokens(1, 0))
    stage_d(3)
    at_edge(lambda: send_back(3))
    mix[...] = jnp.zeros((rows, quarter), jnp.float32)
    gates_in.wait()
    shared_inner()
    combine(0)
    combine(1)
    combine(2)
    shared_end()
    sdown_in.wait()
    hidden = jnp.concatenate([shb[k] for k in range(4)], axis=-1)
    mix[...] += jnp.dot(hidden, sdn[...], preferred_element_type=jnp.float32)
    combine(3)
    out[...] = mix[...].astype(jnp.bfloat16)
    drain()


def shards(
    tokens, norm_gain, expert_ids, expert_gates, gate_proj, up_proj, down_proj,
    shared_gate, shared_up, shared_down, plain,
):
    n = lax.axis_size("ep")
    rows, quarter = tokens.shape
    top = expert_ids.shape[1]
    exp_dev = gate_proj.shape[0]
    cap = 3 * rows * top // (2 * exp_dev * n)
    hid = gate_proj.shape[2]
    depth = shared_gate.shape[0]
    ok = exp_dev == 1 and top == 2 and cap % 16 == 0 and hid % 128 == 0 and rows == 128
    ok = ok and shared_gate.shape[1] == hid and quarter == 2 * depth and depth % 128 == 0
    if plain or not ok:
        return shards_plain(
            tokens, norm_gain, expert_ids, expert_gates, gate_proj, up_proj, down_proj,
            shared_gate, shared_up, shared_down,
        )
    width = norm_gain.shape[0]
    bf = jnp.bfloat16
    nz = n // 2
    dma = pltpu.SemaphoreType.DMA
    vm = pl.BlockSpec(memory_space=pltpu.VMEM)
    hbm = pl.BlockSpec(memory_space=pltpu.HBM)
    operands = (
        tokens, norm_gain.reshape(1, width), expert_ids.T, expert_gates.T, gate_proj, up_proj, down_proj,
        shared_gate, shared_up, shared_down,
    )
    return pl.pallas_call(
        functools.partial(kernel, n),
        out_shape=jax.ShapeDtypeStruct((rows, quarter), bf),
        in_specs=[hbm] * 10,
        out_specs=vm,
        scratch_shapes=[
            pltpu.VMEM(tokens.shape, bf),
            pltpu.VMEM((1, width), jnp.float32),
            pltpu.VMEM((top, rows), jnp.int32),
            pltpu.VMEM((top, rows), jnp.float32),
            pltpu.VMEM((width, 2 * hid), bf),
            pltpu.VMEM(down_proj.shape[1:], bf),
            pltpu.VMEM(shared_down.shape, bf),
            pltpu.VMEM((top, nz, rows, 2 * cap), bf),
            pltpu.VMEM((n, cap, quarter), bf),
            pltpu.VMEM((4, n, cap, quarter), bf),
            pltpu.VMEM((2, 4, 2, rows, depth), bf),
            pltpu.VMEM((2, 4, 8, rows), jnp.float32),
            pltpu.VMEM((4, n, cap, hid), bf),
            pltpu.VMEM((4, rows, hid), bf),
            pltpu.VMEM((n, cap, quarter), bf),
            pltpu.VMEM((n, cap, quarter), bf),
            pltpu.VMEM((nz, depth, 2 * hid), bf),
            pltpu.VMEM((2, rows, 2 * hid), jnp.float32),
            pltpu.VMEM((2, rows, 2 * hid), bf),
            pltpu.VMEM((2, rows, 2 * hid), bf),
            pltpu.VMEM((rows, hid), bf),
            pltpu.VMEM((rows, quarter), jnp.float32),
            dma((8,)), dma((10,)), dma((n,)),
            dma((nz,)), dma((nz,)), dma((7,)), dma((2,)), dma((nz,)), dma((nz,)), dma((2,)), dma((nz,)), dma((nz,)), dma((2,)),
        ],
        compiler_params=pltpu.CompilerParams(
            collective_id=0, has_side_effects=True, vmem_limit_bytes=48 * 1024 * 1024
        ),
    )(*(pltpu.with_memory_space_constraint(a, pltpu.HBM) for a in operands))


def solution(mesh):
    return jax.shard_map(
        functools.partial(shards, plain=not fits(mesh)),
        mesh=mesh,
        in_specs=(
            P("ep", "tp"),
            P(),
            P("ep", None),
            P("ep", None),
            P("ep", None, "tp"),
            P("ep", None, "tp"),
            P("ep", None, "tp"),
            P("ep", "tp"),
            P("ep", "tp"),
            P(None, "tp"),
        ),
        out_specs=P("ep", "tp"),
        check_vma=False,
    )
```

```python
import functools

import jax
import jax.numpy as jnp
from jax import lax
from jax.experimental import pallas as pl
from jax.experimental.pallas import tpu as pltpu
from jax.sharding import PartitionSpec as P

MESH = pl.DeviceIdType.MESH


def shards_plain(
    tokens,
    norm_gain,
    expert_ids,
    expert_gates,
    gate_proj,
    up_proj,
    down_proj,
    shared_gate,
    shared_up,
    shared_down,
):
    n_ep = lax.axis_size("ep")
    n_tp = lax.axis_size("tp")
    whole = lax.all_gather(tokens, "tp", axis=1, tiled=True)
    tok_rows, width = whole.shape
    quarter = width // n_tp
    floats = whole.astype(jnp.float32)
    scale = lax.rsqrt(jnp.mean(floats * floats, axis=-1, keepdims=True) + 1e-06)
    normed = (floats * scale * norm_gain[None, :]).astype(jnp.bfloat16)
    gate_whole, up_whole = (
        lax.all_gather(shared_gate, "ep", axis=0, tiled=True),
        lax.all_gather(shared_up, "ep", axis=0, tiled=True),
    )
    shared_g = jnp.dot(normed, gate_whole, preferred_element_type=jnp.float32)
    shared_u = jnp.dot(normed, up_whole, preferred_element_type=jnp.float32)
    shared_hidden = (jax.nn.silu(shared_g) * shared_u).astype(jnp.bfloat16)
    rows = shared_down
    shared_out = jnp.dot(
        lax.all_gather(shared_hidden, "tp", axis=1, tiled=True),
        rows,
        preferred_element_type=jnp.float32,
    )
    exp_dev = gate_proj.shape[0]
    n_exp = exp_dev * n_ep
    top = expert_ids.shape[1]
    cap = 3 * tok_rows * top // (2 * n_exp)
    flat_ids = expert_ids.reshape(tok_rows * top)
    onehot = (flat_ids[:, None] == jnp.arange(n_exp, dtype=jnp.int32)[None, :]).astype(jnp.int32)
    slots = jnp.sum((jnp.cumsum(onehot, axis=0) - onehot) * onehot, axis=-1)
    dest = flat_ids * cap + slots
    local_tok = jnp.repeat(jnp.arange(tok_rows, dtype=jnp.int32), top)
    owner = jnp.full((n_exp * cap,), tok_rows, jnp.int32).at[dest].set(local_tok)
    padded = jnp.concatenate([normed, jnp.zeros((1, width), jnp.bfloat16)], axis=0)
    outgoing = padded[owner].reshape(n_ep, exp_dev, cap, width)
    received = lax.all_to_all(outgoing, "ep", split_axis=0, concat_axis=0, tiled=True)
    gate_vals = jnp.einsum(
        "secd,edh->sech", received, gate_proj, preferred_element_type=jnp.float32
    )
    up_vals = jnp.einsum("secd,edh->sech", received, up_proj, preferred_element_type=jnp.float32)
    expert_hidden = (jax.nn.silu(gate_vals) * up_vals).astype(jnp.bfloat16)
    rows = down_proj
    expert_out = jnp.einsum(
        "sech,ehd->secd",
        lax.all_gather(expert_hidden, "tp", axis=3, tiled=True),
        rows,
        preferred_element_type=jnp.float32,
    ).astype(jnp.bfloat16)
    returned = lax.all_to_all(expert_out, "ep", split_axis=0, concat_axis=0, tiled=True)
    picked = returned.reshape(n_exp * cap, quarter)[dest].reshape(tok_rows, top, quarter)
    routed = jnp.sum(expert_gates[:, :, None] * picked.astype(jnp.float32), axis=1)
    return (routed + shared_out).astype(jnp.bfloat16)


def fits(mesh):
    return mesh.shape["tp"] == 4 and mesh.shape["ep"] == 8


def remote(src, dst, send, recv, ep, tp):
    return pltpu.make_async_remote_copy(
        src_ref=src, dst_ref=dst, send_sem=send, recv_sem=recv, device_id=(ep, tp), device_id_type=MESH
    )


def silu_mul(v, hid):
    g, u = v[:, :hid], v[:, hid:]
    return ((g / (1.0 + jnp.exp(-g))) * u).astype(jnp.bfloat16)


def kernel(
    n,
    tokens_hbm, gain_hbm, ids_hbm, gates_hbm, gate_w, up_w, down_w, sgate_w, sup_w, sdown_w,
    out,
    tokens, gain, ids, gates, wgu, wdn, sdn, back, outbox, xs, tk, ssq, hb, shb, ob, ret, sw,
    acc, pout, pin, she, mix,
    load_sem, sent, disp_r, far_r, near_r, tk_r, ssq_r, hid_r, hid_far, shid_r, ret_r, sw_r, part_r,
):
    ep, tp = lax.axis_index("ep"), lax.axis_index("tp")
    nz = n // 2
    z, x = ep // 2, ep % 2
    ox = ep + 1 - 2 * x
    mate = tp + 1 - 2 * (tp % 2)
    far = (tp + 2) % 4
    diag = (mate + 2) % 4
    rows, quarter = tokens.shape
    cap = xs.shape[2]
    hid = gate_w.shape[2]
    slots = n * cap
    width = gain.shape[1]
    depth = sgate_w.shape[0]

    side = 1 - 2 * (z // 2)
    inner = ((z + 1) // 2) % 2
    half = ep + 2 * side * (1 - 2 * inner)
    order = [z + side * (i - inner * (0, 2, 0, 2)[i]) for i in range(nz)]

    def load(src, dst, k):
        c = pltpu.make_async_copy(src, dst, load_sem.at[k])
        c.start()
        return c

    ids_in = load(ids_hbm, ids, 0)
    tokens_in = load(tokens_hbm, tokens, 1)
    gates_in = load(gates_hbm, gates, 2)
    gain_in = load(gain_hbm, gain, 3)
    load(sgate_w, sw.at[z, :, pl.ds(0, hid)], 4)
    load(sup_w, sw.at[z, :, pl.ds(hid, hid)], 4)
    load(gate_w.at[0], wgu.at[:, pl.ds(0, hid)], 5)
    load(up_w.at[0], wgu.at[:, pl.ds(hid, hid)], 5)
    down_in = load(down_w.at[0], wdn, 6)
    sdown_in = load(sdown_w, sdn, 7)

    barrier = pltpu.get_barrier_semaphore()
    for d in range(1, n):
        pl.semaphore_signal(barrier, inc=1, device_id=((ep + d) % n, tp), device_id_type=MESH)
    for d in range(1, 4):
        pl.semaphore_signal(barrier, inc=1, device_id=(ep, (tp + d) % 4), device_id_type=MESH)
        pl.semaphore_signal(barrier, inc=1, device_id=(half, (tp + d) % 4), device_id_type=MESH)

    def column(row):
        return jnp.broadcast_to(row.astype(jnp.float32), (rows, rows)).T

    ids_in.wait()
    sub = lax.broadcasted_iota(jnp.int32, (rows, rows), 0)
    tok = lax.broadcasted_iota(jnp.int32, (rows, rows), 1)
    one = ((sub == ids[0:1, :]) | (sub == ids[1:2, :])).astype(jnp.float32).astype(jnp.bfloat16)
    earlier = (sub < tok).astype(jnp.float32).astype(jnp.bfloat16)
    place = jnp.dot(one, earlier, preferred_element_type=jnp.float32).astype(jnp.bfloat16)
    slot = lax.broadcasted_iota(jnp.int32, (slots, rows), 0)
    low = lax.broadcasted_iota(jnp.int32, (slots, rows), 1) * cap
    spread = ((slot >= low) & (slot < low + cap)).astype(jnp.float32).astype(jnp.bfloat16)
    place = jnp.dot(spread, place, preferred_element_type=jnp.float32)
    one = jnp.dot(spread, one, preferred_element_type=jnp.float32)
    slotf = slot.astype(jnp.float32)
    within = slotf - jnp.floor((slotf + 0.5) / cap) * cap
    pick = jnp.where(jnp.abs(place - within) < 0.5, one, 0.0).astype(jnp.bfloat16)
    tokens_in.wait()
    outbox[...] = (
        jnp.dot(pick, tokens[...], preferred_element_type=jnp.float32)
        .astype(jnp.bfloat16)
        .reshape(n, cap, quarter)
    )

    pl.semaphore_wait(barrier, n - 1 + 6)

    def landed(dst, sem):
        remote(dst, dst, sem, sem, ep, mate).wait_recv()

    def gone(src, k):
        remote(src, src, sent.at[k], sent.at[k], ep, mate).wait_send()

    xs[tp, ep] = outbox[ep]

    def dispatch(e):
        remote(outbox.at[e], xs.at[tp, ep], sent.at[0], disp_r.at[ep], e, tp).start()

    def spread_block(i, j):
        s = order[i] * 2 + (x + j) % 2
        blk = xs.at[tp, s]
        remote(blk, blk, sent.at[1], far_r.at[i], ep, far).start()
        remote(blk, blk, sent.at[1], near_r.at[i], ep, mate).start()

    def rows_of(i):
        blk = sw.at[order[i]]
        return remote(blk, blk, sent.at[9], sw_r.at[order[i]], ep + 2 * side, tp)

    def at_inner(f):
        pl.when(inner == 1)(f)

    def at_edge(f):
        pl.when(inner == 0)(f)

    spread_block(0, 0)
    dispatch(ox)
    for i in range(1, nz):
        for j in range(2):
            dispatch(order[i] * 2 + (x + j) % 2)
    pltpu.make_async_copy(sw.at[z], sw.at[z], load_sem.at[4]).wait()
    at_edge(lambda: rows_of(0).start())

    mine = tokens.at[:, pl.ds(pl.multiple_of(x * depth, depth), depth)]
    theirs = tokens.at[:, pl.ds(pl.multiple_of((1 - x) * depth, depth), depth)]
    home = ep + 2 * side * (1 - inner)
    home_ox = ox + 2 * side * (1 - inner)
    edge = ep - 2 * side
    plane = 1 - inner

    def own_tokens():
        remote(mine, tk.at[1, tp, 0], sent.at[4], tk_r.at[0], ep, far).start()
        remote(mine, tk.at[1, tp, 0], sent.at[4], tk_r.at[6], home, tp).start()

    def edge_pass():
        @pl.when(inner == 0)
        def _():
            blk = tk.at[1, far, 0]
            landed(blk, tk_r.at[0])
            remote(blk, blk, sent.at[4], tk_r.at[3], home, tp).start()

    remote(theirs, tk.at[plane, tp, 1], sent.at[4], tk_r.at[plane], home_ox, tp).start()
    at_edge(own_tokens)
    own = tokens[...].astype(jnp.float32)
    sums = jnp.broadcast_to(jnp.sum(own * own, axis=-1, keepdims=True), (rows, 128)).T
    ssq[plane, tp] = sums[0:8, :]
    for d in range(1, 4):
        remote(ssq.at[plane, tp], ssq.at[plane, tp], sent.at[5], ssq_r.at[plane], home, (tp + d) % 4).start()

    def own_square():
        return remote(ssq.at[1, tp], ssq.at[1, tp], sent.at[5], ssq_r.at[1], home, tp)

    at_edge(lambda: own_square().start())

    def first_tokens(who, k):
        return remote(mine, tk.at[0, tp, 0], sent.at[4], tk_r.at[k], ep, who)

    @pl.when(inner == 1)
    def _():
        first_tokens(far, 2).start()
        first_tokens(mate, 4).start()
        tk[0, tp, 0] = mine[...]

    def places():
        lane = lax.broadcasted_iota(jnp.int32, (rows, 128), 1).astype(jnp.float32)
        ones = [(lane == column(ids[k : k + 1, :])).astype(jnp.float32) for k in range(2)]
        named = (ones[0] + ones[1]).astype(jnp.bfloat16)
        before = (tok < sub).astype(jnp.float32).astype(jnp.bfloat16)
        place = jnp.dot(before, named, preferred_element_type=jnp.float32).astype(jnp.bfloat16)
        low = lax.broadcasted_iota(jnp.int32, (128, slots), 0) * cap
        col = lax.broadcasted_iota(jnp.int32, (128, slots), 1)
        spread = ((col >= low) & (col < low + cap)).astype(jnp.float32).astype(jnp.bfloat16)
        place = jnp.dot(place, spread, preferred_element_type=jnp.float32)
        colf = lax.broadcasted_iota(jnp.int32, (rows, slots), 1).astype(jnp.float32)
        within = colf - jnp.floor((colf + 0.5) / cap) * cap
        hit = jnp.abs(place - within) < 0.5
        for k in range(2):
            sel = jnp.where(
                hit, jnp.dot(ones[k].astype(jnp.bfloat16), spread, preferred_element_type=jnp.float32), 0.0
            )
            for e in range(nz):
                back[k, e] = sel[:, 2 * e * cap : 2 * (e + 1) * cap].astype(jnp.bfloat16)

    places()

    def pair(ref, k, i):
        return ref.at[k, pl.ds(order[i] * 2, 2)]

    def stage_a(i):
        for j in range(2):
            s = order[i] * 2 + (x + j) % 2
            if i > 0 or j > 0:
                landed(xs.at[tp, s], disp_r.at[s])
                spread_block(i, j)

    def stage_b(i):
        blk = pair(xs, far, i)
        landed(blk, far_r.at[i])
        remote(blk, blk, sent.at[1], near_r.at[i], ep, mate).start()

    via = (0, 1)

    def stage_c(i):
        landed(xs.at[pl.ds(0, 2), pl.ds(0, 2)], near_r.at[i])
        if i == 0:
            pltpu.make_async_copy(wgu, wgu, load_sem.at[5]).wait()
            gain_in.wait()
        zz = order[i]
        sq = jnp.zeros((2 * cap, 1), jnp.float32)
        for k in range(4):
            v = xs[k, pl.ds(zz * 2, 2)].reshape(2 * cap, quarter).astype(jnp.float32)
            sq = sq + jnp.sum(v * v, axis=-1, keepdims=True)
        scale = lax.rsqrt(sq / width + 1e-06)
        val = jnp.zeros((2 * cap, 2 * hid), jnp.float32)
        for k in range(4):
            cols = slice(k * quarter, (k + 1) * quarter)
            v = xs[k, pl.ds(zz * 2, 2)].reshape(2 * cap, quarter).astype(jnp.float32)
            nk = (v * scale * gain[:, cols]).astype(jnp.bfloat16)
            val = val + jnp.dot(nk, wgu[cols, :], preferred_element_type=jnp.float32)
        hb[tp, pl.ds(zz * 2, 2)] = silu_mul(val, hid).reshape(2, cap, hid)
        blk = pair(hb, tp, i)
        if i in via:
            remote(blk, blk, sent.at[2], hid_far.at[i], ep, far).start()
            remote(blk, blk, sent.at[2], hid_r.at[i], ep, mate).start()
        else:
            for d in (2, 1, 3):
                remote(blk, blk, sent.at[2], hid_r.at[i], ep, (tp + d) % 4).start()

    def hidden_on(i):
        if i in via:
            blk = pair(hb, far, i)
            landed(blk, hid_far.at[i])
            remote(blk, blk, sent.at[2], hid_r.at[i], ep, mate).start()

    def stage_d(i):
        zz = order[i]
        landed(hb.at[pl.ds(0, 2 if i in via else 3), pl.ds(0, 2)], hid_r.at[i])
        if i == 0:
            down_in.wait()
        h = jnp.concatenate([hb[k, pl.ds(zz * 2, 2)].reshape(2 * cap, hid) for k in range(4)], axis=-1)
        res = jnp.dot(h, wdn[...], preferred_element_type=jnp.float32).astype(jnp.bfloat16)
        ob[pl.ds(zz * 2, 2)] = res.reshape(2, cap, quarter)

    def back_to(i, j):
        s = order[i] * 2 + (x + j) % 2
        return remote(ob.at[s], ret.at[ep], sent.at[0], ret_r.at[z], s, tp)

    backs = [[back_to(i, j) for j in range(i == 0, 2)] for i in range(nz)]

    def send_back(i):
        if i == 0:
            ret[ep] = ob[ep]
        for c in backs[i]:
            c.start()

    def rows_pass():
        @pl.when(inner == 1)
        def _():
            landed(sw.at[order[1]], sw_r.at[order[1]])
            rows_of(1).start()

    def tokens_to(p, b, who, k):
        blk = tk.at[p, tp, b]
        return remote(blk, blk, sent.at[3 if (p, b) != (1, 0) else 4], tk_r.at[k + p], ep, who)

    def tokens_on(p):
        return remote(tk.at[p, far], tk.at[p, far], sent.at[3], tk_r.at[4 + p], ep, mate)

    def spread_tokens(p, b):
        landed(tk.at[p, tp, b], tk_r.at[p if b == 1 else 6])
        if (p, b) != (1, 0):
            tokens_to(p, b, far, 2).start()
        tokens_to(p, b, mate, 4).start()

    def pass_tokens(p):
        landed(tk.at[p, far], tk_r.at[2 + p])
        tokens_on(p).start()

    def partial(p):
        return remote(pout.at[p], pin.at[p], sent.at[6], part_r.at[p], ox, tp)

    def shared_sum(p):
        landed(tk.at[p, pl.ds(0, 2)], tk_r.at[4 + p])
        val = jnp.zeros((2 * rows, 2 * hid), jnp.float32)
        for i in (0, 1, 3, 2):
            zz = order[i]
            if p == 1 and i in (2, 3):
                landed(sw.at[zz], sw_r.at[zz])
            cols = pl.ds(pl.multiple_of((2 * zz + x) * depth, depth), depth)
            v = (tk[p, zz].reshape(2 * rows, depth).astype(jnp.float32) * gain[:, cols]).astype(jnp.bfloat16)
            val = val + jnp.dot(v, sw[zz], preferred_element_type=jnp.float32)
        acc[p] = val[0:rows, :]
        pout[p] = val[rows:, :].astype(jnp.bfloat16)
        partial(p).start()

    def hidden_to(p, d):
        frm = shb.at[tp] if p == 0 else she
        return remote(frm, shb.at[tp], sent.at[7 + p], shid_r.at[0], ep if p == 0 else edge, (tp + d) % 4)

    def shared_hidden(p):
        square = jnp.zeros((8, rows), jnp.float32)
        for k in range(4):
            square = square + ssq[p, k]
        scale = column(lax.rsqrt(square[0:1, :] / width + 1e-06))[:, 0:1]
        landed(pin.at[p], part_r.at[p])
        val = silu_mul((acc[p] + pin[p].astype(jnp.float32)) * scale, hid)
        if p == 0:
            shb[tp] = val
        else:
            she[...] = val
        for d in (2, 3, 1) if p == 0 else (2, 0):
            hidden_to(p, d).start()

    def shared_inner():
        @pl.when(inner == 1)
        def _():
            pass_tokens(1)
            landed(ssq.at[0, pl.ds(0, 3)], ssq_r.at[0])
            landed(ssq.at[1], ssq_r.at[1])
            shared_sum(1)
            pass_tokens(0)
            shared_sum(0)
            shared_hidden(1)
            shared_hidden(0)

    def shared_swap():
        @pl.when(inner == 0)
        def _():
            landed(shb.at[pl.ds(0, 2)], shid_r.at[0])
            for k in (tp, far):
                remote(shb.at[k], shb.at[k], sent.at[7], shid_r.at[1], ep, mate).start()

    def shared_end():
        at_inner(lambda: landed(shb.at[pl.ds(0, 3)], shid_r.at[0]))
        at_edge(lambda: landed(shb.at[pl.ds(0, 2)], shid_r.at[1]))

    def drain():
        gone(xs.at[pl.ds(0, 2), pl.ds(0, n - 1)], 0)
        gone(xs.at[pl.ds(0, 3)], 1)
        gone(hb.at[pl.ds(0, 3)], 2)
        gone(tk.at[0, pl.ds(0, 2)], 4)

        @pl.when(inner == 0)
        def _():
            gone(ssq.at[0], 5)
            gone(shb.at[pl.ds(0, 2)], 7)
            gone(sw.at[0], 9)

        @pl.when(inner == 1)
        def _():
            gone(tk.at[0], 3)
            gone(ssq.at[0, pl.ds(0, 3)], 5)
            gone(pin, 6)
            gone(shb.at[pl.ds(0, 3)], 7)
            gone(shb.at[pl.ds(0, 2)], 8)
            gone(sw.at[pl.ds(0, 2)], 9)

    def combined(i):
        zz = order[i]
        landed(ret.at[pl.ds(0, 2)] if i > 0 else ret.at[0], ret_r.at[zz])
        got = ret[pl.ds(zz * 2, 2)].reshape(2 * cap, quarter)
        val = 0.0 if i == 0 else mix[...]
        for k in range(2):
            val = val + column(gates[k : k + 1, :])[:, 0:1] * jnp.dot(
                back[k, zz], got, preferred_element_type=jnp.float32
            )
        return val

    def combine(i):
        mix[...] = combined(i)

    stage_a(0)
    stage_a(1)
    edge_pass()
    stage_b(0)
    stage_c(0)
    stage_b(1)
    stage_a(2)
    hidden_on(0)
    stage_c(1)
    at_inner(lambda: rows_of(0).start())
    stage_d(0)
    send_back(0)
    stage_b(2)
    hidden_on(1)
    stage_a(3)
    stage_d(1)
    send_back(1)
    rows_pass()
    stage_c(2)
    stage_b(3)
    at_inner(lambda: spread_tokens(1, 1))
    at_inner(lambda: spread_tokens(0, 1))
    stage_d(2)
    send_back(2)
    stage_c(3)
    at_inner(lambda: spread_tokens(1, 0))
    stage_d(3)
    send_back(3)
    gates_in.wait()
    shared_inner()
    combine(0)
    combine(1)
    shared_swap()
    combine(2)
    shared_end()
    sdown_in.wait()
    hidden = jnp.concatenate([shb[k] for k in range(4)], axis=-1)
    mix[...] += jnp.dot(hidden, sdn[...], preferred_element_type=jnp.float32)
    out[...] = combined(3).astype(jnp.bfloat16)
    drain()


def shards(
    tokens, norm_gain, expert_ids, expert_gates, gate_proj, up_proj, down_proj,
    shared_gate, shared_up, shared_down, plain,
):
    n = lax.axis_size("ep")
    rows, quarter = tokens.shape
    top = expert_ids.shape[1]
    exp_dev = gate_proj.shape[0]
    cap = 3 * rows * top // (2 * exp_dev * n)
    hid = gate_proj.shape[2]
    depth = shared_gate.shape[0]
    ok = exp_dev == 1 and top == 2 and cap % 16 == 0 and hid % 128 == 0 and rows == 128
    ok = ok and shared_gate.shape[1] == hid and quarter == 2 * depth and depth % 128 == 0
    if plain or not ok:
        return shards_plain(
            tokens, norm_gain, expert_ids, expert_gates, gate_proj, up_proj, down_proj,
            shared_gate, shared_up, shared_down,
        )
    width = norm_gain.shape[0]
    bf = jnp.bfloat16
    nz = n // 2
    dma = pltpu.SemaphoreType.DMA
    vm = pl.BlockSpec(memory_space=pltpu.VMEM)
    hbm = pl.BlockSpec(memory_space=pltpu.HBM)
    operands = (
        tokens, norm_gain.reshape(1, width), expert_ids.T, expert_gates.T, gate_proj, up_proj, down_proj,
        shared_gate, shared_up, shared_down,
    )
    return pl.pallas_call(
        functools.partial(kernel, n),
        out_shape=jax.ShapeDtypeStruct((rows, quarter), bf),
        in_specs=[hbm] * 10,
        out_specs=vm,
        scratch_shapes=[
            pltpu.VMEM(tokens.shape, bf),
            pltpu.VMEM((1, width), jnp.float32),
            pltpu.VMEM((top, rows), jnp.int32),
            pltpu.VMEM((top, rows), jnp.float32),
            pltpu.VMEM((width, 2 * hid), bf),
            pltpu.VMEM(down_proj.shape[1:], bf),
            pltpu.VMEM(shared_down.shape, bf),
            pltpu.VMEM((top, nz, rows, 2 * cap), bf),
            pltpu.VMEM((n, cap, quarter), bf),
            pltpu.VMEM((4, n, cap, quarter), bf),
            pltpu.VMEM((2, 4, 2, rows, depth), bf),
            pltpu.VMEM((2, 4, 8, rows), jnp.float32),
            pltpu.VMEM((4, n, cap, hid), bf),
            pltpu.VMEM((4, rows, hid), bf),
            pltpu.VMEM((n, cap, quarter), bf),
            pltpu.VMEM((n, cap, quarter), bf),
            pltpu.VMEM((nz, depth, 2 * hid), bf),
            pltpu.VMEM((2, rows, 2 * hid), jnp.float32),
            pltpu.VMEM((2, rows, 2 * hid), bf),
            pltpu.VMEM((2, rows, 2 * hid), bf),
            pltpu.VMEM((rows, hid), bf),
            pltpu.VMEM((rows, quarter), jnp.float32),
            dma((8,)), dma((10,)), dma((n,)),
            dma((nz,)), dma((nz,)), dma((7,)), dma((2,)), dma((nz,)), dma((nz,)), dma((2,)), dma((nz,)), dma((nz,)), dma((2,)),
        ],
        compiler_params=pltpu.CompilerParams(
            collective_id=0, has_side_effects=True, vmem_limit_bytes=48 * 1024 * 1024
        ),
    )(*(pltpu.with_memory_space_constraint(a, pltpu.HBM) for a in operands))


def solution(mesh):
    return jax.shard_map(
        functools.partial(shards, plain=not fits(mesh)),
        mesh=mesh,
        in_specs=(
            P("ep", "tp"),
            P(),
            P("ep", None),
            P("ep", None),
            P("ep", None, "tp"),
            P("ep", None, "tp"),
            P("ep", None, "tp"),
            P("ep", "tp"),
            P("ep", "tp"),
            P(None, "tp"),
        ),
        out_specs=P("ep", "tp"),
        check_vma=False,
    )
```

```python
import functools

import jax
import jax.numpy as jnp
from jax import lax
from jax.experimental import pallas as pl
from jax.experimental.pallas import tpu as pltpu
from jax.sharding import PartitionSpec as P

MESH = pl.DeviceIdType.MESH


def shards_plain(
    tokens,
    norm_gain,
    expert_ids,
    expert_gates,
    gate_proj,
    up_proj,
    down_proj,
    shared_gate,
    shared_up,
    shared_down,
):
    n_ep = lax.axis_size("ep")
    n_tp = lax.axis_size("tp")
    whole = lax.all_gather(tokens, "tp", axis=1, tiled=True)
    tok_rows, width = whole.shape
    quarter = width // n_tp
    floats = whole.astype(jnp.float32)
    scale = lax.rsqrt(jnp.mean(floats * floats, axis=-1, keepdims=True) + 1e-06)
    normed = (floats * scale * norm_gain[None, :]).astype(jnp.bfloat16)
    gate_whole, up_whole = (
        lax.all_gather(shared_gate, "ep", axis=0, tiled=True),
        lax.all_gather(shared_up, "ep", axis=0, tiled=True),
    )
    shared_g = jnp.dot(normed, gate_whole, preferred_element_type=jnp.float32)
    shared_u = jnp.dot(normed, up_whole, preferred_element_type=jnp.float32)
    shared_hidden = (jax.nn.silu(shared_g) * shared_u).astype(jnp.bfloat16)
    rows = shared_down
    shared_out = jnp.dot(
        lax.all_gather(shared_hidden, "tp", axis=1, tiled=True),
        rows,
        preferred_element_type=jnp.float32,
    )
    exp_dev = gate_proj.shape[0]
    n_exp = exp_dev * n_ep
    top = expert_ids.shape[1]
    cap = 3 * tok_rows * top // (2 * n_exp)
    flat_ids = expert_ids.reshape(tok_rows * top)
    onehot = (flat_ids[:, None] == jnp.arange(n_exp, dtype=jnp.int32)[None, :]).astype(jnp.int32)
    slots = jnp.sum((jnp.cumsum(onehot, axis=0) - onehot) * onehot, axis=-1)
    dest = flat_ids * cap + slots
    local_tok = jnp.repeat(jnp.arange(tok_rows, dtype=jnp.int32), top)
    owner = jnp.full((n_exp * cap,), tok_rows, jnp.int32).at[dest].set(local_tok)
    padded = jnp.concatenate([normed, jnp.zeros((1, width), jnp.bfloat16)], axis=0)
    outgoing = padded[owner].reshape(n_ep, exp_dev, cap, width)
    received = lax.all_to_all(outgoing, "ep", split_axis=0, concat_axis=0, tiled=True)
    gate_vals = jnp.einsum(
        "secd,edh->sech", received, gate_proj, preferred_element_type=jnp.float32
    )
    up_vals = jnp.einsum("secd,edh->sech", received, up_proj, preferred_element_type=jnp.float32)
    expert_hidden = (jax.nn.silu(gate_vals) * up_vals).astype(jnp.bfloat16)
    rows = down_proj
    expert_out = jnp.einsum(
        "sech,ehd->secd",
        lax.all_gather(expert_hidden, "tp", axis=3, tiled=True),
        rows,
        preferred_element_type=jnp.float32,
    ).astype(jnp.bfloat16)
    returned = lax.all_to_all(expert_out, "ep", split_axis=0, concat_axis=0, tiled=True)
    picked = returned.reshape(n_exp * cap, quarter)[dest].reshape(tok_rows, top, quarter)
    routed = jnp.sum(expert_gates[:, :, None] * picked.astype(jnp.float32), axis=1)
    return (routed + shared_out).astype(jnp.bfloat16)


def fits(mesh):
    return mesh.shape["tp"] == 4 and mesh.shape["ep"] == 8


def remote(src, dst, send, recv, ep, tp):
    return pltpu.make_async_remote_copy(
        src_ref=src, dst_ref=dst, send_sem=send, recv_sem=recv, device_id=(ep, tp), device_id_type=MESH
    )


def silu_mul(v, hid):
    g, u = v[:, :hid], v[:, hid:]
    return ((g / (1.0 + jnp.exp(-g))) * u).astype(jnp.bfloat16)


def kernel(
    n,
    tokens_hbm, gain_hbm, ids_hbm, gates_hbm, gate_w, up_w, down_w, sgate_w, sup_w, sdown_w,
    out,
    tokens, gain, ids, gates, wgu, wdn, sdn, back, outbox, xs, tk, ssq, hb, shb, ob, ret, sw,
    acc, pout, pin, she, mix,
    load_sem, sent, disp_r, far_r, near_r, tk_r, ssq_r, hid_r, hid_far, shid_r, ret_r, sw_r, part_r,
):
    ep, tp = lax.axis_index("ep"), lax.axis_index("tp")
    nz = n // 2
    z, x = ep // 2, ep % 2
    ox = ep + 1 - 2 * x
    mate = tp + 1 - 2 * (tp % 2)
    far = (tp + 2) % 4
    diag = (mate + 2) % 4
    rows, quarter = tokens.shape
    cap = xs.shape[2]
    hid = gate_w.shape[2]
    slots = n * cap
    width = gain.shape[1]
    depth = sgate_w.shape[0]

    side = 1 - 2 * (z // 2)
    inner = ((z + 1) // 2) % 2
    half = ep + 2 * side * (1 - 2 * inner)
    order = [z + side * (i - inner * (0, 2, 0, 2)[i]) for i in range(nz)]

    def load(src, dst, k):
        c = pltpu.make_async_copy(src, dst, load_sem.at[k])
        c.start()
        return c

    ids_in = load(ids_hbm, ids, 0)
    tokens_in = load(tokens_hbm, tokens, 1)
    gates_in = load(gates_hbm, gates, 2)
    gain_in = load(gain_hbm, gain, 3)
    load(sgate_w, sw.at[z, :, pl.ds(0, hid)], 4)
    load(sup_w, sw.at[z, :, pl.ds(hid, hid)], 4)
    load(gate_w.at[0], wgu.at[:, pl.ds(0, hid)], 5)
    load(up_w.at[0], wgu.at[:, pl.ds(hid, hid)], 5)
    down_in = load(down_w.at[0], wdn, 6)
    sdown_in = load(sdown_w, sdn, 7)

    barrier = pltpu.get_barrier_semaphore()
    for d in range(1, n):
        pl.semaphore_signal(barrier, inc=1, device_id=((ep + d) % n, tp), device_id_type=MESH)
    for d in range(1, 4):
        pl.semaphore_signal(barrier, inc=1, device_id=(ep, (tp + d) % 4), device_id_type=MESH)
        pl.semaphore_signal(barrier, inc=1, device_id=(half, (tp + d) % 4), device_id_type=MESH)

    def column(row):
        return jnp.broadcast_to(row.astype(jnp.float32), (rows, rows)).T

    ids_in.wait()
    sub = lax.broadcasted_iota(jnp.int32, (rows, rows), 0)
    tok = lax.broadcasted_iota(jnp.int32, (rows, rows), 1)
    one = ((sub == ids[0:1, :]) | (sub == ids[1:2, :])).astype(jnp.float32).astype(jnp.bfloat16)
    earlier = (sub < tok).astype(jnp.float32).astype(jnp.bfloat16)
    place = jnp.dot(one, earlier, preferred_element_type=jnp.float32).astype(jnp.bfloat16)
    slot = lax.broadcasted_iota(jnp.int32, (slots, rows), 0)
    low = lax.broadcasted_iota(jnp.int32, (slots, rows), 1) * cap
    spread = ((slot >= low) & (slot < low + cap)).astype(jnp.float32).astype(jnp.bfloat16)
    place = jnp.dot(spread, place, preferred_element_type=jnp.float32)
    one = jnp.dot(spread, one, preferred_element_type=jnp.float32)
    slotf = slot.astype(jnp.float32)
    within = slotf - jnp.floor((slotf + 0.5) / cap) * cap
    pick = jnp.where(jnp.abs(place - within) < 0.5, one, 0.0).astype(jnp.bfloat16)
    tokens_in.wait()
    outbox[...] = (
        jnp.dot(pick, tokens[...], preferred_element_type=jnp.float32)
        .astype(jnp.bfloat16)
        .reshape(n, cap, quarter)
    )

    pl.semaphore_wait(barrier, n - 1 + 6)

    def landed(dst, sem):
        remote(dst, dst, sem, sem, ep, mate).wait_recv()

    def gone(src, k):
        remote(src, src, sent.at[k], sent.at[k], ep, mate).wait_send()

    xs[tp, ep] = outbox[ep]

    def dispatch(e):
        remote(outbox.at[e], xs.at[tp, ep], sent.at[0], disp_r.at[ep], e, tp).start()

    def spread_block(i, j):
        s = order[i] * 2 + (x + j) % 2
        blk = xs.at[tp, s]
        remote(blk, blk, sent.at[1], far_r.at[i], ep, far).start()
        remote(blk, blk, sent.at[1], near_r.at[i], ep, mate).start()

    def rows_of(i):
        blk = sw.at[order[i]]
        return remote(blk, blk, sent.at[9], sw_r.at[order[i]], ep + 2 * side, tp)

    def at_inner(f):
        pl.when(inner == 1)(f)

    def at_edge(f):
        pl.when(inner == 0)(f)

    spread_block(0, 0)
    dispatch(ox)
    for i in range(1, nz):
        for j in range(2):
            dispatch(order[i] * 2 + (x + j) % 2)
    pltpu.make_async_copy(sw.at[z], sw.at[z], load_sem.at[4]).wait()
    at_edge(lambda: rows_of(0).start())

    mine = tokens.at[:, pl.ds(pl.multiple_of(x * depth, depth), depth)]
    theirs = tokens.at[:, pl.ds(pl.multiple_of((1 - x) * depth, depth), depth)]
    home = ep + 2 * side * (1 - inner)
    home_ox = ox + 2 * side * (1 - inner)
    edge = ep - 2 * side
    plane = 1 - inner

    def own_tokens():
        remote(mine, tk.at[1, tp, 0], sent.at[4], tk_r.at[0], ep, far).start()
        remote(mine, tk.at[1, tp, 0], sent.at[4], tk_r.at[6], home, tp).start()

    def edge_pass():
        @pl.when(inner == 0)
        def _():
            blk = tk.at[1, far, 0]
            landed(blk, tk_r.at[0])
            remote(blk, blk, sent.at[4], tk_r.at[3], home, tp).start()

    remote(theirs, tk.at[plane, tp, 1], sent.at[4], tk_r.at[plane], home_ox, tp).start()
    at_edge(own_tokens)
    own = tokens[...].astype(jnp.float32)
    sums = jnp.broadcast_to(jnp.sum(own * own, axis=-1, keepdims=True), (rows, 128)).T
    ssq[plane, tp] = sums[0:8, :]
    for d in range(1, 4):
        remote(ssq.at[plane, tp], ssq.at[plane, tp], sent.at[5], ssq_r.at[plane], home, (tp + d) % 4).start()

    def own_square():
        return remote(ssq.at[1, tp], ssq.at[1, tp], sent.at[5], ssq_r.at[1], home, tp)

    at_edge(lambda: own_square().start())

    def first_tokens(who, k):
        return remote(mine, tk.at[0, tp, 0], sent.at[4], tk_r.at[k], ep, who)

    @pl.when(inner == 1)
    def _():
        first_tokens(far, 2).start()
        first_tokens(mate, 4).start()
        tk[0, tp, 0] = mine[...]

    def places():
        lane = lax.broadcasted_iota(jnp.int32, (rows, 128), 1).astype(jnp.float32)
        ones = [(lane == column(ids[k : k + 1, :])).astype(jnp.float32) for k in range(2)]
        named = (ones[0] + ones[1]).astype(jnp.bfloat16)
        before = (tok < sub).astype(jnp.float32).astype(jnp.bfloat16)
        place = jnp.dot(before, named, preferred_element_type=jnp.float32).astype(jnp.bfloat16)
        low = lax.broadcasted_iota(jnp.int32, (128, slots), 0) * cap
        col = lax.broadcasted_iota(jnp.int32, (128, slots), 1)
        spread = ((col >= low) & (col < low + cap)).astype(jnp.float32).astype(jnp.bfloat16)
        place = jnp.dot(place, spread, preferred_element_type=jnp.float32)
        colf = lax.broadcasted_iota(jnp.int32, (rows, slots), 1).astype(jnp.float32)
        within = colf - jnp.floor((colf + 0.5) / cap) * cap
        hit = jnp.abs(place - within) < 0.5
        for k in range(2):
            sel = jnp.where(
                hit, jnp.dot(ones[k].astype(jnp.bfloat16), spread, preferred_element_type=jnp.float32), 0.0
            )
            for e in range(nz):
                back[k, e] = sel[:, 2 * e * cap : 2 * (e + 1) * cap].astype(jnp.bfloat16)

    places()

    def pair(ref, k, i):
        return ref.at[k, pl.ds(order[i] * 2, 2)]

    def stage_a(i):
        for j in range(2):
            s = order[i] * 2 + (x + j) % 2
            if i > 0 or j > 0:
                landed(xs.at[tp, s], disp_r.at[s])
                spread_block(i, j)

    def stage_b(i):
        blk = pair(xs, far, i)
        landed(blk, far_r.at[i])
        remote(blk, blk, sent.at[1], near_r.at[i], ep, mate).start()

    via = (0, 1)

    def stage_c(i):
        landed(xs.at[pl.ds(0, 2), pl.ds(0, 2)], near_r.at[i])
        if i == 0:
            pltpu.make_async_copy(wgu, wgu, load_sem.at[5]).wait()
            gain_in.wait()
        zz = order[i]
        sq = jnp.zeros((2 * cap, 1), jnp.float32)
        for k in range(4):
            v = xs[k, pl.ds(zz * 2, 2)].reshape(2 * cap, quarter).astype(jnp.float32)
            sq = sq + jnp.sum(v * v, axis=-1, keepdims=True)
        scale = lax.rsqrt(sq / width + 1e-06)
        val = jnp.zeros((2 * cap, 2 * hid), jnp.float32)
        for k in range(4):
            cols = slice(k * quarter, (k + 1) * quarter)
            v = xs[k, pl.ds(zz * 2, 2)].reshape(2 * cap, quarter).astype(jnp.float32)
            nk = (v * scale * gain[:, cols]).astype(jnp.bfloat16)
            val = val + jnp.dot(nk, wgu[cols, :], preferred_element_type=jnp.float32)
        hb[tp, pl.ds(zz * 2, 2)] = silu_mul(val, hid).reshape(2, cap, hid)
        blk = pair(hb, tp, i)
        if i in via:
            remote(blk, blk, sent.at[2], hid_far.at[i], ep, far).start()
            remote(blk, blk, sent.at[2], hid_r.at[i], ep, mate).start()
        else:
            for d in (2, 1, 3):
                remote(blk, blk, sent.at[2], hid_r.at[i], ep, (tp + d) % 4).start()

    def hidden_on(i):
        if i in via:
            blk = pair(hb, far, i)
            landed(blk, hid_far.at[i])
            remote(blk, blk, sent.at[2], hid_r.at[i], ep, mate).start()

    def stage_d(i):
        zz = order[i]
        landed(hb.at[pl.ds(0, 2 if i in via else 3), pl.ds(0, 2)], hid_r.at[i])
        if i == 0:
            down_in.wait()
        h = jnp.concatenate([hb[k, pl.ds(zz * 2, 2)].reshape(2 * cap, hid) for k in range(4)], axis=-1)
        res = jnp.dot(h, wdn[...], preferred_element_type=jnp.float32).astype(jnp.bfloat16)
        ob[pl.ds(zz * 2, 2)] = res.reshape(2, cap, quarter)

    def back_to(i, j):
        s = order[i] * 2 + (x + j) % 2
        return remote(ob.at[s], ret.at[ep], sent.at[0], ret_r.at[z], s, tp)

    backs = [[back_to(i, j) for j in range(i == 0, 2)] for i in range(nz)]

    def send_back(i):
        if i == 0:
            ret[ep] = ob[ep]
        for c in backs[i]:
            c.start()

    def rows_pass():
        @pl.when(inner == 1)
        def _():
            landed(sw.at[order[1]], sw_r.at[order[1]])
            rows_of(1).start()

    def tokens_to(p, b, who, k):
        blk = tk.at[p, tp, b]
        return remote(blk, blk, sent.at[3 if (p, b) != (1, 0) else 4], tk_r.at[k + p], ep, who)

    def tokens_on(p):
        return remote(tk.at[p, far], tk.at[p, far], sent.at[3], tk_r.at[4 + p], ep, mate)

    def spread_tokens(p, b):
        landed(tk.at[p, tp, b], tk_r.at[p if b == 1 else 6])
        if (p, b) != (1, 0):
            tokens_to(p, b, far, 2).start()
        tokens_to(p, b, mate, 4).start()

    def pass_tokens(p):
        landed(tk.at[p, far], tk_r.at[2 + p])
        tokens_on(p).start()

    def partial(p):
        return remote(pout.at[p], pin.at[p], sent.at[6], part_r.at[p], ox, tp)

    def shared_sum(p):
        landed(tk.at[p, pl.ds(0, 2)], tk_r.at[4 + p])
        val = jnp.zeros((2 * rows, 2 * hid), jnp.float32)
        for i in (0, 1, 3, 2):
            zz = order[i]
            if p == 1 and i in (2, 3):
                landed(sw.at[zz], sw_r.at[zz])
            cols = pl.ds(pl.multiple_of((2 * zz + x) * depth, depth), depth)
            v = (tk[p, zz].reshape(2 * rows, depth).astype(jnp.float32) * gain[:, cols]).astype(jnp.bfloat16)
            val = val + jnp.dot(v, sw[zz], preferred_element_type=jnp.float32)
        acc[p] = val[0:rows, :]
        pout[p] = val[rows:, :].astype(jnp.bfloat16)
        partial(p).start()

    def hidden_to(p, d):
        frm = shb.at[tp] if p == 0 else she
        return remote(frm, shb.at[tp], sent.at[7 + p], shid_r.at[0], ep if p == 0 else edge, (tp + d) % 4)

    def shared_hidden(p):
        square = jnp.zeros((8, rows), jnp.float32)
        for k in range(4):
            square = square + ssq[p, k]
        scale = column(lax.rsqrt(square[0:1, :] / width + 1e-06))[:, 0:1]
        landed(pin.at[p], part_r.at[p])
        val = silu_mul((acc[p] + pin[p].astype(jnp.float32)) * scale, hid)
        if p == 0:
            shb[tp] = val
        else:
            she[...] = val
        for d in (2, 3, 1) if p == 0 else (2, 0):
            hidden_to(p, d).start()

    def shared_inner():
        @pl.when(inner == 1)
        def _():
            pass_tokens(1)
            landed(ssq.at[0, pl.ds(0, 3)], ssq_r.at[0])
            landed(ssq.at[1], ssq_r.at[1])
            shared_sum(1)
            pass_tokens(0)
            shared_sum(0)
            shared_hidden(1)
            shared_hidden(0)

    def shared_swap():
        @pl.when(inner == 0)
        def _():
            landed(shb.at[pl.ds(0, 2)], shid_r.at[0])
            for k in (tp, far):
                remote(shb.at[k], shb.at[k], sent.at[7], shid_r.at[1], ep, mate).start()

    def shared_end():
        at_inner(lambda: landed(shb.at[pl.ds(0, 3)], shid_r.at[0]))
        at_edge(lambda: landed(shb.at[pl.ds(0, 2)], shid_r.at[1]))

    def drain():
        gone(xs.at[pl.ds(0, 2), pl.ds(0, n - 1)], 0)
        gone(xs.at[pl.ds(0, 3)], 1)
        gone(hb.at[pl.ds(0, 3)], 2)
        gone(tk.at[0, pl.ds(0, 2)], 4)

        @pl.when(inner == 0)
        def _():
            gone(ssq.at[0], 5)
            gone(shb.at[pl.ds(0, 2)], 7)
            gone(sw.at[0], 9)

        @pl.when(inner == 1)
        def _():
            gone(tk.at[0], 3)
            gone(ssq.at[0, pl.ds(0, 3)], 5)
            gone(pin, 6)
            gone(shb.at[pl.ds(0, 3)], 7)
            gone(shb.at[pl.ds(0, 2)], 8)
            gone(sw.at[pl.ds(0, 2)], 9)

    def combined(i):
        zz = order[i]
        landed(ret.at[pl.ds(0, 2)] if i > 0 else ret.at[0], ret_r.at[zz])
        got = ret[pl.ds(zz * 2, 2)].reshape(2 * cap, quarter)
        val = 0.0 if i == 0 else mix[...]
        for k in range(2):
            val = val + column(gates[k : k + 1, :])[:, 0:1] * jnp.dot(
                back[k, zz], got, preferred_element_type=jnp.float32
            )
        return val

    def combine(i):
        mix[...] = combined(i)

    stage_a(0)
    stage_a(1)
    edge_pass()
    stage_b(0)
    stage_c(0)
    stage_b(1)
    stage_a(2)
    hidden_on(0)
    stage_c(1)
    at_inner(lambda: rows_of(0).start())
    stage_d(0)
    send_back(0)
    stage_b(2)
    hidden_on(1)
    stage_a(3)
    stage_d(1)
    send_back(1)
    stage_c(2)
    rows_pass()
    stage_b(3)
    at_inner(lambda: spread_tokens(1, 1))
    at_inner(lambda: spread_tokens(0, 1))
    stage_d(2)
    send_back(2)
    stage_c(3)
    at_inner(lambda: spread_tokens(1, 0))
    stage_d(3)
    send_back(3)
    gates_in.wait()
    shared_inner()
    combine(0)
    combine(1)
    shared_swap()
    combine(2)
    shared_end()
    sdown_in.wait()
    hidden = jnp.concatenate([shb[k] for k in range(4)], axis=-1)
    mix[...] += jnp.dot(hidden, sdn[...], preferred_element_type=jnp.float32)
    out[...] = combined(3).astype(jnp.bfloat16)
    drain()


def shards(
    tokens, norm_gain, expert_ids, expert_gates, gate_proj, up_proj, down_proj,
    shared_gate, shared_up, shared_down, plain,
):
    n = lax.axis_size("ep")
    rows, quarter = tokens.shape
    top = expert_ids.shape[1]
    exp_dev = gate_proj.shape[0]
    cap = 3 * rows * top // (2 * exp_dev * n)
    hid = gate_proj.shape[2]
    depth = shared_gate.shape[0]
    ok = exp_dev == 1 and top == 2 and cap % 16 == 0 and hid % 128 == 0 and rows == 128
    ok = ok and shared_gate.shape[1] == hid and quarter == 2 * depth and depth % 128 == 0
    if plain or not ok:
        return shards_plain(
            tokens, norm_gain, expert_ids, expert_gates, gate_proj, up_proj, down_proj,
            shared_gate, shared_up, shared_down,
        )
    width = norm_gain.shape[0]
    bf = jnp.bfloat16
    nz = n // 2
    dma = pltpu.SemaphoreType.DMA
    vm = pl.BlockSpec(memory_space=pltpu.VMEM)
    hbm = pl.BlockSpec(memory_space=pltpu.HBM)
    operands = (
        tokens, norm_gain.reshape(1, width), expert_ids.T, expert_gates.T, gate_proj, up_proj, down_proj,
        shared_gate, shared_up, shared_down,
    )
    return pl.pallas_call(
        functools.partial(kernel, n),
        out_shape=jax.ShapeDtypeStruct((rows, quarter), bf),
        in_specs=[hbm] * 10,
        out_specs=vm,
        scratch_shapes=[
            pltpu.VMEM(tokens.shape, bf),
            pltpu.VMEM((1, width), jnp.float32),
            pltpu.VMEM((top, rows), jnp.int32),
            pltpu.VMEM((top, rows), jnp.float32),
            pltpu.VMEM((width, 2 * hid), bf),
            pltpu.VMEM(down_proj.shape[1:], bf),
            pltpu.VMEM(shared_down.shape, bf),
            pltpu.VMEM((top, nz, rows, 2 * cap), bf),
            pltpu.VMEM((n, cap, quarter), bf),
            pltpu.VMEM((4, n, cap, quarter), bf),
            pltpu.VMEM((2, 4, 2, rows, depth), bf),
            pltpu.VMEM((2, 4, 8, rows), jnp.float32),
            pltpu.VMEM((4, n, cap, hid), bf),
            pltpu.VMEM((4, rows, hid), bf),
            pltpu.VMEM((n, cap, quarter), bf),
            pltpu.VMEM((n, cap, quarter), bf),
            pltpu.VMEM((nz, depth, 2 * hid), bf),
            pltpu.VMEM((2, rows, 2 * hid), jnp.float32),
            pltpu.VMEM((2, rows, 2 * hid), bf),
            pltpu.VMEM((2, rows, 2 * hid), bf),
            pltpu.VMEM((rows, hid), bf),
            pltpu.VMEM((rows, quarter), jnp.float32),
            dma((8,)), dma((10,)), dma((n,)),
            dma((nz,)), dma((nz,)), dma((7,)), dma((2,)), dma((nz,)), dma((nz,)), dma((2,)), dma((nz,)), dma((nz,)), dma((2,)),
        ],
        compiler_params=pltpu.CompilerParams(
            collective_id=0, has_side_effects=True, vmem_limit_bytes=48 * 1024 * 1024,
        ),
    )(*(pltpu.with_memory_space_constraint(a, pltpu.HBM) for a in operands))


def solution(mesh):
    return jax.shard_map(
        functools.partial(shards, plain=not fits(mesh)),
        mesh=mesh,
        in_specs=(
            P("ep", "tp"),
            P(),
            P("ep", None),
            P("ep", None),
            P("ep", None, "tp"),
            P("ep", None, "tp"),
            P("ep", None, "tp"),
            P("ep", "tp"),
            P("ep", "tp"),
            P(None, "tp"),
        ),
        out_specs=P("ep", "tp"),
        check_vma=False,
    )
```
